32 devices in a mesh: sp: 8 (over z, core), tp: 4 (over y, x).
Axes of the slice: x: 2, y: 2, z: 4, core: 2. Of those that a mesh axis runs over, the one named last changes fastest.
Arguments:
- residual_in: bfloat16 [2048, 2048], P('sp', 'tp'), may hold values from -20 to 20
- conv_value: bfloat16 [2048, 2048], P('sp', 'tp'), may hold values from -6 to 6
- conv_gate: bfloat16 [2048, 2048], P('sp', 'tp'), may hold values from -9 to 9
- doc_ids: int32 [2048], P('sp'), may hold values from 0 to 3, never falling along the last dimension, each value on 1 to 1024 neighbouring positions
- conv_kernel: bfloat16 [31, 2048], P(None, 'tp'), may hold values from -3 to 3
- ln_gain: bfloat16 [2048], P('tp'), may hold values from 0.099609375 to 1.8984375
- out_weight: bfloat16 [2048, 2048], P(None, 'tp'), may hold values from -0.25 to 0.25
- norm_gain: bfloat16 [2048], P('tp'), may hold values from 0.099609375 to 1.8984375
- routes: int32 [2048, 2], P('sp'), may hold values from 0 to 7, all different within a row; in each aligned block of 256 rows (0 to 255, 256 to 511, ...) at most 128 rows name the same one
- route_weight: float32 [2048, 2], P('sp'), may hold values from 0.1 to 1
- gate_w: bfloat16 [8, 2048, 4096], P('sp', None, 'tp'), may hold values from -0.125 to 0.125
- up_w: bfloat16 [8, 2048, 4096], P('sp', None, 'tp'), may hold values from -0.125 to 0.125
- down_w: bfloat16 [8, 4096, 2048], P('sp', 'tp'), may hold values from -0.125 to 0.125
Outputs:
- mixed: bfloat16 [2048, 2048], P('sp', 'tp')
The draws below stay inside these ranges and needn't reach their ends.
Inputs may be any that keep to these rules, and one draw needn't show every extreme that they name: `routes`: in each aligned block of 256 positions no expert is named by more than 128 positions, a bound that some block reaches; a position's two experts differ. `doc_ids`: never falls along the positions; each document spans 1 to 1024 positions, one exactly that many.
All inputs are finite; a program needn't handle non-finite values.
Results may differ from the reference program's by a relative error of at most 0.012.
Values may be sent and summed in bfloat16 or wider, within the bound.
A program may use at most 64 MiB of HBM per device.

```python
import math
import jax
import jax.numpy as jnp
import numpy as np
from jax import lax

D = 2048
C = 2048
FE = 4096
KW = 31
TOK_SP = 256
TOKENS = 2048
EXPERTS = 8
CAP = 128
N_SP = 8
N_TP = 4


def draw_residual_in(key, part):
    column = jnp.arange(D, dtype=jnp.float32) / D
    scale = 0.3 * 10.0 ** column
    base = jnp.clip(jax.random.normal(key, (TOKENS, D), jnp.float32), -6.0, 6.0)
    return (base * scale).astype(jnp.bfloat16)


def draw_conv_kernel(key, part):
    channel = jnp.arange(C, dtype=jnp.float32) / C
    scale = KW ** (-0.5) * 10.0 ** channel / 3.0
    base = jnp.clip(jax.random.normal(key, (KW, C), jnp.float32), -4.0, 4.0)
    return (base * scale).astype(jnp.bfloat16)


def strengthened(array, own_key, source, target, blocks, factor):
    owner, partner = [(jnp.arange(array.shape[dim]) // (array.shape[dim] // blocks)).reshape([-1 if axis == dim else 1 for axis in range(array.ndim)]) for dim in (source, target)]
    chosen = jax.random.permutation(own_key, blocks)[partner]
    strong = (owner == chosen) | (owner == (partner + blocks // 2) % blocks)
    return jnp.where(strong, factor * array, array)


def levels(own_key, extent, shards, least, top_value):
    def one(dim, shards_of):
        heights = jax.random.uniform(jax.random.fold_in(jax.random.fold_in(own_key, 6), dim), (shards_of,), jnp.float32, least / len(shards), top_value / len(shards))
        return jnp.repeat(jnp.exp(heights), extent[dim] // shards_of).reshape((-1,) + (1,) * (len(extent) - dim - 1))

    gain = one(*shards[0])
    for cut in shards[1:]:
        gain = gain * one(*cut)
    return gain


def length_profile(amount, total, bound, skew):
    portions = [(1 << 20) // math.isqrt(grade ** skew) + 1 for grade in range(2, amount + 1)]
    spare, given = total - bound - (amount - 1), [1] * (amount - 1)
    while spare > 0:
        free = [i for i in range(amount - 1) if given[i] < bound]
        whole, left = sum([portions[i] for i in free]), spare
        for i in free:
            extra = min(bound - given[i], max(1, left * portions[i] // whole), spare)
            given[i] = given[i] + extra
            spare = spare - extra
    return np.array([bound] + given)


def uneven(stream_key, amount, total, bound, lean):
    if amount == 2:
        one = jax.random.randint(stream_key, (), max(1, total - bound), min(bound, total - 1) + 1)
        return jnp.stack([one, total - one])
    tallies = jnp.asarray(length_profile(amount, total, bound, lean), jnp.int32)
    couples = (amount - 1) // 2
    source_of, receiver = tallies[1:1 + 2 * couples:2], tallies[2:2 + 2 * couples:2]
    room = jnp.minimum(source_of - 1, bound - receiver)
    passed = jax.random.randint(jax.random.fold_in(stream_key, 1), (couples,), 0, 1 << 20) % (room + 1)
    tallies = tallies.at[1:1 + 2 * couples:2].set(source_of - passed).at[2:2 + 2 * couples:2].set(receiver + passed)
    return tallies[jax.random.permutation(jax.random.fold_in(stream_key, 2), amount)]


def routed_block(key, own, number, rows, number_of, top, most, lean):
    ranking = jax.random.permutation(key, number_of)
    crowded, usual = shares(number_of, rows * top, most, lean, True), shares(number_of, rows * top, most, lean, False)
    places = jnp.arange(number_of)

    def named(sizes, turn):
        used = int((sizes > 0).sum())
        fixed = max(1, used // 4)
        shifted = fixed + (places - fixed + turn * (used - fixed)) % max(1, number_of - fixed)
        return jnp.zeros((number_of,), jnp.int32).at[ranking[jnp.where(places < fixed, places, shifted)]].set(jnp.asarray(sizes, jnp.int32))

    sizes = jnp.where(number % 4 == 0, named(crowded, number // 4), named(usual, number - number // 4 - 1))
    mixed = jax.random.permutation(jax.random.fold_in(own, 3), number_of)
    source_of, receiver = mixed[0:number_of // 2 * 2:2], mixed[1:number_of // 2 * 2:2]
    margin = jnp.minimum(sizes[source_of] - 1, most - sizes[receiver]) // 2
    margin = jnp.where((source_of == ranking[0]) | (receiver == ranking[0]) | (sizes[receiver] == 0), 0, jnp.maximum(margin, 0))
    shifted = jax.random.randint(jax.random.fold_in(own, 4), (number_of // 2,), 0, 1 << 20) % (margin + 1)
    sizes = sizes.at[source_of].add(-shifted).at[receiver].add(shifted)
    labels = jnp.searchsorted(jnp.cumsum(sizes), jnp.arange(rows * top), side="right").astype(jnp.int32)
    listing = labels.reshape(top, rows).T
    listing = listing[jax.random.permutation(jax.random.fold_in(own, 1), rows)]
    turn = jax.random.randint(jax.random.fold_in(own, 2), (rows, 1), 0, top)
    return jnp.take_along_axis(listing, (jnp.arange(top)[None, :] + turn) % top, axis=1)


def shares(amount, total, reach, lean, full):
    weights = [(1 << 20) // math.isqrt(grade ** lean) + 1 for grade in range(1, amount + 1)]
    largest = reach if full else min(reach, max(-(-total // amount), total * weights[0] // sum(weights)))
    least = 1 if total - largest >= amount - 1 else 0
    counts, rest = [largest] + [least] * (amount - 1), total - largest - least * (amount - 1)
    while rest > 0:
        movable = [i for i in range(1, amount) if counts[i] < largest] or [i for i in range(1, amount) if counts[i] < reach]
        mass, remaining = sum([weights[i] for i in movable]), rest
        for i in movable:
            more = min(reach - counts[i], max(1, remaining * weights[i] // mass), rest)
            counts[i] = counts[i] + more
            rest = rest - more
    return np.array(counts)


def scatter_about(stream_key, dims, width, most, cuts=(), kind=jnp.bfloat16):
    gain = levels(stream_key, dims, cuts, -0.22, 0.18) if cuts else 1.0
    drawn = jax.random.normal(stream_key, dims, jnp.float32) * width * gain
    return jnp.minimum(jnp.maximum(drawn, -most), most).astype(kind)


def bell_draw_with(own_key, dims, deviation, reach, pieces, heavy, kind=jnp.bfloat16):
    drawn = deviation * jax.random.normal(own_key, dims, jnp.float32)
    if pieces:
        drawn = drawn * levels(own_key, dims, pieces, -0.22, 0.18)
    return jnp.clip(strengthened(drawn, jax.random.fold_in(own_key, 3), *heavy), -reach, reach).astype(kind)


def setup_inputs(seed: int = 0) -> dict:
    key_list = jax.random.split(jax.random.key(seed), 14)
    residual_in = draw_residual_in(jax.random.fold_in(key_list[13], 71), 0)
    conv_value = scatter_about(key_list[1], (TOKENS, C), 1.0, 6.0, ((0, 8), (1, 4)))
    conv_gate = scatter_about(key_list[2], (TOKENS, C), 1.5, 9.0, ((0, 8), (1, 4)))
    doc_ids = jnp.searchsorted(jnp.cumsum(uneven(key_list[3], N_SP // 2, TOKENS, 4 * TOK_SP, 0)), jnp.arange(TOKENS), side="right").astype(jnp.int32)
    conv_kernel = draw_conv_kernel(jax.random.fold_in(key_list[13], 71), 0)
    ln_gain = jnp.clip(1.0 + 0.18 * jax.random.normal(key_list[5], (C,), jnp.float32), 0.099609375, 1.8984375).astype(jnp.bfloat16)
    out_weight = scatter_about(key_list[6], (C, D), (C // 4) ** -0.5, 0.25, ((1, 4),))
    norm_gain = jnp.clip(1.0 + 0.18 * jax.random.normal(key_list[7], (D,), jnp.float32), 0.099609375, 1.8984375).astype(jnp.bfloat16)
    routes_keys = jax.random.split(jax.random.fold_in(key_list[8], 1), TOKENS // TOK_SP)
    routes_turns = jax.random.permutation(jax.random.fold_in(key_list[8], 3), TOKENS // TOK_SP)
    routes = jax.vmap(lambda own, number: routed_block(jax.random.fold_in(key_list[8], 2), own, number, TOK_SP, EXPERTS, 2, CAP, 1))(routes_keys, routes_turns).reshape((TOKENS, 2))
    route_weight = jnp.clip(jnp.exp(math.log(1.0) - 2.3025851 * jax.random.uniform(key_list[9], (TOKENS, 2), jnp.float32) ** levels(key_list[9], (TOKENS, 2), ((0, 8),), -0.2, 0.2)), 0.1, 1.0)
    gate_w = scatter_about(key_list[10], (EXPERTS, D, FE), D ** -0.5, 0.125, ((0, 8), (2, 4)))
    up_w = scatter_about(key_list[11], (EXPERTS, D, FE), D ** -0.5, 0.125, ((0, 8), (2, 4)))
    down_w = bell_draw_with(key_list[12], (EXPERTS, FE, D), FE ** -0.5, 0.125, ((0, 8), (1, 4)), (1, 2, 4, 2.0))
    return {"residual_in": residual_in, "conv_value": conv_value, "conv_gate": conv_gate, "doc_ids": doc_ids, "conv_kernel": conv_kernel, "ln_gain": ln_gain, "out_weight": out_weight, "norm_gain": norm_gain, "routes": routes, "route_weight": route_weight, "gate_w": gate_w, "up_w": up_w, "down_w": down_w}


epsilon = 1e-06

def reference(residual_in, conv_value, conv_gate, doc_ids, conv_kernel, ln_gain, out_weight, norm_gain, routes, route_weight, gate_w, up_w, down_w):
    gated = (conv_value.astype(jnp.float32) * jax.nn.sigmoid(conv_gate.astype(jnp.float32))).astype(jnp.bfloat16)
    positions = gated.shape[0]
    lookback = KW - 1
    padded = jnp.concatenate([jnp.zeros((lookback, C), jnp.bfloat16), gated], 0)
    doc_padded = jnp.concatenate([jnp.full((lookback,), -1, jnp.int32), doc_ids], 0)
    kernel = conv_kernel.astype(jnp.float32)
    conv_out = jnp.zeros((positions, C), jnp.float32)
    for kernel_tap in range(KW):
        same_doc = (doc_padded[kernel_tap:kernel_tap + positions] == doc_ids)[:, None]
        conv_out = conv_out + jnp.where(same_doc, padded[kernel_tap:kernel_tap + positions].astype(jnp.float32) * kernel[kernel_tap], 0.0)
    chan_mean = lax.optimization_barrier(jnp.mean(conv_out, 1, keepdims=True))
    chan_square = lax.optimization_barrier(jnp.mean(conv_out * conv_out, 1, keepdims=True))
    activated = jax.nn.silu((conv_out - chan_mean) * lax.rsqrt(chan_square - chan_mean * chan_mean + epsilon) * ln_gain.astype(jnp.float32)).astype(jnp.bfloat16)
    projected = jnp.dot(activated, out_weight, preferred_element_type=jnp.float32).astype(jnp.bfloat16)
    stream = (residual_in.astype(jnp.float32) + projected.astype(jnp.float32)).astype(jnp.bfloat16)
    stream_f = stream.astype(jnp.float32)
    normed = (stream_f * lax.rsqrt(lax.optimization_barrier(jnp.mean(stream_f * stream_f, 1, keepdims=True)) + epsilon) * norm_gain.astype(jnp.float32)).astype(jnp.bfloat16)
    capacity = 4 * TOK_SP // EXPERTS
    flat_routes = routes.reshape(N_SP, TOK_SP * 2)
    onehot = (flat_routes[:, :, None] == jnp.arange(EXPERTS, dtype=jnp.int32)).astype(jnp.int32)
    slot_rank = lax.optimization_barrier(jnp.sum((jnp.cumsum(onehot, 1) - onehot) * onehot, 2)).astype(jnp.int32)
    token_local = jnp.arange(TOK_SP * 2, dtype=jnp.int32) // 2
    block_start = (jnp.arange(N_SP, dtype=jnp.int32) * TOK_SP)[:, None]
    token_global = token_local[None, :] + block_start
    slot_token = jnp.full((N_SP, EXPERTS * capacity), positions, jnp.int32)
    slot_token = slot_token.at[jnp.arange(N_SP, dtype=jnp.int32)[:, None], flat_routes * capacity + slot_rank].set(token_global)
    slot_token = slot_token.reshape(N_SP, EXPERTS, capacity).transpose(1, 0, 2).reshape(EXPERTS, N_SP * capacity)

    def expert(operands):
        chosen, weight_gate, weight_up, weight_down = operands
        gathered = jnp.take(normed, chosen, axis=0, mode='fill', fill_value=0)
        hidden = (jax.nn.silu(jnp.dot(gathered, weight_gate, preferred_element_type=jnp.float32)) * jnp.dot(gathered, weight_up, preferred_element_type=jnp.float32)).astype(jnp.bfloat16)
        blocks = hidden.reshape(-1, N_TP, FE // N_TP).astype(jnp.float32)
        partials = jnp.einsum('rnf,nfd->nrd', blocks, weight_down.reshape(N_TP, FE // N_TP, D).astype(jnp.float32))
        partials = lax.optimization_barrier(partials.astype(jnp.bfloat16)).astype(jnp.float32)
        return lax.optimization_barrier(jnp.sum(partials, 0)).astype(jnp.bfloat16)
    expert_out = lax.map(expert, (slot_token, gate_w, up_w, down_w))
    source_row = jnp.arange(N_SP, dtype=jnp.int32)[:, None] * capacity
    pick_index = (flat_routes * (N_SP * capacity) + source_row + slot_rank).reshape(-1)
    picked = jnp.take(expert_out.reshape(-1, D), pick_index, axis=0).reshape(positions, 2, D)
    routed = lax.optimization_barrier(jnp.sum(picked.astype(jnp.float32) * route_weight[:, :, None], 1))
    return (stream_f + routed).astype(jnp.bfloat16)
```

```python
import functools

import jax
import jax.numpy as jnp
from jax import lax
from jax.experimental import pallas as pl
from jax.experimental.pallas import tpu as pltpu
from jax.sharding import PartitionSpec as P

epsilon = 1e-06
groups = 4


def transposed_dot(a, b):
    return lax.dot_general(a, b, (((0,), (0,)), ((), ())), preferred_element_type=jnp.float32)


def remote(src, dst, send_sem, recv_sem, sp, tp):
    return pltpu.make_async_remote_copy(
        src_ref=src,
        dst_ref=dst,
        send_sem=send_sem,
        recv_sem=recv_sem,
        device_id=(sp, tp),
        device_id_type=pl.DeviceIdType.MESH,
    )


def layer_kernel(
    n_sp,
    n_tp,
    cap,
    residual,
    conv_value,
    conv_gate,
    docs,
    conv_kernel,
    ln_gain,
    norm_gain,
    routes,
    route_weight,
    proj_hbm,
    gate_hbm,
    up_hbm,
    down_hbm,
    mixed,
    proj,
    gate,
    up,
    down,
    taps,
    extended,
    doc_extended,
    since,
    conv,
    tail,
    tail_docs,
    halo,
    halo_docs,
    stats,
    activated,
    projected,
    stream,
    normed,
    chosen,
    outbound,
    slots,
    hidden,
    partial,
    arrived,
    summed,
    returned,
    weight_hi,
    weight_lo,
    local_sem,
    halo_send,
    halo_recv,
    stat_send,
    stat_recv,
    act_send,
    act_recv,
    out_send,
    out_recv,
    spread_send,
    spread_recv,
    sum_send,
    sum_recv,
    back_send,
    back_recv,
):
    sp = lax.axis_index("sp")
    tp = lax.axis_index("tp")
    rows, cols = residual.shape
    width = cols * n_tp
    lookback = conv_kernel.shape[0] - 1
    pad = tail.shape[0]
    per_group = n_sp // groups
    group_rows = per_group * cap
    my_group = sp // per_group
    my_member = sp % per_group
    relays = n_tp == 4
    across_x = tp + 1 - 2 * (tp % 2)
    across_y = (tp + 2) % n_tp
    diagonal = (across_x + 2) % n_tp
    loads = [
        pltpu.make_async_copy(src, dst, local_sem.at[i])
        for i, (src, dst) in enumerate(
            ((proj_hbm, proj), (gate_hbm, gate), (up_hbm, up), (down_hbm, down))
        )
    ]
    for load in loads:
        load.start()

    barrier = pltpu.get_barrier_semaphore()
    for i in range(1, n_sp):
        pl.semaphore_signal(
            barrier, inc=1, device_id=((sp + i) % n_sp, tp), device_id_type=pl.DeviceIdType.MESH
        )
    for i in range(1, n_tp):
        pl.semaphore_signal(
            barrier, inc=1, device_id=(sp, (tp + i) % n_tp), device_id_type=pl.DeviceIdType.MESH
        )
    sends = []

    def go(*args):
        send = remote(*args)
        send.start()
        sends.append(send)

    def landed(ref, sem):
        remote(ref, ref, act_send.at[0], sem, sp, tp).wait_recv()

    def col_block(t):
        return pl.ds(pl.multiple_of(t * cols, 128), cols)

    def spread_start(ref, start, size, ss, rs):
        block = ref.at[pl.ds(start, size), col_block(tp)]
        if relays:
            go(block, block, ss(1), rs(1), sp, across_x)
            go(block, block, ss(2), rs(2), sp, across_y)
        else:
            for j in range(1, n_tp):
                go(block, block, ss(j), rs(j), sp, (tp + j) % n_tp)

    def spread_relay(ref, start, size, ss, rs):
        if relays:
            half = size // 2
            landed(ref.at[pl.ds(start, size), col_block(across_x)], rs(1))
            block = ref.at[pl.ds(start, half), col_block(across_x)]
            go(block, block, ss(3), rs(3), sp, across_y)
            landed(ref.at[pl.ds(start, size), col_block(across_y)], rs(2))
            block = ref.at[pl.ds(start + half, half), col_block(across_y)]
            go(block, block, ss(0), rs(0), sp, across_x)

    def spread_finish(ref, start, size, rs):
        if relays:
            half = size // 2
            landed(ref.at[pl.ds(start, half), col_block(diagonal)], rs(3))
            landed(ref.at[pl.ds(start + half, half), col_block(diagonal)], rs(0))
        else:
            for j in range(1, n_tp):
                landed(
                    ref.at[pl.ds(start, size), col_block((tp - j + n_tp) % n_tp)], rs(j)
                )

    def stats_start(i, first, second):
        lane = lax.broadcasted_iota(jnp.int32, (rows, 128), 1)
        both = jnp.where(lane == 0, first, jnp.where(lane == 1, second, 0.0))
        stats[i, 0] = jnp.transpose(both)[0:8]
        for j in range(1, n_tp):
            go(
                stats.at[i, 0],
                stats.at[i, j],
                stat_send.at[i, j],
                stat_recv.at[i, j],
                sp,
                (tp + j) % n_tp,
            )

    def stats_finish(i):
        total = stats[i, 0]
        for j in range(1, n_tp):
            landed(stats.at[i, j], stat_recv.at[i, j])
            total = total + stats[i, j]
        back = jnp.transpose(jnp.concatenate([total] * 16, 0))
        return back[:, 0:1], back[:, 1:2]

    gated = (
        conv_value[...].astype(jnp.float32) * jax.nn.sigmoid(conv_gate[...].astype(jnp.float32))
    ).astype(jnp.bfloat16)
    extended[pl.ds(pad, rows), :] = gated.astype(jnp.float32)
    tail[...] = gated[rows - pad :]
    doc_rows = jnp.transpose(
        jnp.broadcast_to(docs[...].astype(jnp.float32), (128, rows))
    )
    doc_extended[pl.ds(pad, rows), :] = doc_rows
    tail_docs[...] = doc_rows[rows - pad :]
    taps[...] = conv_kernel[...].astype(jnp.float32)
    pl.semaphore_wait(barrier, n_sp - 1 + n_tp - 1)
    next_sp = (sp + 1) % n_sp
    tails = [
        remote(tail, halo, halo_send.at[0], halo_recv.at[0], next_sp, tp),
        remote(tail_docs, halo_docs, halo_send.at[1], halo_recv.at[1], next_sp, tp),
    ]
    for send in tails:
        send.start()
        sends.append(send)

    part = min(64, rows)

    def convolve(r):
        here = pl.ds(r * part, part)
        own = doc_extended[pl.ds(pad + r * part, part), :]
        count = jnp.zeros((part, 128), jnp.float32)
        for back in range(1, lookback + 1):
            count = count + jnp.where(
                doc_extended[pl.ds(pad + r * part - back, part), :] == own, 1.0, 0.0
            )
        since[here, :] = count

        @pl.loop(0, cols // 128)
        def _(c):
            at = pl.ds(pl.multiple_of(c * 128, 128), 128)
            reach = since[here, :]
            total = jnp.zeros((part, 128), jnp.float32)
            for tap in range(lookback + 1):
                value = extended[pl.ds(pad - lookback + r * part + tap, part), at]
                total = total + jnp.where(
                    reach >= lookback - tap, value * taps[tap : tap + 1, at], 0.0
                )
            conv[here, at] = total

    for r in range(1, rows // part):
        convolve(r)
    landed(halo, halo_recv.at[0])
    landed(halo_docs, halo_recv.at[1])
    inside = sp > 0
    extended[pl.ds(0, pad), :] = jnp.where(inside, halo[...].astype(jnp.float32), 0.0)
    doc_extended[pl.ds(0, pad), :] = jnp.where(inside, halo_docs[...], -1.0)
    convolve(0)
    conv_out = conv[...]
    stats_start(
        0,
        jnp.sum(conv_out, 1, keepdims=True),
        jnp.sum(conv_out * conv_out, 1, keepdims=True),
    )

    expert_id = lax.broadcasted_iota(jnp.int32, (rows, n_sp), 1)
    first = routes[:, 0:1] == expert_id
    second = routes[:, 1:2] == expert_id
    named = jnp.where(first | second, 1.0, 0.0)
    earlier = jnp.where(
        lax.broadcasted_iota(jnp.int32, (rows, rows), 1)
        < lax.broadcasted_iota(jnp.int32, (rows, rows), 0),
        1.0,
        0.0,
    ).astype(jnp.bfloat16)
    rank = jnp.dot(earlier, named.astype(jnp.bfloat16), preferred_element_type=jnp.float32)
    slot = jnp.where(first | second, rank, -1.0).astype(jnp.int32)
    weight = jnp.where(first, route_weight[:, 0:1], 0.0) + jnp.where(
        second, route_weight[:, 1:2], 0.0
    )
    slot_id = lax.broadcasted_iota(jnp.int32, (rows, cap), 1)
    for e in range(n_sp):
        chosen[e] = jnp.where(slot[:, e : e + 1] == slot_id, 1.0, 0.0).astype(jnp.bfloat16)

    channel_sum, channel_sq = stats_finish(0)
    mean = channel_sum / width
    scale = lax.rsqrt(channel_sq / width - mean * mean + epsilon)
    v = (conv[...] - mean) * scale * ln_gain[...].astype(jnp.float32)
    activated[:, col_block(tp)] = (v * jax.nn.sigmoid(v)).astype(jnp.bfloat16)

    def act_block(i):
        return act_send.at[i]

    def act_arrival(i):
        return act_recv.at[i]

    spread_start(activated, 0, rows, act_block, act_arrival)
    loads[0].wait()

    def project(t):
        return jnp.dot(
            activated[:, col_block(t)],
            proj[pl.ds(pl.multiple_of(t * cols, 128), cols), :],
            preferred_element_type=jnp.float32,
        )

    projected[...] = project(tp)
    for e in range(n_sp):
        at = jnp.where(slot[:, e : e + 1] == slot_id, weight[:, e : e + 1], 0.0)
        hi = at.astype(jnp.bfloat16)
        weight_hi[e] = hi
        weight_lo[e] = (at - hi.astype(jnp.float32)).astype(jnp.bfloat16)
    spread_relay(activated, 0, rows, act_block, act_arrival)
    if relays:
        projected[...] += project(across_x) + project(across_y)
    spread_finish(activated, 0, rows, act_arrival)
    if relays:
        projected[...] += project(diagonal)
    else:
        for j in range(1, n_tp):
            projected[...] += project((tp + j) % n_tp)
    stream[...] = (
        residual[...].astype(jnp.float32)
        + projected[...].astype(jnp.bfloat16).astype(jnp.float32)
    ).astype(jnp.bfloat16)
    stream_part = stream[...].astype(jnp.float32)
    square = jnp.sum(stream_part * stream_part, 1, keepdims=True)
    stats_start(1, square, square)
    row_total, _ = stats_finish(1)
    normed[...] = (
        stream[...].astype(jnp.float32)
        * lax.rsqrt(row_total / width + epsilon)
        * norm_gain[...].astype(jnp.float32)
    ).astype(jnp.bfloat16)

    def source_rows(s):
        return pl.ds(pl.multiple_of(s * cap, cap), cap)

    def group_start(k):
        return pl.multiple_of((my_group + k) % groups * group_rows, group_rows)

    for k in range(groups):
        for j in range(per_group):
            dest = (my_group - k + groups) % groups * per_group + (my_member + j) % per_group
            rows_out = transposed_dot(chosen[dest], normed[...]).astype(jnp.bfloat16)
            if k == 0 and j == 0:
                slots[source_rows(sp), col_block(tp)] = rows_out
                continue
            outbound[dest] = rows_out
            go(
                outbound.at[dest],
                slots.at[source_rows(sp), col_block(tp)],
                out_send.at[k * per_group + j],
                out_recv.at[sp],
                dest,
                tp,
            )

    def spread_sems(sems, k):
        return lambda i: sems.at[k, i]

    def spread(k):
        for j in range(per_group):
            if k == 0 and j == 0:
                continue
            source = (my_group + k) % groups * per_group + (my_member + j) % per_group
            landed(slots.at[source_rows(source), col_block(tp)], out_recv.at[source])
        spread_start(
            slots, group_start(k), group_rows, spread_sems(spread_send, k), spread_sems(spread_recv, k)
        )

    def relay(k):
        spread_relay(
            slots, group_start(k), group_rows, spread_sems(spread_send, k), spread_sems(spread_recv, k)
        )

    half = group_rows // 2
    low, high = pl.ds(0, half), pl.ds(half, half)

    def compute(k):
        spread_finish(slots, group_start(k), group_rows, spread_sems(spread_recv, k))
        x = pl.ds(group_start(k), group_rows)
        units = gate.shape[1]
        tile = min(256, units)

        @pl.loop(0, units // tile)
        def _(n):
            at = pl.ds(pl.multiple_of(n * tile, tile), tile)
            g = jnp.dot(slots[x, :], gate[:, at], preferred_element_type=jnp.float32)
            u = jnp.dot(slots[x, :], up[:, at], preferred_element_type=jnp.float32)
            hidden[:, at] = (g * jax.nn.sigmoid(g) * u).astype(jnp.bfloat16)

        @pl.loop(0, width // 256)
        def _(n):
            at = pl.ds(pl.multiple_of(n * 256, 256), 256)
            partial[k, :, at] = jnp.dot(
                hidden[...], down[:, at], preferred_element_type=jnp.float32
            ).astype(jnp.bfloat16)

        if relays:
            for i, (part_rows, block, peer) in enumerate(
                (
                    (low, across_x, across_x),
                    (low, diagonal, across_x),
                    (high, across_y, across_y),
                    (high, diagonal, across_y),
                )
            ):
                go(
                    partial.at[k, part_rows, col_block(block)],
                    arrived.at[k, i, low],
                    sum_send.at[k, i],
                    sum_recv.at[k, i],
                    sp,
                    peer,
                )
        else:
            for j in range(1, n_tp):
                peer = (tp + j) % n_tp
                go(
                    partial.at[k, :, col_block(peer)],
                    arrived.at[k, j],
                    sum_send.at[k, j],
                    sum_recv.at[k, j],
                    sp,
                    peer,
                )

    def pass_on(k):
        if relays:
            for i, (part_rows, peer) in enumerate(((low, across_y), (high, across_x))):
                landed(arrived.at[k, 2 * i + 1, low], sum_recv.at[k, 2 * i + 1])
                arrived[k, 2 + i, high] = (
                    partial[k, part_rows, col_block(peer)].astype(jnp.float32)
                    + arrived[k, 2 * i + 1, low].astype(jnp.float32)
                ).astype(jnp.bfloat16)
                go(
                    arrived.at[k, 2 + i, high],
                    arrived.at[k, i, high],
                    sum_send.at[k, 4 + i],
                    sum_recv.at[k, 4 + i],
                    sp,
                    peer,
                )

    def give_back(k):
        if relays:
            for i, part_rows in enumerate((low, high)):
                landed(arrived.at[k, 2 * i, low], sum_recv.at[k, 2 * i])
                landed(arrived.at[k, i, high], sum_recv.at[k, 4 + i])
                summed[k, part_rows] = (
                    partial[k, part_rows, col_block(tp)].astype(jnp.float32)
                    + arrived[k, 2 * i, low].astype(jnp.float32)
                    + arrived[k, i, high].astype(jnp.float32)
                ).astype(jnp.bfloat16)
        else:
            total = partial[k, :, col_block(tp)].astype(jnp.float32)
            for j in range(1, n_tp):
                landed(arrived.at[k, j], sum_recv.at[k, j])
                total = total + arrived[k, j].astype(jnp.float32)
            summed[k] = total.astype(jnp.bfloat16)
        for j in range(per_group):
            member = (my_member + j) % per_group
            source = (my_group + k) % groups * per_group + member
            part = pl.ds(pl.multiple_of(member * cap, cap), cap)
            if k == 0 and j == 0:
                returned[sp] = summed[k, part, :]
                continue
            go(
                summed.at[k, part, :],
                returned.at[sp],
                back_send.at[k * per_group + j],
                back_recv.at[sp],
                source,
                tp,
            )

    spread(0)
    spread(1)
    relay(0)
    spread(2)
    relay(1)
    for load in loads[1:]:
        load.wait()
    compute(0)
    spread(3)
    relay(2)
    compute(1)
    pass_on(0)
    relay(3)
    compute(2)
    pass_on(1)
    give_back(0)
    compute(3)
    pass_on(2)
    give_back(1)
    pass_on(3)
    give_back(2)
    give_back(3)
    for i in range(1, n_sp):
        e = (sp + i) % n_sp
        landed(returned.at[e], back_recv.at[e])
    routed = jnp.zeros((rows, cols), jnp.float32)
    for e in range(n_sp):
        routed = routed + jnp.dot(weight_hi[e], returned[e], preferred_element_type=jnp.float32)
        routed = routed + jnp.dot(weight_lo[e], returned[e], preferred_element_type=jnp.float32)
    mixed[...] = (stream[...].astype(jnp.float32) + routed).astype(jnp.bfloat16)
    for send in sends:
        send.wait_send()


def fused_kernel(
    n_sp,
    n_tp,
    cap,
    residual,
    conv_value,
    conv_gate,
    docs,
    conv_kernel,
    ln_gain,
    norm_gain,
    routes,
    route_weight,
    proj_hbm,
    gate_hbm,
    up_hbm,
    down_hbm,
    mixed,
    proj,
    gate,
    up,
    down,
    taps,
    extended,
    doc_extended,
    since,
    conv,
    tail,
    tail_docs,
    halo,
    halo_docs,
    stats,
    plans,
    scales,
    activated,
    projected,
    stream,
    tokens,
    picks,
    blends,
    slots,
    hidden,
    pairs,
    outbound,
    blended,
    arrived,
    summed,
    returned,
    local_sem,
    halo_send,
    halo_recv,
    stat_send,
    stat_recv,
    plan_send,
    plan_recv,
    scale_send,
    scale_recv,
    act_send,
    act_recv,
    plane_send,
    plane_recv,
    spread_send,
    spread_recv,
    twin_send,
    twin_recv,
    swap_send,
    swap_recv,
    sum_send,
    sum_recv,
    back_send,
    back_recv,
):
    sp = lax.axis_index("sp")
    tp = lax.axis_index("tp")
    rows, cols = residual.shape
    width = cols * n_tp
    lookback = conv_kernel.shape[0] - 1
    pad = tail.shape[0]
    planes = n_sp // 2
    plane = sp // 2
    core = sp % 2
    twin = plane * 2 + 1 - core
    chunk = rows // 2
    half = chunk // 2
    across_x = tp + 1 - 2 * (tp % 2)
    across_y = (tp + 2) % n_tp
    diagonal = (across_x + 2) % n_tp
    loads = [
        pltpu.make_async_copy(src, dst, local_sem.at[i])
        for i, (src, dst) in enumerate(
            ((proj_hbm, proj), (gate_hbm, gate), (up_hbm, up), (down_hbm, down))
        )
    ]
    for load in loads:
        load.start()

    barrier = pltpu.get_barrier_semaphore()
    for i in range(1, n_sp):
        pl.semaphore_signal(
            barrier, inc=1, device_id=((sp + i) % n_sp, tp), device_id_type=pl.DeviceIdType.MESH
        )
    for i in range(1, n_tp):
        pl.semaphore_signal(
            barrier, inc=1, device_id=(sp, (tp + i) % n_tp), device_id_type=pl.DeviceIdType.MESH
        )
    sends = []

    def go(*args):
        send = remote(*args)
        send.start()
        sends.append(send)

    def landed(ref, sem):
        remote(ref, ref, act_send.at[0, 0], sem, sp, tp).wait_recv()

    def col_block(t):
        return pl.ds(pl.multiple_of(t * cols, 128), cols)

    def row_block(start, size):
        return pl.ds(pl.multiple_of(start, size), size)

    def spread_start(ref, start, ss, rs):
        block = ref.at[row_block(start, chunk), col_block(tp)]
        go(block, block, ss(1), rs(1), sp, across_x)
        go(block, block, ss(2), rs(2), sp, across_y)

    def spread_relay(ref, start, ss, rs):
        landed(ref.at[row_block(start, chunk), col_block(across_x)], rs(1))
        block = ref.at[row_block(start, half), col_block(across_x)]
        go(block, block, ss(3), rs(3), sp, across_y)
        landed(ref.at[row_block(start, chunk), col_block(across_y)], rs(2))
        block = ref.at[row_block(start + half, half), col_block(across_y)]
        go(block, block, ss(0), rs(0), sp, across_x)

    def spread_finish(ref, start, rs):
        landed(ref.at[row_block(start, half), col_block(diagonal)], rs(3))
        landed(ref.at[row_block(start + half, half), col_block(diagonal)], rs(0))

    def stats_start(i, q, first, second):
        lane = lax.broadcasted_iota(jnp.int32, (chunk, 128), 1)
        both = jnp.where(lane == 0, first, jnp.where(lane == 1, second, 0.0))
        stats[i, q, 0] = jnp.transpose(both)[0:8]
        for j in range(1, n_tp):
            go(
                stats.at[i, q, 0],
                stats.at[i, q, j],
                stat_send.at[i, q, j],
                stat_recv.at[i, q, j],
                sp,
                (tp + j) % n_tp,
            )

    def stats_total(i, q):
        total = stats[i, q, 0]
        for j in range(1, n_tp):
            landed(stats.at[i, q, j], stat_recv.at[i, q, j])
            total = total + stats[i, q, j]
        return total

    def gain_row(ref):
        return jnp.concatenate(
            [ref[i : i + 1, :].astype(jnp.float32) for i in range(cols // 128)], 1
        )

    gated = (
        conv_value[...].astype(jnp.float32) * jax.nn.sigmoid(conv_gate[...].astype(jnp.float32))
    ).astype(jnp.bfloat16)
    extended[pl.ds(pad, rows), :] = gated.astype(jnp.float32)
    tail[...] = gated[rows - pad :]
    doc_rows = jnp.transpose(jnp.broadcast_to(docs[...].astype(jnp.float32), (128, rows)))
    doc_extended[pl.ds(pad, rows), :] = doc_rows
    tail_docs[...] = doc_rows[rows - pad :]
    taps[...] = conv_kernel[...].astype(jnp.float32)
    plans[sp] = jnp.concatenate(
        [routes[...].astype(jnp.float32), route_weight[...], jnp.zeros((4, rows), jnp.float32)], 0
    )
    pl.semaphore_wait(barrier, n_sp - 1 + n_tp - 1)
    next_sp = (sp + 1) % n_sp
    go(tail, halo, halo_send.at[0], halo_recv.at[0], next_sp, tp)
    go(tail_docs, halo_docs, halo_send.at[1], halo_recv.at[1], next_sp, tp)
    for i in range(1, n_sp):
        go(plans.at[sp], plans.at[sp], plan_send.at[i], plan_recv.at[sp], (sp + i) % n_sp, tp)

    part = min(64, chunk)

    def convolve(r):
        here = pl.ds(r * part, part)
        own = doc_extended[pl.ds(pad + r * part, part), :]
        count = jnp.zeros((part, 128), jnp.float32)
        for back in range(1, lookback + 1):
            count = count + jnp.where(
                doc_extended[pl.ds(pad + r * part - back, part), :] == own, 1.0, 0.0
            )
        since[here, :] = count

        @pl.loop(0, cols // 128)
        def _(c):
            at = pl.ds(pl.multiple_of(c * 128, 128), 128)
            reach = since[here, :]
            total = jnp.zeros((part, 128), jnp.float32)
            for tap in range(lookback + 1):
                value = extended[pl.ds(pad - lookback + r * part + tap, part), at]
                total = total + jnp.where(
                    reach >= lookback - tap, value * taps[tap : tap + 1, at], 0.0
                )
            conv[here, at] = total

    def channel_stats(q):
        conv_out = conv[pl.ds(q * chunk, chunk), :]
        stats_start(
            0,
            q,
            jnp.sum(conv_out, 1, keepdims=True),
            jnp.sum(conv_out * conv_out, 1, keepdims=True),
        )

    def sems(ref, *index):
        return lambda i: ref.at[(*index, i)]

    def activate(q):
        here = pl.ds(q * chunk, chunk)
        back = jnp.transpose(jnp.concatenate([stats_total(0, q)] * 16, 0))
        mean = back[:, 0:1] / width
        scale = lax.rsqrt(back[:, 1:2] / width - mean * mean + epsilon)
        v = (conv[here, :] - mean) * scale * gain_row(ln_gain)
        activated[here, col_block(tp)] = (v * jax.nn.sigmoid(v)).astype(jnp.bfloat16)
        spread_start(activated, q * chunk, sems(act_send, q), sems(act_recv, q))

    def project(q, t):
        return jnp.dot(
            activated[pl.ds(q * chunk, chunk), col_block(t)],
            proj[col_block(t), :],
            preferred_element_type=jnp.float32,
        )

    parts = chunk // part
    for r in range(parts, 2 * parts):
        convolve(r)
    channel_stats(1)
    for r in range(1, parts):
        convolve(r)
    landed(halo, halo_recv.at[0])
    landed(halo_docs, halo_recv.at[1])
    inside = sp > 0
    extended[pl.ds(0, pad), :] = jnp.where(inside, halo[...].astype(jnp.float32), 0.0)
    doc_extended[pl.ds(0, pad), :] = jnp.where(inside, halo_docs[...], -1.0)
    convolve(0)
    channel_stats(0)
    activate(1)
    activate(0)

    for i in range(1, n_sp):
        e = (sp + i) % n_sp
        landed(plans.at[e], plan_recv.at[e])
    token = lax.broadcasted_iota(jnp.int32, (rows, rows), 0)
    later = jnp.where(
        token < lax.broadcasted_iota(jnp.int32, (rows, rows), 1), 1.0, 0.0
    ).astype(jnp.bfloat16)
    slot_id = lax.broadcasted_iota(jnp.int32, (cap, rows), 0)

    def named_by(s, expert):
        plan = plans[s]
        first = plan[0:1] == expert
        second = plan[1:2] == expert
        weight = jnp.where(first, plan[2:3], 0.0) + jnp.where(second, plan[3:4], 0.0)
        return jnp.where(first | second, 1.0, 0.0), weight

    def slots_of(sources, expert):
        both = [named_by(s, expert) for s in sources]
        named = jnp.concatenate([n for n, _ in both] + [jnp.zeros_like(both[0][0])] * (8 - len(both)), 0)
        rank = jnp.dot(named.astype(jnp.bfloat16), later, preferred_element_type=jnp.float32)
        slot = jnp.where(named > 0.5, rank, -1.0).astype(jnp.int32)
        return [(slot[i : i + 1], weight) for i, (_, weight) in enumerate(both)]

    mine = slots_of([2 * p + core for p in range(planes)], sp.astype(jnp.float32))
    rest = slots_of([2 * p + 1 - core for p in range(planes)], sp.astype(jnp.float32))
    other = slots_of([2 * p + core for p in range(planes)], twin.astype(jnp.float32))
    for p in range(planes):
        slot, weight = mine[p]
        picks[p, 0:cap] = jnp.where(slot == slot_id, 1.0, 0.0).astype(jnp.bfloat16)
        blends[p, 0:cap] = jnp.where(slot == slot_id, weight, 0.0).astype(jnp.bfloat16)
        slot, weight = rest[p]
        picks[p, cap : 2 * cap] = jnp.where(slot == slot_id, 1.0, 0.0).astype(jnp.bfloat16)
        slot, weight = other[p]
        blends[p, cap : 2 * cap] = jnp.where(slot == slot_id, weight, 0.0).astype(jnp.bfloat16)

    near = [0]
    for d in range(1, planes // 2 + 1):
        near += [d] if 2 * d == planes else [d, planes - d]

    def source(k):
        return (plane + k) % planes * 2 + core

    def first_row(k, q):
        return source(k) * rows + q * chunk

    def residual_rows(q):
        here = pl.ds(q * chunk, chunk)
        spread_relay(activated, q * chunk, sems(act_send, q), sems(act_recv, q))
        projected[here, :] += project(q, across_x) + project(q, across_y)
        spread_finish(activated, q * chunk, sems(act_recv, q))
        total = projected[here, :] + project(q, diagonal)
        stream_rows = (
            residual[here, :].astype(jnp.float32)
            + total.astype(jnp.bfloat16).astype(jnp.float32)
        ).astype(jnp.bfloat16)
        stream[here, :] = stream_rows
        stream_part = stream_rows.astype(jnp.float32)
        tokens[row_block(first_row(0, q), chunk), col_block(tp)] = (
            stream_part * gain_row(norm_gain)
        ).astype(jnp.bfloat16)
        block = tokens.at[row_block(first_row(0, q), chunk), col_block(tp)]
        spread_start(tokens, first_row(0, q), sems(spread_send, 0, q), sems(spread_recv, 0, q))
        for k in near[1:]:
            go(
                block,
                block,
                plane_send.at[k, q],
                plane_recv.at[k, q],
                (plane - k + planes) % planes * 2 + core,
                tp,
            )
        square = jnp.sum(stream_part * stream_part, 1, keepdims=True)
        stats_start(1, q, square, square)

    loads[0].wait()
    for q in (1, 0):
        projected[pl.ds(q * chunk, chunk), :] = project(q, tp)
    residual_rows(1)
    residual_rows(0)

    def spread(k, q):
        block = tokens.at[row_block(first_row(k, q), chunk), col_block(tp)]
        landed(block, plane_recv.at[k, q])
        spread_start(tokens, first_row(k, q), sems(spread_send, k, q), sems(spread_recv, k, q))

    def relay(k, q):
        spread_relay(tokens, first_row(k, q), sems(spread_send, k, q), sems(spread_recv, k, q))

    def finish(k, q):
        spread_finish(tokens, first_row(k, q), sems(spread_recv, k, q))
        block = tokens.at[row_block(first_row(k, q), chunk), :]
        go(block, block, twin_send.at[k, q], twin_recv.at[k, q], twin, tp)

    def share_scales():
        for q in range(2):
            scales[sp, :, pl.ds(q * chunk, chunk)] = lax.rsqrt(
                stats_total(1, q) / width + epsilon
            )
        for i in range(1, n_sp):
            go(
                scales.at[sp],
                scales.at[sp],
                scale_send.at[i],
                scale_recv.at[sp],
                (sp + i) % n_sp,
                tp,
            )

    def gather(k):
        p = (plane + k) % planes
        for q in range(2):
            start = (2 * p + 1 - core) * rows + q * chunk
            landed(tokens.at[row_block(start, chunk), :], twin_recv.at[k, q])
        for j in range(2):
            s = 2 * p + (core if j == 0 else 1 - core)
            if k == 0 and j == 0:
                pass
            else:
                landed(scales.at[s], scale_recv.at[s])
            here = pl.ds(j * cap, cap)
            pick = picks[p, here, :]
            slots[here, :] = jnp.dot(
                pick, tokens[row_block(s * rows, rows), :], preferred_element_type=jnp.float32
            ).astype(jnp.bfloat16)
            scale = jnp.sum(pick.astype(jnp.float32) * scales[s][0:1, :], 1, keepdims=True)
            since[here, :] = jnp.broadcast_to(scale, (cap, 128))

    def raise_up(k):
        units = gate.shape[1]
        tile = min(256, units)

        @pl.loop(0, units // tile)
        def _(n):
            at = pl.ds(pl.multiple_of(n * tile, tile), tile)
            scale = since[0 : 2 * cap, 0:1]
            g = scale * jnp.dot(slots[...], gate[:, at], preferred_element_type=jnp.float32)
            u = scale * jnp.dot(slots[...], up[:, at], preferred_element_type=jnp.float32)
            hidden[:, at] = (g * jax.nn.sigmoid(g) * u).astype(jnp.bfloat16)

    def bring_down(k):
        @pl.loop(0, width // 256)
        def _(n):
            at = pl.ds(pl.multiple_of(n * 256, 256), 256)
            result = jnp.dot(
                hidden[...], down[:, at], preferred_element_type=jnp.float32
            ).astype(jnp.bfloat16)
            pairs[k, 0:cap, at] = result[0:cap]
            outbound[k, :, at] = result[cap:]

        go(
            outbound.at[k],
            pairs.at[k, pl.ds(cap, cap), :],
            swap_send.at[k],
            swap_recv.at[k],
            twin,
            tp,
        )

    low, high = pl.ds(0, chunk), pl.ds(chunk, chunk)

    def combine(k):
        p = (plane + k) % planes
        landed(pairs.at[k, pl.ds(cap, cap), :], swap_recv.at[k])

        @pl.loop(0, width // 256)
        def _(n):
            at = pl.ds(pl.multiple_of(n * 256, 256), 256)
            blended[k, :, at] = transposed_dot(blends[p], pairs[k, :, at]).astype(jnp.bfloat16)

        for i, (part_rows, block, peer) in enumerate(
            (
                (low, diagonal, across_x),
                (high, diagonal, across_y),
                (low, across_x, across_x),
                (high, across_y, across_y),
            )
        ):
            go(
                blended.at[k, part_rows, col_block(block)],
                arrived.at[k, i, low],
                sum_send.at[k, i],
                sum_recv.at[k, i],
                sp,
                peer,
            )

    def pass_on(k):
        for i, (part_rows, peer) in enumerate(((low, across_y), (high, across_x))):
            landed(arrived.at[k, i, low], sum_recv.at[k, i])
            arrived[k, 2 + i, high] = (
                blended[k, part_rows, col_block(peer)].astype(jnp.float32)
                + arrived[k, i, low].astype(jnp.float32)
            ).astype(jnp.bfloat16)
            go(
                arrived.at[k, 2 + i, high],
                arrived.at[k, i, high],
                sum_send.at[k, 4 + i],
                sum_recv.at[k, 4 + i],
                sp,
                peer,
            )

    def give_back(k):
        for i, part_rows in enumerate((low, high)):
            landed(arrived.at[k, 2 + i, low], sum_recv.at[k, 2 + i])
            landed(arrived.at[k, i, high], sum_recv.at[k, 4 + i])
            total = (
                blended[k, part_rows, col_block(tp)].astype(jnp.float32)
                + arrived[k, 2 + i, low].astype(jnp.float32)
                + arrived[k, i, high].astype(jnp.float32)
            )
            if k == 0:
                here = pl.ds(i * chunk, chunk)
                total = total + stream[here, :].astype(jnp.float32)
                for j in near[1:]:
                    landed(returned.at[j, part_rows], back_recv.at[j, i])
                    total = total + returned[j, part_rows].astype(jnp.float32)
                mixed[here, :] = total.astype(jnp.bfloat16)
            else:
                summed[k, part_rows] = total.astype(jnp.bfloat16)
                go(
                    summed.at[k, part_rows],
                    returned.at[k, part_rows],
                    back_send.at[k, i],
                    back_recv.at[k, i],
                    source(k),
                    tp,
                )

    near_order = near
    relay(0, 1)
    relay(0, 0)
    share_scales()
    a, b, c, d = near_order
    for q in (1, 0):
        spread(b, q)
    finish(0, 1)
    finish(0, 0)
    for q in (1, 0):
        relay(b, q)
        spread(c, q)
    for load in loads[1:]:
        load.wait()
    gather(0)
    raise_up(0)
    finish(b, 1)
    finish(b, 0)
    relay(c, 1)
    spread(d, 1)
    bring_down(0)
    relay(c, 0)
    spread(d, 0)
    gather(b)
    raise_up(b)
    finish(c, 1)
    finish(c, 0)
    bring_down(b)
    relay(d, 1)
    relay(d, 0)
    combine(b)
    gather(c)
    raise_up(c)
    finish(d, 1)
    finish(d, 0)
    bring_down(c)
    pass_on(b)
    combine(c)
    gather(d)
    raise_up(d)
    give_back(b)
    bring_down(d)
    pass_on(c)
    combine(d)
    give_back(c)
    combine(0)
    pass_on(d)
    pass_on(0)
    give_back(d)
    give_back(0)
    for send in sends:
        send.wait_send()


def fused(operands, rows, cols, n_sp, n_tp, cap, width, units, taps):
    planes = n_sp // 2
    pad = (taps - 1 + 15) // 16 * 16
    chunk = rows // 2
    bf16, f32 = jnp.bfloat16, jnp.float32
    dma = pltpu.SemaphoreType.DMA
    vmem = pl.BlockSpec(memory_space=pltpu.VMEM)
    anywhere = pl.BlockSpec(memory_space=pl.ANY)
    return pl.pallas_call(
        functools.partial(fused_kernel, n_sp, n_tp, cap),
        out_shape=jax.ShapeDtypeStruct((rows, cols), bf16),
        in_specs=[vmem] * 9 + [anywhere] * 4,
        out_specs=vmem,
        scratch_shapes=[
            pltpu.VMEM((width, cols), bf16),
            pltpu.VMEM((width, units), bf16),
            pltpu.VMEM((width, units), bf16),
            pltpu.VMEM((units, width), bf16),
            pltpu.VMEM((taps, cols), f32),
            pltpu.VMEM((pad + rows, cols), f32),
            pltpu.VMEM((pad + rows, 128), f32),
            pltpu.VMEM((max(rows, 2 * cap), 128), f32),
            pltpu.VMEM((rows, cols), f32),
            pltpu.VMEM((pad, cols), bf16),
            pltpu.VMEM((pad, 128), f32),
            pltpu.VMEM((pad, cols), bf16),
            pltpu.VMEM((pad, 128), f32),
            pltpu.VMEM((2, 2, n_tp, 8, chunk), f32),
            pltpu.VMEM((n_sp, 8, rows), f32),
            pltpu.VMEM((n_sp, 8, rows), f32),
            pltpu.VMEM((rows, width), bf16),
            pltpu.VMEM((rows, cols), f32),
            pltpu.VMEM((rows, cols), bf16),
            pltpu.VMEM((n_sp * rows, width), bf16),
            pltpu.VMEM((planes, 2 * cap, rows), bf16),
            pltpu.VMEM((planes, 2 * cap, rows), bf16),
            pltpu.VMEM((2 * cap, width), bf16),
            pltpu.VMEM((2 * cap, units), bf16),
            pltpu.VMEM((planes, 2 * cap, width), bf16),
            pltpu.VMEM((planes, cap, width), bf16),
            pltpu.VMEM((planes, rows, width), bf16),
            pltpu.VMEM((planes, 4, rows, cols), bf16),
            pltpu.VMEM((planes, rows, cols), bf16),
            pltpu.VMEM((planes, rows, cols), bf16),
            dma((4,)),
            dma((2,)),
            dma((2,)),
            dma((2, 2, n_tp)),
            dma((2, 2, n_tp)),
            dma((n_sp,)),
            dma((n_sp,)),
            dma((n_sp,)),
            dma((n_sp,)),
            dma((2, 4)),
            dma((2, 4)),
            dma((planes, 2)),
            dma((planes, 2)),
            dma((planes, 2, 4)),
            dma((planes, 2, 4)),
            dma((planes, 2)),
            dma((planes, 2)),
            dma((planes,)),
            dma((planes,)),
            dma((planes, 6)),
            dma((planes, 6)),
            dma((planes, 2)),
            dma((planes, 2)),
        ],
        compiler_params=pltpu.CompilerParams(
            collective_id=0, has_side_effects=True, vmem_limit_bytes=56 << 20
        ),
    )(*operands)


def per_device(
    residual_in,
    conv_value,
    conv_gate,
    doc_ids,
    conv_kernel,
    ln_gain,
    out_weight,
    norm_gain,
    routes,
    route_weight,
    gate_w,
    up_w,
    down_w,
):
    rows, cols = residual_in.shape
    n_sp = lax.axis_size("sp")
    n_tp = lax.axis_size("tp")
    cap = 4 * rows // n_sp
    _, width, units = gate_w.shape
    group_rows = n_sp // groups * cap
    taps = conv_kernel.shape[0]
    pad = (taps - 1 + 15) // 16 * 16
    if n_tp == 4 and n_sp == 8:
        operands = (
            residual_in,
            conv_value,
            conv_gate,
            doc_ids.reshape(1, rows),
            conv_kernel,
            ln_gain.reshape(cols // 128, 128),
            norm_gain.reshape(cols // 128, 128),
            routes.T,
            route_weight.T,
            out_weight,
            gate_w[0],
            up_w[0],
            down_w[0],
        )
        return fused(operands, rows, cols, n_sp, n_tp, cap, width, units, taps)
    bf16, f32 = jnp.bfloat16, jnp.float32
    dma = pltpu.SemaphoreType.DMA
    vmem = pl.BlockSpec(memory_space=pltpu.VMEM)
    anywhere = pl.BlockSpec(memory_space=pl.ANY)
    return pl.pallas_call(
        functools.partial(layer_kernel, n_sp, n_tp, cap),
        out_shape=jax.ShapeDtypeStruct((rows, cols), bf16),
        in_specs=[vmem] * 9 + [anywhere] * 4,
        out_specs=vmem,
        scratch_shapes=[
            pltpu.VMEM((width, cols), bf16),
            pltpu.VMEM((width, units), bf16),
            pltpu.VMEM((width, units), bf16),
            pltpu.VMEM((units, width), bf16),
            pltpu.VMEM((taps, cols), f32),
            pltpu.VMEM((pad + rows, cols), f32),
            pltpu.VMEM((pad + rows, 128), f32),
            pltpu.VMEM((rows, 128), f32),
            pltpu.VMEM((rows, cols), f32),
            pltpu.VMEM((pad, cols), bf16),
            pltpu.VMEM((pad, 128), f32),
            pltpu.VMEM((pad, cols), bf16),
            pltpu.VMEM((pad, 128), f32),
            pltpu.VMEM((2, n_tp, 8, rows), f32),
            pltpu.VMEM((rows, width), bf16),
            pltpu.VMEM((rows, cols), f32),
            pltpu.VMEM((rows, cols), bf16),
            pltpu.VMEM((rows, cols), bf16),
            pltpu.VMEM((n_sp, rows, cap), bf16),
            pltpu.VMEM((n_sp, cap, cols), bf16),
            pltpu.VMEM((n_sp * cap, width), bf16),
            pltpu.VMEM((group_rows, units), bf16),
            pltpu.VMEM((groups, group_rows, width), bf16),
            pltpu.VMEM((groups, n_tp, group_rows, cols), bf16),
            pltpu.VMEM((groups, group_rows, cols), bf16),
            pltpu.VMEM((n_sp, cap, cols), bf16),
            pltpu.VMEM((n_sp, rows, cap), bf16),
            pltpu.VMEM((n_sp, rows, cap), bf16),
            dma((4,)),
            dma((2,)),
            dma((2,)),
            dma((2, n_tp)),
            dma((2, n_tp)),
            dma((n_tp,)),
            dma((n_tp,)),
            dma((n_sp,)),
            dma((n_sp,)),
            dma((groups, n_tp)),
            dma((groups, n_tp)),
            dma((groups, n_tp + 2)),
            dma((groups, n_tp + 2)),
            dma((n_sp,)),
            dma((n_sp,)),
        ],
        compiler_params=pltpu.CompilerParams(
            collective_id=0, has_side_effects=True, vmem_limit_bytes=54 << 20
        ),
    )(
        residual_in,
        conv_value,
        conv_gate,
        doc_ids.reshape(1, rows),
        conv_kernel,
        ln_gain.reshape(1, cols),
        norm_gain.reshape(1, cols),
        routes,
        route_weight,
        out_weight,
        gate_w[0],
        up_w[0],
        down_w[0],
    )


def solution(mesh):
    in_specs = (
        P("sp", "tp"),
        P("sp", "tp"),
        P("sp", "tp"),
        P("sp"),
        P(None, "tp"),
        P("tp"),
        P(None, "tp"),
        P("tp"),
        P("sp", None),
        P("sp", None),
        P("sp", None, "tp"),
        P("sp", None, "tp"),
        P("sp", "tp", None),
    )
    out_specs = P("sp", "tp")
    return jax.shard_map(
        per_device, mesh=mesh, in_specs=in_specs, out_specs=out_specs, check_vma=False
    )
```

```python
import functools

import jax
import jax.numpy as jnp
from jax import lax
from jax.experimental import pallas as pl
from jax.experimental.pallas import tpu as pltpu
from jax.sharding import PartitionSpec as P

epsilon = 1e-06
groups = 4


def transposed_dot(a, b):
    return lax.dot_general(a, b, (((0,), (0,)), ((), ())), preferred_element_type=jnp.float32)


def remote(src, dst, send_sem, recv_sem, sp, tp):
    return pltpu.make_async_remote_copy(
        src_ref=src,
        dst_ref=dst,
        send_sem=send_sem,
        recv_sem=recv_sem,
        device_id=(sp, tp),
        device_id_type=pl.DeviceIdType.MESH,
    )


def layer_kernel(
    n_sp,
    n_tp,
    cap,
    residual,
    conv_value,
    conv_gate,
    docs,
    conv_kernel,
    ln_gain,
    norm_gain,
    routes,
    route_weight,
    proj_hbm,
    gate_hbm,
    up_hbm,
    down_hbm,
    mixed,
    proj,
    gate,
    up,
    down,
    taps,
    extended,
    doc_extended,
    since,
    conv,
    tail,
    tail_docs,
    halo,
    halo_docs,
    stats,
    activated,
    projected,
    stream,
    normed,
    chosen,
    outbound,
    slots,
    hidden,
    partial,
    arrived,
    summed,
    returned,
    weight_hi,
    weight_lo,
    local_sem,
    halo_send,
    halo_recv,
    stat_send,
    stat_recv,
    act_send,
    act_recv,
    out_send,
    out_recv,
    spread_send,
    spread_recv,
    sum_send,
    sum_recv,
    back_send,
    back_recv,
):
    sp = lax.axis_index("sp")
    tp = lax.axis_index("tp")
    rows, cols = residual.shape
    width = cols * n_tp
    lookback = conv_kernel.shape[0] - 1
    pad = tail.shape[0]
    per_group = n_sp // groups
    group_rows = per_group * cap
    my_group = sp // per_group
    my_member = sp % per_group
    relays = n_tp == 4
    across_x = tp + 1 - 2 * (tp % 2)
    across_y = (tp + 2) % n_tp
    diagonal = (across_x + 2) % n_tp
    loads = [
        pltpu.make_async_copy(src, dst, local_sem.at[i])
        for i, (src, dst) in enumerate(
            ((proj_hbm, proj), (gate_hbm, gate), (up_hbm, up), (down_hbm, down))
        )
    ]
    for load in loads:
        load.start()

    barrier = pltpu.get_barrier_semaphore()
    for i in range(1, n_sp):
        pl.semaphore_signal(
            barrier, inc=1, device_id=((sp + i) % n_sp, tp), device_id_type=pl.DeviceIdType.MESH
        )
    for i in range(1, n_tp):
        pl.semaphore_signal(
            barrier, inc=1, device_id=(sp, (tp + i) % n_tp), device_id_type=pl.DeviceIdType.MESH
        )
    sends = []

    def go(*args):
        send = remote(*args)
        send.start()
        sends.append(send)

    def landed(ref, sem):
        remote(ref, ref, act_send.at[0], sem, sp, tp).wait_recv()

    def col_block(t):
        return pl.ds(pl.multiple_of(t * cols, 128), cols)

    def spread_start(ref, start, size, ss, rs):
        block = ref.at[pl.ds(start, size), col_block(tp)]
        if relays:
            go(block, block, ss(1), rs(1), sp, across_x)
            go(block, block, ss(2), rs(2), sp, across_y)
        else:
            for j in range(1, n_tp):
                go(block, block, ss(j), rs(j), sp, (tp + j) % n_tp)

    def spread_relay(ref, start, size, ss, rs):
        if relays:
            half = size // 2
            landed(ref.at[pl.ds(start, size), col_block(across_x)], rs(1))
            block = ref.at[pl.ds(start, half), col_block(across_x)]
            go(block, block, ss(3), rs(3), sp, across_y)
            landed(ref.at[pl.ds(start, size), col_block(across_y)], rs(2))
            block = ref.at[pl.ds(start + half, half), col_block(across_y)]
            go(block, block, ss(0), rs(0), sp, across_x)

    def spread_finish(ref, start, size, rs):
        if relays:
            half = size // 2
            landed(ref.at[pl.ds(start, half), col_block(diagonal)], rs(3))
            landed(ref.at[pl.ds(start + half, half), col_block(diagonal)], rs(0))
        else:
            for j in range(1, n_tp):
                landed(
                    ref.at[pl.ds(start, size), col_block((tp - j + n_tp) % n_tp)], rs(j)
                )

    def stats_start(i, first, second):
        lane = lax.broadcasted_iota(jnp.int32, (rows, 128), 1)
        both = jnp.where(lane == 0, first, jnp.where(lane == 1, second, 0.0))
        stats[i, 0] = jnp.transpose(both)[0:8]
        for j in range(1, n_tp):
            go(
                stats.at[i, 0],
                stats.at[i, j],
                stat_send.at[i, j],
                stat_recv.at[i, j],
                sp,
                (tp + j) % n_tp,
            )

    def stats_finish(i):
        total = stats[i, 0]
        for j in range(1, n_tp):
            landed(stats.at[i, j], stat_recv.at[i, j])
            total = total + stats[i, j]
        back = jnp.transpose(jnp.concatenate([total] * 16, 0))
        return back[:, 0:1], back[:, 1:2]

    gated = (
        conv_value[...].astype(jnp.float32) * jax.nn.sigmoid(conv_gate[...].astype(jnp.float32))
    ).astype(jnp.bfloat16)
    extended[pl.ds(pad, rows), :] = gated.astype(jnp.float32)
    tail[...] = gated[rows - pad :]
    doc_rows = jnp.transpose(
        jnp.broadcast_to(docs[...].astype(jnp.float32), (128, rows))
    )
    doc_extended[pl.ds(pad, rows), :] = doc_rows
    tail_docs[...] = doc_rows[rows - pad :]
    taps[...] = conv_kernel[...].astype(jnp.float32)
    pl.semaphore_wait(barrier, n_sp - 1 + n_tp - 1)
    next_sp = (sp + 1) % n_sp
    tails = [
        remote(tail, halo, halo_send.at[0], halo_recv.at[0], next_sp, tp),
        remote(tail_docs, halo_docs, halo_send.at[1], halo_recv.at[1], next_sp, tp),
    ]
    for send in tails:
        send.start()
        sends.append(send)

    part = min(64, rows)

    def convolve(r):
        here = pl.ds(r * part, part)
        own = doc_extended[pl.ds(pad + r * part, part), :]
        count = jnp.zeros((part, 128), jnp.float32)
        for back in range(1, lookback + 1):
            count = count + jnp.where(
                doc_extended[pl.ds(pad + r * part - back, part), :] == own, 1.0, 0.0
            )
        since[here, :] = count

        @pl.loop(0, cols // 128)
        def _(c):
            at = pl.ds(pl.multiple_of(c * 128, 128), 128)
            reach = since[here, :]
            total = jnp.zeros((part, 128), jnp.float32)
            for tap in range(lookback + 1):
                value = extended[pl.ds(pad - lookback + r * part + tap, part), at]
                total = total + jnp.where(
                    reach >= lookback - tap, value * taps[tap : tap + 1, at], 0.0
                )
            conv[here, at] = total

    for r in range(1, rows // part):
        convolve(r)
    landed(halo, halo_recv.at[0])
    landed(halo_docs, halo_recv.at[1])
    inside = sp > 0
    extended[pl.ds(0, pad), :] = jnp.where(inside, halo[...].astype(jnp.float32), 0.0)
    doc_extended[pl.ds(0, pad), :] = jnp.where(inside, halo_docs[...], -1.0)
    convolve(0)
    conv_out = conv[...]
    stats_start(
        0,
        jnp.sum(conv_out, 1, keepdims=True),
        jnp.sum(conv_out * conv_out, 1, keepdims=True),
    )

    expert_id = lax.broadcasted_iota(jnp.int32, (rows, n_sp), 1)
    first = routes[:, 0:1] == expert_id
    second = routes[:, 1:2] == expert_id
    named = jnp.where(first | second, 1.0, 0.0)
    earlier = jnp.where(
        lax.broadcasted_iota(jnp.int32, (rows, rows), 1)
        < lax.broadcasted_iota(jnp.int32, (rows, rows), 0),
        1.0,
        0.0,
    ).astype(jnp.bfloat16)
    rank = jnp.dot(earlier, named.astype(jnp.bfloat16), preferred_element_type=jnp.float32)
    slot = jnp.where(first | second, rank, -1.0).astype(jnp.int32)
    weight = jnp.where(first, route_weight[:, 0:1], 0.0) + jnp.where(
        second, route_weight[:, 1:2], 0.0
    )
    slot_id = lax.broadcasted_iota(jnp.int32, (rows, cap), 1)
    for e in range(n_sp):
        chosen[e] = jnp.where(slot[:, e : e + 1] == slot_id, 1.0, 0.0).astype(jnp.bfloat16)

    channel_sum, channel_sq = stats_finish(0)
    mean = channel_sum / width
    scale = lax.rsqrt(channel_sq / width - mean * mean + epsilon)
    v = (conv[...] - mean) * scale * ln_gain[...].astype(jnp.float32)
    activated[:, col_block(tp)] = (v * jax.nn.sigmoid(v)).astype(jnp.bfloat16)

    def act_block(i):
        return act_send.at[i]

    def act_arrival(i):
        return act_recv.at[i]

    spread_start(activated, 0, rows, act_block, act_arrival)
    loads[0].wait()

    def project(t):
        return jnp.dot(
            activated[:, col_block(t)],
            proj[pl.ds(pl.multiple_of(t * cols, 128), cols), :],
            preferred_element_type=jnp.float32,
        )

    projected[...] = project(tp)
    for e in range(n_sp):
        at = jnp.where(slot[:, e : e + 1] == slot_id, weight[:, e : e + 1], 0.0)
        hi = at.astype(jnp.bfloat16)
        weight_hi[e] = hi
        weight_lo[e] = (at - hi.astype(jnp.float32)).astype(jnp.bfloat16)
    spread_relay(activated, 0, rows, act_block, act_arrival)
    if relays:
        projected[...] += project(across_x) + project(across_y)
    spread_finish(activated, 0, rows, act_arrival)
    if relays:
        projected[...] += project(diagonal)
    else:
        for j in range(1, n_tp):
            projected[...] += project((tp + j) % n_tp)
    stream[...] = (
        residual[...].astype(jnp.float32)
        + projected[...].astype(jnp.bfloat16).astype(jnp.float32)
    ).astype(jnp.bfloat16)
    stream_part = stream[...].astype(jnp.float32)
    square = jnp.sum(stream_part * stream_part, 1, keepdims=True)
    stats_start(1, square, square)
    row_total, _ = stats_finish(1)
    normed[...] = (
        stream[...].astype(jnp.float32)
        * lax.rsqrt(row_total / width + epsilon)
        * norm_gain[...].astype(jnp.float32)
    ).astype(jnp.bfloat16)

    def source_rows(s):
        return pl.ds(pl.multiple_of(s * cap, cap), cap)

    def group_start(k):
        return pl.multiple_of((my_group + k) % groups * group_rows, group_rows)

    for k in range(groups):
        for j in range(per_group):
            dest = (my_group - k + groups) % groups * per_group + (my_member + j) % per_group
            rows_out = transposed_dot(chosen[dest], normed[...]).astype(jnp.bfloat16)
            if k == 0 and j == 0:
                slots[source_rows(sp), col_block(tp)] = rows_out
                continue
            outbound[dest] = rows_out
            go(
                outbound.at[dest],
                slots.at[source_rows(sp), col_block(tp)],
                out_send.at[k * per_group + j],
                out_recv.at[sp],
                dest,
                tp,
            )

    def spread_sems(sems, k):
        return lambda i: sems.at[k, i]

    def spread(k):
        for j in range(per_group):
            if k == 0 and j == 0:
                continue
            source = (my_group + k) % groups * per_group + (my_member + j) % per_group
            landed(slots.at[source_rows(source), col_block(tp)], out_recv.at[source])
        spread_start(
            slots, group_start(k), group_rows, spread_sems(spread_send, k), spread_sems(spread_recv, k)
        )

    def relay(k):
        spread_relay(
            slots, group_start(k), group_rows, spread_sems(spread_send, k), spread_sems(spread_recv, k)
        )

    half = group_rows // 2
    low, high = pl.ds(0, half), pl.ds(half, half)

    def compute(k):
        spread_finish(slots, group_start(k), group_rows, spread_sems(spread_recv, k))
        x = pl.ds(group_start(k), group_rows)
        units = gate.shape[1]
        tile = min(256, units)

        @pl.loop(0, units // tile)
        def _(n):
            at = pl.ds(pl.multiple_of(n * tile, tile), tile)
            g = jnp.dot(slots[x, :], gate[:, at], preferred_element_type=jnp.float32)
            u = jnp.dot(slots[x, :], up[:, at], preferred_element_type=jnp.float32)
            hidden[:, at] = (g * jax.nn.sigmoid(g) * u).astype(jnp.bfloat16)

        @pl.loop(0, width // 256)
        def _(n):
            at = pl.ds(pl.multiple_of(n * 256, 256), 256)
            partial[k, :, at] = jnp.dot(
                hidden[...], down[:, at], preferred_element_type=jnp.float32
            ).astype(jnp.bfloat16)

        if relays:
            for i, (part_rows, block, peer) in enumerate(
                (
                    (low, across_x, across_x),
                    (low, diagonal, across_x),
                    (high, across_y, across_y),
                    (high, diagonal, across_y),
                )
            ):
                go(
                    partial.at[k, part_rows, col_block(block)],
                    arrived.at[k, i, low],
                    sum_send.at[k, i],
                    sum_recv.at[k, i],
                    sp,
                    peer,
                )
        else:
            for j in range(1, n_tp):
                peer = (tp + j) % n_tp
                go(
                    partial.at[k, :, col_block(peer)],
                    arrived.at[k, j],
                    sum_send.at[k, j],
                    sum_recv.at[k, j],
                    sp,
                    peer,
                )

    def pass_on(k):
        if relays:
            for i, (part_rows, peer) in enumerate(((low, across_y), (high, across_x))):
                landed(arrived.at[k, 2 * i + 1, low], sum_recv.at[k, 2 * i + 1])
                arrived[k, 2 + i, high] = (
                    partial[k, part_rows, col_block(peer)].astype(jnp.float32)
                    + arrived[k, 2 * i + 1, low].astype(jnp.float32)
                ).astype(jnp.bfloat16)
                go(
                    arrived.at[k, 2 + i, high],
                    arrived.at[k, i, high],
                    sum_send.at[k, 4 + i],
                    sum_recv.at[k, 4 + i],
                    sp,
                    peer,
                )

    def give_back(k):
        if relays:
            for i, part_rows in enumerate((low, high)):
                landed(arrived.at[k, 2 * i, low], sum_recv.at[k, 2 * i])
                landed(arrived.at[k, i, high], sum_recv.at[k, 4 + i])
                summed[k, part_rows] = (
                    partial[k, part_rows, col_block(tp)].astype(jnp.float32)
                    + arrived[k, 2 * i, low].astype(jnp.float32)
                    + arrived[k, i, high].astype(jnp.float32)
                ).astype(jnp.bfloat16)
        else:
            total = partial[k, :, col_block(tp)].astype(jnp.float32)
            for j in range(1, n_tp):
                landed(arrived.at[k, j], sum_recv.at[k, j])
                total = total + arrived[k, j].astype(jnp.float32)
            summed[k] = total.astype(jnp.bfloat16)
        for j in range(per_group):
            member = (my_member + j) % per_group
            source = (my_group + k) % groups * per_group + member
            part = pl.ds(pl.multiple_of(member * cap, cap), cap)
            if k == 0 and j == 0:
                returned[sp] = summed[k, part, :]
                continue
            go(
                summed.at[k, part, :],
                returned.at[sp],
                back_send.at[k * per_group + j],
                back_recv.at[sp],
                source,
                tp,
            )

    spread(0)
    spread(1)
    relay(0)
    spread(2)
    relay(1)
    for load in loads[1:]:
        load.wait()
    compute(0)
    spread(3)
    relay(2)
    compute(1)
    pass_on(0)
    relay(3)
    compute(2)
    pass_on(1)
    give_back(0)
    compute(3)
    pass_on(2)
    give_back(1)
    pass_on(3)
    give_back(2)
    give_back(3)
    for i in range(1, n_sp):
        e = (sp + i) % n_sp
        landed(returned.at[e], back_recv.at[e])
    routed = jnp.zeros((rows, cols), jnp.float32)
    for e in range(n_sp):
        routed = routed + jnp.dot(weight_hi[e], returned[e], preferred_element_type=jnp.float32)
        routed = routed + jnp.dot(weight_lo[e], returned[e], preferred_element_type=jnp.float32)
    mixed[...] = (stream[...].astype(jnp.float32) + routed).astype(jnp.bfloat16)
    for send in sends:
        send.wait_send()


schedule = (
    "R01", "R00", "H",
    "S11", "S10",
    "F01", "F00",
    "R11", "S21", "R10", "S20", "L",
    "G0", "U00", "U01",
    "F11", "F10", "R21", "S31",
    "D00", "D01", "R20", "S30",
    "G1", "U10", "U11", "F21", "F20", "D10", "D11",
    "R31", "R30", "C1",
    "G2", "U20", "U21", "F31", "F30", "D20", "D21",
    "P1", "C2",
    "G3", "U30", "U31", "V1", "D30", "D31",
    "P2", "C3", "V2", "C0", "P3", "P0", "V3", "V0",
)


def fused_kernel(
    n_sp,
    n_tp,
    cap,
    residual,
    conv_value,
    conv_gate,
    docs,
    conv_kernel,
    ln_gain,
    norm_gain,
    routes,
    route_weight,
    proj_hbm,
    gate_hbm,
    up_hbm,
    down_hbm,
    mixed,
    proj,
    gate,
    up,
    down,
    taps,
    extended,
    doc_extended,
    since,
    conv,
    tail,
    tail_docs,
    halo,
    halo_docs,
    stats,
    plans,
    scales,
    activated,
    projected,
    stream,
    tokens,
    picks,
    blends,
    slots,
    hidden,
    pairs,
    outbound,
    blended,
    arrived,
    summed,
    returned,
    local_sem,
    halo_send,
    halo_recv,
    stat_send,
    stat_recv,
    plan_send,
    plan_recv,
    scale_send,
    scale_recv,
    act_send,
    act_recv,
    plane_send,
    plane_recv,
    spread_send,
    spread_recv,
    twin_send,
    twin_recv,
    swap_send,
    swap_recv,
    sum_send,
    sum_recv,
    back_send,
    back_recv,
):
    sp = lax.axis_index("sp")
    tp = lax.axis_index("tp")
    rows, cols = residual.shape
    width = cols * n_tp
    lookback = conv_kernel.shape[0] - 1
    pad = tail.shape[0]
    planes = n_sp // 2
    plane = sp // 2
    core = sp % 2
    twin = plane * 2 + 1 - core
    chunk = rows // 2
    half = chunk // 2
    across_x = tp + 1 - 2 * (tp % 2)
    across_y = (tp + 2) % n_tp
    diagonal = (across_x + 2) % n_tp
    loads = [
        pltpu.make_async_copy(src, dst, local_sem.at[i])
        for i, (src, dst) in enumerate(
            ((proj_hbm, proj), (gate_hbm, gate), (up_hbm, up), (down_hbm, down))
        )
    ]
    for load in loads:
        load.start()

    barrier = pltpu.get_barrier_semaphore()
    for i in range(1, n_sp):
        pl.semaphore_signal(
            barrier, inc=1, device_id=((sp + i) % n_sp, tp), device_id_type=pl.DeviceIdType.MESH
        )
    for i in range(1, n_tp):
        pl.semaphore_signal(
            barrier, inc=1, device_id=(sp, (tp + i) % n_tp), device_id_type=pl.DeviceIdType.MESH
        )
    sends = []

    def go(*args):
        send = remote(*args)
        send.start()
        sends.append(send)

    def landed(ref, sem):
        remote(ref, ref, act_send.at[0, 0], sem, sp, tp).wait_recv()

    def col_block(t):
        return pl.ds(pl.multiple_of(t * cols, 128), cols)

    def row_block(start, size):
        return pl.ds(pl.multiple_of(start, size), size)

    def spread_start(ref, start, ss, rs):
        block = ref.at[row_block(start, chunk), col_block(tp)]
        go(block, block, ss(1), rs(1), sp, across_x)
        go(block, block, ss(2), rs(2), sp, across_y)

    def spread_relay(ref, start, ss, rs):
        landed(ref.at[row_block(start, chunk), col_block(across_x)], rs(1))
        block = ref.at[row_block(start, half), col_block(across_x)]
        go(block, block, ss(3), rs(3), sp, across_y)
        landed(ref.at[row_block(start, chunk), col_block(across_y)], rs(2))
        block = ref.at[row_block(start + half, half), col_block(across_y)]
        go(block, block, ss(0), rs(0), sp, across_x)

    def spread_finish(ref, start, rs):
        landed(ref.at[row_block(start, half), col_block(diagonal)], rs(3))
        landed(ref.at[row_block(start + half, half), col_block(diagonal)], rs(0))

    def stats_start(i, q, first, second):
        lane = lax.broadcasted_iota(jnp.int32, (chunk, 128), 1)
        both = jnp.where(lane == 0, first, jnp.where(lane == 1, second, 0.0))
        stats[i, q, 0] = jnp.transpose(both)[0:8]
        for j in range(1, n_tp):
            go(
                stats.at[i, q, 0],
                stats.at[i, q, j],
                stat_send.at[i, q, j],
                stat_recv.at[i, q, j],
                sp,
                (tp + j) % n_tp,
            )

    def stats_total(i, q):
        total = stats[i, q, 0]
        for j in range(1, n_tp):
            landed(stats.at[i, q, j], stat_recv.at[i, q, j])
            total = total + stats[i, q, j]
        return total

    def gain_row(ref):
        return jnp.concatenate(
            [ref[i : i + 1, :].astype(jnp.float32) for i in range(cols // 128)], 1
        )

    gated = (
        conv_value[...].astype(jnp.float32) * jax.nn.sigmoid(conv_gate[...].astype(jnp.float32))
    ).astype(jnp.bfloat16)
    extended[pl.ds(pad, rows), :] = gated.astype(jnp.float32)
    tail[...] = gated[rows - pad :]
    doc_rows = jnp.transpose(jnp.broadcast_to(docs[...].astype(jnp.float32), (128, rows)))
    doc_extended[pl.ds(pad, rows), :] = doc_rows
    tail_docs[...] = doc_rows[rows - pad :]
    taps[...] = conv_kernel[...].astype(jnp.float32)
    plans[sp] = jnp.concatenate(
        [routes[...].astype(jnp.float32), route_weight[...], jnp.zeros((4, rows), jnp.float32)], 0
    )
    pl.semaphore_wait(barrier, n_sp - 1 + n_tp - 1)
    next_sp = (sp + 1) % n_sp
    go(tail, halo, halo_send.at[0], halo_recv.at[0], next_sp, tp)
    go(tail_docs, halo_docs, halo_send.at[1], halo_recv.at[1], next_sp, tp)
    for i in range(1, n_sp):
        go(plans.at[sp], plans.at[sp], plan_send.at[i], plan_recv.at[sp], (sp + i) % n_sp, tp)

    part = min(64, chunk)

    def convolve(r):
        here = pl.ds(r * part, part)
        own = doc_extended[pl.ds(pad + r * part, part), :]
        count = jnp.zeros((part, 128), jnp.float32)
        for back in range(1, lookback + 1):
            count = count + jnp.where(
                doc_extended[pl.ds(pad + r * part - back, part), :] == own, 1.0, 0.0
            )
        since[here, :] = count

        @pl.loop(0, cols // 128)
        def _(c):
            at = pl.ds(pl.multiple_of(c * 128, 128), 128)
            reach = since[here, :]
            total = jnp.zeros((part, 128), jnp.float32)
            for tap in range(lookback + 1):
                value = extended[pl.ds(pad - lookback + r * part + tap, part), at]
                total = total + jnp.where(
                    reach >= lookback - tap, value * taps[tap : tap + 1, at], 0.0
                )
            conv[here, at] = total

    def channel_stats(q):
        conv_out = conv[pl.ds(q * chunk, chunk), :]
        stats_start(
            0,
            q,
            jnp.sum(conv_out, 1, keepdims=True),
            jnp.sum(conv_out * conv_out, 1, keepdims=True),
        )

    def sems(ref, *index):
        return lambda i: ref.at[(*index, i)]

    def activate(q):
        here = pl.ds(q * chunk, chunk)
        back = jnp.transpose(jnp.concatenate([stats_total(0, q)] * 16, 0))
        mean = back[:, 0:1] / width
        scale = lax.rsqrt(back[:, 1:2] / width - mean * mean + epsilon)
        v = (conv[here, :] - mean) * scale * gain_row(ln_gain)
        activated[here, col_block(tp)] = (v * jax.nn.sigmoid(v)).astype(jnp.bfloat16)
        spread_start(activated, q * chunk, sems(act_send, q), sems(act_recv, q))

    def project(q, t):
        return jnp.dot(
            activated[pl.ds(q * chunk, chunk), col_block(t)],
            proj[col_block(t), :],
            preferred_element_type=jnp.float32,
        )

    parts = chunk // part
    for r in range(parts, 2 * parts):
        convolve(r)
    channel_stats(1)
    for r in range(1, parts):
        convolve(r)
    landed(halo, halo_recv.at[0])
    landed(halo_docs, halo_recv.at[1])
    inside = sp > 0
    extended[pl.ds(0, pad), :] = jnp.where(inside, halo[...].astype(jnp.float32), 0.0)
    doc_extended[pl.ds(0, pad), :] = jnp.where(inside, halo_docs[...], -1.0)
    convolve(0)
    channel_stats(0)
    activate(1)
    activate(0)

    for i in range(1, n_sp):
        e = (sp + i) % n_sp
        landed(plans.at[e], plan_recv.at[e])
    token = lax.broadcasted_iota(jnp.int32, (rows, rows), 0)
    later = jnp.where(
        token < lax.broadcasted_iota(jnp.int32, (rows, rows), 1), 1.0, 0.0
    ).astype(jnp.bfloat16)
    slot_id = lax.broadcasted_iota(jnp.int32, (cap, rows), 0)

    def named_by(s, expert):
        plan = plans[s]
        first = plan[0:1] == expert
        second = plan[1:2] == expert
        weight = jnp.where(first, plan[2:3], 0.0) + jnp.where(second, plan[3:4], 0.0)
        return jnp.where(first | second, 1.0, 0.0), weight

    def slots_of(sources, expert):
        both = [named_by(s, expert) for s in sources]
        named = jnp.concatenate([n for n, _ in both] + [jnp.zeros_like(both[0][0])] * (8 - len(both)), 0)
        rank = jnp.dot(named.astype(jnp.bfloat16), later, preferred_element_type=jnp.float32)
        slot = jnp.where(named > 0.5, rank, -1.0).astype(jnp.int32)
        return [(slot[i : i + 1], weight) for i, (_, weight) in enumerate(both)]

    mine = slots_of([2 * p + core for p in range(planes)], sp.astype(jnp.float32))
    rest = slots_of([2 * p + 1 - core for p in range(planes)], sp.astype(jnp.float32))
    other = slots_of([2 * p + core for p in range(planes)], twin.astype(jnp.float32))
    for p in range(planes):
        slot, weight = mine[p]
        picks[p, 0:cap] = jnp.where(slot == slot_id, 1.0, 0.0).astype(jnp.bfloat16)
        own_blend = jnp.where(slot == slot_id, weight, 0.0)
        slot, weight = rest[p]
        picks[p, cap : 2 * cap] = jnp.where(slot == slot_id, 1.0, 0.0).astype(jnp.bfloat16)
        slot, weight = other[p]
        twin_blend = jnp.where(slot == slot_id, weight, 0.0)
        blends[p] = jnp.transpose(jnp.concatenate([own_blend, twin_blend], 0)).astype(jnp.bfloat16)

    order = [0] + sorted(range(1, planes), key=lambda k: -min(k, planes - k))

    plane_order = {
        1: [(order[1], 1)],
        0: [(order[1], 0)] + [(k, q) for k in order[2:] for q in (1, 0)],
    }

    def source(k):
        return (plane + k) % planes * 2 + core

    def first_row(k, q):
        return source(k) * rows + q * chunk

    def residual_rows(q):
        here = pl.ds(q * chunk, chunk)
        spread_relay(activated, q * chunk, sems(act_send, q), sems(act_recv, q))
        projected[here, :] += project(q, across_x) + project(q, across_y)
        spread_finish(activated, q * chunk, sems(act_recv, q))
        total = projected[here, :] + project(q, diagonal)
        stream_rows = (
            residual[here, :].astype(jnp.float32)
            + total.astype(jnp.bfloat16).astype(jnp.float32)
        ).astype(jnp.bfloat16)
        stream[here, :] = stream_rows
        stream_part = stream_rows.astype(jnp.float32)
        tokens[row_block(first_row(0, q), chunk), col_block(tp)] = (
            stream_part * gain_row(norm_gain)
        ).astype(jnp.bfloat16)
        spread_start(tokens, first_row(0, q), sems(spread_send, 0, q), sems(spread_recv, 0, q))
        for k, part_q in plane_order[q]:
            block = tokens.at[row_block(first_row(0, part_q), chunk), col_block(tp)]
            go(
                block,
                block,
                plane_send.at[k, part_q],
                plane_recv.at[k, part_q],
                (plane - k + planes) % planes * 2 + core,
                tp,
            )
        square = jnp.sum(stream_part * stream_part, 1, keepdims=True)
        stats_start(1, q, square, square)

    loads[0].wait()
    for q in (1, 0):
        projected[pl.ds(q * chunk, chunk), :] = project(q, tp)
    residual_rows(1)
    residual_rows(0)

    def spread(k, q):
        block = tokens.at[row_block(first_row(k, q), chunk), col_block(tp)]
        landed(block, plane_recv.at[k, q])
        spread_start(tokens, first_row(k, q), sems(spread_send, k, q), sems(spread_recv, k, q))

    def relay(k, q):
        spread_relay(tokens, first_row(k, q), sems(spread_send, k, q), sems(spread_recv, k, q))

    def finish(k, q):
        spread_finish(tokens, first_row(k, q), sems(spread_recv, k, q))
        block = tokens.at[row_block(first_row(k, q), chunk), :]
        go(block, block, twin_send.at[k, q], twin_recv.at[k, q], twin, tp)

    def share_scales():
        for q in range(2):
            scales[sp, :, pl.ds(q * chunk, chunk)] = lax.rsqrt(
                stats_total(1, q) / width + epsilon
            )
        for i in range(1, n_sp):
            go(
                scales.at[sp],
                scales.at[sp],
                scale_send.at[i],
                scale_recv.at[sp],
                (sp + i) % n_sp,
                tp,
            )

    def gather(k):
        p = (plane + k) % planes
        for q in range(2):
            start = (2 * p + 1 - core) * rows + q * chunk
            landed(tokens.at[row_block(start, chunk), :], twin_recv.at[k, q])
        for j in range(2):
            s = 2 * p + (core if j == 0 else 1 - core)
            if k == 0 and j == 0:
                pass
            else:
                landed(scales.at[s], scale_recv.at[s])
            here = pl.ds(j * cap, cap)
            pick = picks[p, here, :]
            slots[here, :] = jnp.dot(
                pick, tokens[row_block(s * rows, rows), :], preferred_element_type=jnp.float32
            ).astype(jnp.bfloat16)
            scale = jnp.sum(pick.astype(jnp.float32) * scales[s][0:1, :], 1, keepdims=True)
            since[here, :] = jnp.broadcast_to(scale, (cap, 128))

    def raise_up(k, piece):
        size = gate.shape[1] // 2
        at = pl.ds(piece * size, size)
        scale = jnp.concatenate([since[0 : 2 * cap, :]] * (size // 128), 1)
        g = scale * jnp.dot(slots[...], gate[:, at], preferred_element_type=jnp.float32)
        u = scale * jnp.dot(slots[...], up[:, at], preferred_element_type=jnp.float32)
        hidden[:, at] = (g * jax.nn.sigmoid(g) * u).astype(jnp.bfloat16)

    def bring_down(k, piece):
        size = width // 2
        at = pl.ds(piece * size, size)
        result = jnp.dot(
            hidden[...], down[:, at], preferred_element_type=jnp.float32
        ).astype(jnp.bfloat16)
        pairs[k, 0:cap, at] = result[0:cap]
        outbound[k, :, at] = result[cap:]
        if piece == 1:
            go(
                outbound.at[k],
                pairs.at[k, pl.ds(cap, cap), :],
                swap_send.at[k],
                swap_recv.at[k],
                twin,
                tp,
            )

    low, high = pl.ds(0, chunk), pl.ds(chunk, chunk)

    def combine(k):
        p = (plane + k) % planes
        landed(pairs.at[k, pl.ds(cap, cap), :], swap_recv.at[k])

        blended[k] = jnp.dot(
            blends[p], pairs[k], preferred_element_type=jnp.float32
        ).astype(jnp.bfloat16)

        for i, (part_rows, block, peer) in enumerate(
            (
                (low, diagonal, across_x),
                (high, diagonal, across_y),
                (low, across_x, across_x),
                (high, across_y, across_y),
            )
        ):
            go(
                blended.at[k, part_rows, col_block(block)],
                arrived.at[k, i, low],
                sum_send.at[k, i],
                sum_recv.at[k, i],
                sp,
                peer,
            )

    def pass_on(k):
        for i, (part_rows, peer) in enumerate(((low, across_y), (high, across_x))):
            landed(arrived.at[k, i, low], sum_recv.at[k, i])
            arrived[k, 2 + i, high] = (
                blended[k, part_rows, col_block(peer)].astype(jnp.float32)
                + arrived[k, i, low].astype(jnp.float32)
            ).astype(jnp.bfloat16)
            go(
                arrived.at[k, 2 + i, high],
                arrived.at[k, i, high],
                sum_send.at[k, 4 + i],
                sum_recv.at[k, 4 + i],
                sp,
                peer,
            )

    def give_back(k):
        for i, part_rows in enumerate((low, high)):
            landed(arrived.at[k, 2 + i, low], sum_recv.at[k, 2 + i])
            landed(arrived.at[k, i, high], sum_recv.at[k, 4 + i])
            total = (
                blended[k, part_rows, col_block(tp)].astype(jnp.float32)
                + arrived[k, 2 + i, low].astype(jnp.float32)
                + arrived[k, i, high].astype(jnp.float32)
            )
            if k == 0:
                here = pl.ds(i * chunk, chunk)
                total = total + stream[here, :].astype(jnp.float32)
                for j in order[1:]:
                    landed(returned.at[j, part_rows], back_recv.at[j, i])
                    total = total + returned[j, part_rows].astype(jnp.float32)
                mixed[here, :] = total.astype(jnp.bfloat16)
            else:
                summed[k, part_rows] = total.astype(jnp.bfloat16)
                go(
                    summed.at[k, part_rows],
                    returned.at[k, part_rows],
                    back_send.at[k, i],
                    back_recv.at[k, i],
                    source(k),
                    tp,
                )

    def weights_ready():
        for load in loads[1:]:
            load.wait()

    steps = {
        "R": relay,
        "S": spread,
        "F": finish,
        "G": gather,
        "U": raise_up,
        "D": bring_down,
        "C": combine,
        "P": pass_on,
        "V": give_back,
        "H": share_scales,
        "L": weights_ready,
    }
    for word in schedule:
        indices = [int(digit) for digit in word[1:]]
        steps[word[0]](*[order[i] for i in indices[:1]], *indices[1:])
    for send in sends:
        send.wait_send()


def fused(operands, rows, cols, n_sp, n_tp, cap, width, units, taps):
    planes = n_sp // 2
    pad = (taps - 1 + 15) // 16 * 16
    chunk = rows // 2
    bf16, f32 = jnp.bfloat16, jnp.float32
    dma = pltpu.SemaphoreType.DMA
    vmem = pl.BlockSpec(memory_space=pltpu.VMEM)
    anywhere = pl.BlockSpec(memory_space=pl.ANY)
    return pl.pallas_call(
        functools.partial(fused_kernel, n_sp, n_tp, cap),
        out_shape=jax.ShapeDtypeStruct((rows, cols), bf16),
        in_specs=[vmem] * 9 + [anywhere] * 4,
        out_specs=vmem,
        scratch_shapes=[
            pltpu.VMEM((width, cols), bf16),
            pltpu.VMEM((width, units), bf16),
            pltpu.VMEM((width, units), bf16),
            pltpu.VMEM((units, width), bf16),
            pltpu.VMEM((taps, cols), f32),
            pltpu.VMEM((pad + rows, cols), f32),
            pltpu.VMEM((pad + rows, 128), f32),
            pltpu.VMEM((max(rows, 2 * cap), 128), f32),
            pltpu.VMEM((rows, cols), f32),
            pltpu.VMEM((pad, cols), bf16),
            pltpu.VMEM((pad, 128), f32),
            pltpu.VMEM((pad, cols), bf16),
            pltpu.VMEM((pad, 128), f32),
            pltpu.VMEM((2, 2, n_tp, 8, chunk), f32),
            pltpu.VMEM((n_sp, 8, rows), f32),
            pltpu.VMEM((n_sp, 8, rows), f32),
            pltpu.VMEM((rows, width), bf16),
            pltpu.VMEM((rows, cols), f32),
            pltpu.VMEM((rows, cols), bf16),
            pltpu.VMEM((n_sp * rows, width), bf16),
            pltpu.VMEM((planes, 2 * cap, rows), bf16),
            pltpu.VMEM((planes, rows, 2 * cap), bf16),
            pltpu.VMEM((2 * cap, width), bf16),
            pltpu.VMEM((2 * cap, units), bf16),
            pltpu.VMEM((planes, 2 * cap, width), bf16),
            pltpu.VMEM((planes, cap, width), bf16),
            pltpu.VMEM((planes, rows, width), bf16),
            pltpu.VMEM((planes, 4, rows, cols), bf16),
            pltpu.VMEM((planes, rows, cols), bf16),
            pltpu.VMEM((planes, rows, cols), bf16),
            dma((4,)),
            dma((2,)),
            dma((2,)),
            dma((2, 2, n_tp)),
            dma((2, 2, n_tp)),
            dma((n_sp,)),
            dma((n_sp,)),
            dma((n_sp,)),
            dma((n_sp,)),
            dma((2, 4)),
            dma((2, 4)),
            dma((planes, 2)),
            dma((planes, 2)),
            dma((planes, 2, 4)),
            dma((planes, 2, 4)),
            dma((planes, 2)),
            dma((planes, 2)),
            dma((planes,)),
            dma((planes,)),
            dma((planes, 6)),
            dma((planes, 6)),
            dma((planes, 2)),
            dma((planes, 2)),
        ],
        compiler_params=pltpu.CompilerParams(
            collective_id=0, has_side_effects=True, vmem_limit_bytes=56 << 20
        ),
    )(*operands)


def per_device(
    residual_in,
    conv_value,
    conv_gate,
    doc_ids,
    conv_kernel,
    ln_gain,
    out_weight,
    norm_gain,
    routes,
    route_weight,
    gate_w,
    up_w,
    down_w,
):
    rows, cols = residual_in.shape
    n_sp = lax.axis_size("sp")
    n_tp = lax.axis_size("tp")
    cap = 4 * rows // n_sp
    _, width, units = gate_w.shape
    group_rows = n_sp // groups * cap
    taps = conv_kernel.shape[0]
    pad = (taps - 1 + 15) // 16 * 16
    if n_tp == 4 and n_sp == 8:
        operands = (
            residual_in,
            conv_value,
            conv_gate,
            doc_ids.reshape(1, rows),
            conv_kernel,
            ln_gain.reshape(cols // 128, 128),
            norm_gain.reshape(cols // 128, 128),
            routes.T,
            route_weight.T,
            out_weight,
            gate_w[0],
            up_w[0],
            down_w[0],
        )
        return fused(operands, rows, cols, n_sp, n_tp, cap, width, units, taps)
    bf16, f32 = jnp.bfloat16, jnp.float32
    dma = pltpu.SemaphoreType.DMA
    vmem = pl.BlockSpec(memory_space=pltpu.VMEM)
    anywhere = pl.BlockSpec(memory_space=pl.ANY)
    return pl.pallas_call(
        functools.partial(layer_kernel, n_sp, n_tp, cap),
        out_shape=jax.ShapeDtypeStruct((rows, cols), bf16),
        in_specs=[vmem] * 9 + [anywhere] * 4,
        out_specs=vmem,
        scratch_shapes=[
            pltpu.VMEM((width, cols), bf16),
            pltpu.VMEM((width, units), bf16),
            pltpu.VMEM((width, units), bf16),
            pltpu.VMEM((units, width), bf16),
            pltpu.VMEM((taps, cols), f32),
            pltpu.VMEM((pad + rows, cols), f32),
            pltpu.VMEM((pad + rows, 128), f32),
            pltpu.VMEM((rows, 128), f32),
            pltpu.VMEM((rows, cols), f32),
            pltpu.VMEM((pad, cols), bf16),
            pltpu.VMEM((pad, 128), f32),
            pltpu.VMEM((pad, cols), bf16),
            pltpu.VMEM((pad, 128), f32),
            pltpu.VMEM((2, n_tp, 8, rows), f32),
            pltpu.VMEM((rows, width), bf16),
            pltpu.VMEM((rows, cols), f32),
            pltpu.VMEM((rows, cols), bf16),
            pltpu.VMEM((rows, cols), bf16),
            pltpu.VMEM((n_sp, rows, cap), bf16),
            pltpu.VMEM((n_sp, cap, cols), bf16),
            pltpu.VMEM((n_sp * cap, width), bf16),
            pltpu.VMEM((group_rows, units), bf16),
            pltpu.VMEM((groups, group_rows, width), bf16),
            pltpu.VMEM((groups, n_tp, group_rows, cols), bf16),
            pltpu.VMEM((groups, group_rows, cols), bf16),
            pltpu.VMEM((n_sp, cap, cols), bf16),
            pltpu.VMEM((n_sp, rows, cap), bf16),
            pltpu.VMEM((n_sp, rows, cap), bf16),
            dma((4,)),
            dma((2,)),
            dma((2,)),
            dma((2, n_tp)),
            dma((2, n_tp)),
            dma((n_tp,)),
            dma((n_tp,)),
            dma((n_sp,)),
            dma((n_sp,)),
            dma((groups, n_tp)),
            dma((groups, n_tp)),
            dma((groups, n_tp + 2)),
            dma((groups, n_tp + 2)),
            dma((n_sp,)),
            dma((n_sp,)),
        ],
        compiler_params=pltpu.CompilerParams(
            collective_id=0, has_side_effects=True, vmem_limit_bytes=54 << 20
        ),
    )(
        residual_in,
        conv_value,
        conv_gate,
        doc_ids.reshape(1, rows),
        conv_kernel,
        ln_gain.reshape(1, cols),
        norm_gain.reshape(1, cols),
        routes,
        route_weight,
        out_weight,
        gate_w[0],
        up_w[0],
        down_w[0],
    )


def solution(mesh):
    in_specs = (
        P("sp", "tp"),
        P("sp", "tp"),
        P("sp", "tp"),
        P("sp"),
        P(None, "tp"),
        P("tp"),
        P(None, "tp"),
        P("tp"),
        P("sp", None),
        P("sp", None),
        P("sp", None, "tp"),
        P("sp", None, "tp"),
        P("sp", "tp", None),
    )
    out_specs = P("sp", "tp")
    return jax.shard_map(
        per_device, mesh=mesh, in_specs=in_specs, out_specs=out_specs, check_vma=False
    )
```

```python
import functools

import jax
import jax.numpy as jnp
from jax import lax
from jax.experimental import pallas as pl
from jax.experimental.pallas import tpu as pltpu
from jax.sharding import PartitionSpec as P

epsilon = 1e-06
groups = 4


def transposed_dot(a, b):
    return lax.dot_general(a, b, (((0,), (0,)), ((), ())), preferred_element_type=jnp.float32)


def remote(src, dst, send_sem, recv_sem, sp, tp):
    return pltpu.make_async_remote_copy(
        src_ref=src,
        dst_ref=dst,
        send_sem=send_sem,
        recv_sem=recv_sem,
        device_id=(sp, tp),
        device_id_type=pl.DeviceIdType.MESH,
    )


def layer_kernel(
    n_sp,
    n_tp,
    cap,
    residual,
    conv_value,
    conv_gate,
    docs,
    conv_kernel,
    ln_gain,
    norm_gain,
    routes,
    route_weight,
    proj_hbm,
    gate_hbm,
    up_hbm,
    down_hbm,
    mixed,
    proj,
    gate,
    up,
    down,
    taps,
    extended,
    doc_extended,
    since,
    conv,
    tail,
    tail_docs,
    halo,
    halo_docs,
    stats,
    activated,
    projected,
    stream,
    normed,
    chosen,
    outbound,
    slots,
    hidden,
    partial,
    arrived,
    summed,
    returned,
    weight_hi,
    weight_lo,
    local_sem,
    halo_send,
    halo_recv,
    stat_send,
    stat_recv,
    act_send,
    act_recv,
    out_send,
    out_recv,
    spread_send,
    spread_recv,
    sum_send,
    sum_recv,
    back_send,
    back_recv,
):
    sp = lax.axis_index("sp")
    tp = lax.axis_index("tp")
    rows, cols = residual.shape
    width = cols * n_tp
    lookback = conv_kernel.shape[0] - 1
    pad = tail.shape[0]
    per_group = n_sp // groups
    group_rows = per_group * cap
    my_group = sp // per_group
    my_member = sp % per_group
    relays = n_tp == 4
    across_x = tp + 1 - 2 * (tp % 2)
    across_y = (tp + 2) % n_tp
    diagonal = (across_x + 2) % n_tp
    loads = [
        pltpu.make_async_copy(src, dst, local_sem.at[i])
        for i, (src, dst) in enumerate(
            ((proj_hbm, proj), (gate_hbm, gate), (up_hbm, up), (down_hbm, down))
        )
    ]
    for load in loads:
        load.start()

    barrier = pltpu.get_barrier_semaphore()
    for i in range(1, n_sp):
        pl.semaphore_signal(
            barrier, inc=1, device_id=((sp + i) % n_sp, tp), device_id_type=pl.DeviceIdType.MESH
        )
    for i in range(1, n_tp):
        pl.semaphore_signal(
            barrier, inc=1, device_id=(sp, (tp + i) % n_tp), device_id_type=pl.DeviceIdType.MESH
        )
    sends = []

    def go(*args):
        send = remote(*args)
        send.start()
        sends.append(send)

    def landed(ref, sem):
        remote(ref, ref, act_send.at[0], sem, sp, tp).wait_recv()

    def col_block(t):
        return pl.ds(pl.multiple_of(t * cols, 128), cols)

    def spread_start(ref, start, size, ss, rs):
        block = ref.at[pl.ds(start, size), col_block(tp)]
        if relays:
            go(block, block, ss(1), rs(1), sp, across_x)
            go(block, block, ss(2), rs(2), sp, across_y)
        else:
            for j in range(1, n_tp):
                go(block, block, ss(j), rs(j), sp, (tp + j) % n_tp)

    def spread_relay(ref, start, size, ss, rs):
        if relays:
            half = size // 2
            landed(ref.at[pl.ds(start, size), col_block(across_x)], rs(1))
            block = ref.at[pl.ds(start, half), col_block(across_x)]
            go(block, block, ss(3), rs(3), sp, across_y)
            landed(ref.at[pl.ds(start, size), col_block(across_y)], rs(2))
            block = ref.at[pl.ds(start + half, half), col_block(across_y)]
            go(block, block, ss(0), rs(0), sp, across_x)

    def spread_finish(ref, start, size, rs):
        if relays:
            half = size // 2
            landed(ref.at[pl.ds(start, half), col_block(diagonal)], rs(3))
            landed(ref.at[pl.ds(start + half, half), col_block(diagonal)], rs(0))
        else:
            for j in range(1, n_tp):
                landed(
                    ref.at[pl.ds(start, size), col_block((tp - j + n_tp) % n_tp)], rs(j)
                )

    def stats_start(i, first, second):
        lane = lax.broadcasted_iota(jnp.int32, (rows, 128), 1)
        both = jnp.where(lane == 0, first, jnp.where(lane == 1, second, 0.0))
        stats[i, 0] = jnp.transpose(both)[0:8]
        for j in range(1, n_tp):
            go(
                stats.at[i, 0],
                stats.at[i, j],
                stat_send.at[i, j],
                stat_recv.at[i, j],
                sp,
                (tp + j) % n_tp,
            )

    def stats_finish(i):
        total = stats[i, 0]
        for j in range(1, n_tp):
            landed(stats.at[i, j], stat_recv.at[i, j])
            total = total + stats[i, j]
        back = jnp.transpose(jnp.concatenate([total] * 16, 0))
        return back[:, 0:1], back[:, 1:2]

    gated = (
        conv_value[...].astype(jnp.float32) * jax.nn.sigmoid(conv_gate[...].astype(jnp.float32))
    ).astype(jnp.bfloat16)
    extended[pl.ds(pad, rows), :] = gated.astype(jnp.float32)
    tail[...] = gated[rows - pad :]
    doc_rows = jnp.transpose(
        jnp.broadcast_to(docs[...].astype(jnp.float32), (128, rows))
    )
    doc_extended[pl.ds(pad, rows), :] = doc_rows
    tail_docs[...] = doc_rows[rows - pad :]
    taps[...] = conv_kernel[...].astype(jnp.float32)
    pl.semaphore_wait(barrier, n_sp - 1 + n_tp - 1)
    next_sp = (sp + 1) % n_sp
    tails = [
        remote(tail, halo, halo_send.at[0], halo_recv.at[0], next_sp, tp),
        remote(tail_docs, halo_docs, halo_send.at[1], halo_recv.at[1], next_sp, tp),
    ]
    for send in tails:
        send.start()
        sends.append(send)

    part = min(64, rows)

    def convolve(r):
        here = pl.ds(r * part, part)
        own = doc_extended[pl.ds(pad + r * part, part), :]
        count = jnp.zeros((part, 128), jnp.float32)
        for back in range(1, lookback + 1):
            count = count + jnp.where(
                doc_extended[pl.ds(pad + r * part - back, part), :] == own, 1.0, 0.0
            )
        since[here, :] = count

        @pl.loop(0, cols // 128)
        def _(c):
            at = pl.ds(pl.multiple_of(c * 128, 128), 128)
            reach = since[here, :]
            total = jnp.zeros((part, 128), jnp.float32)
            for tap in range(lookback + 1):
                value = extended[pl.ds(pad - lookback + r * part + tap, part), at]
                total = total + jnp.where(
                    reach >= lookback - tap, value * taps[tap : tap + 1, at], 0.0
                )
            conv[here, at] = total

    for r in range(1, rows // part):
        convolve(r)
    landed(halo, halo_recv.at[0])
    landed(halo_docs, halo_recv.at[1])
    inside = sp > 0
    extended[pl.ds(0, pad), :] = jnp.where(inside, halo[...].astype(jnp.float32), 0.0)
    doc_extended[pl.ds(0, pad), :] = jnp.where(inside, halo_docs[...], -1.0)
    convolve(0)
    conv_out = conv[...]
    stats_start(
        0,
        jnp.sum(conv_out, 1, keepdims=True),
        jnp.sum(conv_out * conv_out, 1, keepdims=True),
    )

    expert_id = lax.broadcasted_iota(jnp.int32, (rows, n_sp), 1)
    first = routes[:, 0:1] == expert_id
    second = routes[:, 1:2] == expert_id
    named = jnp.where(first | second, 1.0, 0.0)
    earlier = jnp.where(
        lax.broadcasted_iota(jnp.int32, (rows, rows), 1)
        < lax.broadcasted_iota(jnp.int32, (rows, rows), 0),
        1.0,
        0.0,
    ).astype(jnp.bfloat16)
    rank = jnp.dot(earlier, named.astype(jnp.bfloat16), preferred_element_type=jnp.float32)
    slot = jnp.where(first | second, rank, -1.0).astype(jnp.int32)
    weight = jnp.where(first, route_weight[:, 0:1], 0.0) + jnp.where(
        second, route_weight[:, 1:2], 0.0
    )
    slot_id = lax.broadcasted_iota(jnp.int32, (rows, cap), 1)
    for e in range(n_sp):
        chosen[e] = jnp.where(slot[:, e : e + 1] == slot_id, 1.0, 0.0).astype(jnp.bfloat16)

    channel_sum, channel_sq = stats_finish(0)
    mean = channel_sum / width
    scale = lax.rsqrt(channel_sq / width - mean * mean + epsilon)
    v = (conv[...] - mean) * scale * ln_gain[...].astype(jnp.float32)
    activated[:, col_block(tp)] = (v * jax.nn.sigmoid(v)).astype(jnp.bfloat16)

    def act_block(i):
        return act_send.at[i]

    def act_arrival(i):
        return act_recv.at[i]

    spread_start(activated, 0, rows, act_block, act_arrival)
    loads[0].wait()

    def project(t):
        return jnp.dot(
            activated[:, col_block(t)],
            proj[pl.ds(pl.multiple_of(t * cols, 128), cols), :],
            preferred_element_type=jnp.float32,
        )

    projected[...] = project(tp)
    for e in range(n_sp):
        at = jnp.where(slot[:, e : e + 1] == slot_id, weight[:, e : e + 1], 0.0)
        hi = at.astype(jnp.bfloat16)
        weight_hi[e] = hi
        weight_lo[e] = (at - hi.astype(jnp.float32)).astype(jnp.bfloat16)
    spread_relay(activated, 0, rows, act_block, act_arrival)
    if relays:
        projected[...] += project(across_x) + project(across_y)
    spread_finish(activated, 0, rows, act_arrival)
    if relays:
        projected[...] += project(diagonal)
    else:
        for j in range(1, n_tp):
            projected[...] += project((tp + j) % n_tp)
    stream[...] = (
        residual[...].astype(jnp.float32)
        + projected[...].astype(jnp.bfloat16).astype(jnp.float32)
    ).astype(jnp.bfloat16)
    stream_part = stream[...].astype(jnp.float32)
    square = jnp.sum(stream_part * stream_part, 1, keepdims=True)
    stats_start(1, square, square)
    row_total, _ = stats_finish(1)
    normed[...] = (
        stream[...].astype(jnp.float32)
        * lax.rsqrt(row_total / width + epsilon)
        * norm_gain[...].astype(jnp.float32)
    ).astype(jnp.bfloat16)

    def source_rows(s):
        return pl.ds(pl.multiple_of(s * cap, cap), cap)

    def group_start(k):
        return pl.multiple_of((my_group + k) % groups * group_rows, group_rows)

    for k in range(groups):
        for j in range(per_group):
            dest = (my_group - k + groups) % groups * per_group + (my_member + j) % per_group
            rows_out = transposed_dot(chosen[dest], normed[...]).astype(jnp.bfloat16)
            if k == 0 and j == 0:
                slots[source_rows(sp), col_block(tp)] = rows_out
                continue
            outbound[dest] = rows_out
            go(
                outbound.at[dest],
                slots.at[source_rows(sp), col_block(tp)],
                out_send.at[k * per_group + j],
                out_recv.at[sp],
                dest,
                tp,
            )

    def spread_sems(sems, k):
        return lambda i: sems.at[k, i]

    def spread(k):
        for j in range(per_group):
            if k == 0 and j == 0:
                continue
            source = (my_group + k) % groups * per_group + (my_member + j) % per_group
            landed(slots.at[source_rows(source), col_block(tp)], out_recv.at[source])
        spread_start(
            slots, group_start(k), group_rows, spread_sems(spread_send, k), spread_sems(spread_recv, k)
        )

    def relay(k):
        spread_relay(
            slots, group_start(k), group_rows, spread_sems(spread_send, k), spread_sems(spread_recv, k)
        )

    half = group_rows // 2
    low, high = pl.ds(0, half), pl.ds(half, half)

    def compute(k):
        spread_finish(slots, group_start(k), group_rows, spread_sems(spread_recv, k))
        x = pl.ds(group_start(k), group_rows)
        units = gate.shape[1]
        tile = min(256, units)

        @pl.loop(0, units // tile)
        def _(n):
            at = pl.ds(pl.multiple_of(n * tile, tile), tile)
            g = jnp.dot(slots[x, :], gate[:, at], preferred_element_type=jnp.float32)
            u = jnp.dot(slots[x, :], up[:, at], preferred_element_type=jnp.float32)
            hidden[:, at] = (g * jax.nn.sigmoid(g) * u).astype(jnp.bfloat16)

        @pl.loop(0, width // 256)
        def _(n):
            at = pl.ds(pl.multiple_of(n * 256, 256), 256)
            partial[k, :, at] = jnp.dot(
                hidden[...], down[:, at], preferred_element_type=jnp.float32
            ).astype(jnp.bfloat16)

        if relays:
            for i, (part_rows, block, peer) in enumerate(
                (
                    (low, across_x, across_x),
                    (low, diagonal, across_x),
                    (high, across_y, across_y),
                    (high, diagonal, across_y),
                )
            ):
                go(
                    partial.at[k, part_rows, col_block(block)],
                    arrived.at[k, i, low],
                    sum_send.at[k, i],
                    sum_recv.at[k, i],
                    sp,
                    peer,
                )
        else:
            for j in range(1, n_tp):
                peer = (tp + j) % n_tp
                go(
                    partial.at[k, :, col_block(peer)],
                    arrived.at[k, j],
                    sum_send.at[k, j],
                    sum_recv.at[k, j],
                    sp,
                    peer,
                )

    def pass_on(k):
        if relays:
            for i, (part_rows, peer) in enumerate(((low, across_y), (high, across_x))):
                landed(arrived.at[k, 2 * i + 1, low], sum_recv.at[k, 2 * i + 1])
                arrived[k, 2 + i, high] = (
                    partial[k, part_rows, col_block(peer)].astype(jnp.float32)
                    + arrived[k, 2 * i + 1, low].astype(jnp.float32)
                ).astype(jnp.bfloat16)
                go(
                    arrived.at[k, 2 + i, high],
                    arrived.at[k, i, high],
                    sum_send.at[k, 4 + i],
                    sum_recv.at[k, 4 + i],
                    sp,
                    peer,
                )

    def give_back(k):
        if relays:
            for i, part_rows in enumerate((low, high)):
                landed(arrived.at[k, 2 * i, low], sum_recv.at[k, 2 * i])
                landed(arrived.at[k, i, high], sum_recv.at[k, 4 + i])
                summed[k, part_rows] = (
                    partial[k, part_rows, col_block(tp)].astype(jnp.float32)
                    + arrived[k, 2 * i, low].astype(jnp.float32)
                    + arrived[k, i, high].astype(jnp.float32)
                ).astype(jnp.bfloat16)
        else:
            total = partial[k, :, col_block(tp)].astype(jnp.float32)
            for j in range(1, n_tp):
                landed(arrived.at[k, j], sum_recv.at[k, j])
                total = total + arrived[k, j].astype(jnp.float32)
            summed[k] = total.astype(jnp.bfloat16)
        for j in range(per_group):
            member = (my_member + j) % per_group
            source = (my_group + k) % groups * per_group + member
            part = pl.ds(pl.multiple_of(member * cap, cap), cap)
            if k == 0 and j == 0:
                returned[sp] = summed[k, part, :]
                continue
            go(
                summed.at[k, part, :],
                returned.at[sp],
                back_send.at[k * per_group + j],
                back_recv.at[sp],
                source,
                tp,
            )

    spread(0)
    spread(1)
    relay(0)
    spread(2)
    relay(1)
    for load in loads[1:]:
        load.wait()
    compute(0)
    spread(3)
    relay(2)
    compute(1)
    pass_on(0)
    relay(3)
    compute(2)
    pass_on(1)
    give_back(0)
    compute(3)
    pass_on(2)
    give_back(1)
    pass_on(3)
    give_back(2)
    give_back(3)
    for i in range(1, n_sp):
        e = (sp + i) % n_sp
        landed(returned.at[e], back_recv.at[e])
    routed = jnp.zeros((rows, cols), jnp.float32)
    for e in range(n_sp):
        routed = routed + jnp.dot(weight_hi[e], returned[e], preferred_element_type=jnp.float32)
        routed = routed + jnp.dot(weight_lo[e], returned[e], preferred_element_type=jnp.float32)
    mixed[...] = (stream[...].astype(jnp.float32) + routed).astype(jnp.bfloat16)
    for send in sends:
        send.wait_send()


schedule = (
    "R01", "R00", "H",
    "S11", "S10",
    "F01", "F00",
    "R11", "S21", "R10", "S20", "L",
    "G0", "U00", "U01",
    "F11", "F10", "R21", "S31",
    "D00", "D01", "R20", "S30",
    "G1", "U10", "U11", "F21", "F20", "D10", "D11",
    "R31", "R30", "C1",
    "G2", "U20", "U21", "F31", "F30", "D20", "D21",
    "P1", "C2",
    "G3", "U30", "U31", "V1", "D30", "D31",
    "P2", "C3", "V2", "P3", "C0", "V3", "P0", "V0",
)


def fused_kernel(
    n_sp,
    n_tp,
    cap,
    residual,
    conv_value,
    conv_gate,
    docs,
    conv_kernel,
    ln_gain,
    norm_gain,
    routes,
    route_weight,
    proj_hbm,
    gate_hbm,
    up_hbm,
    down_hbm,
    mixed,
    proj,
    gate,
    up,
    down,
    taps,
    extended,
    doc_extended,
    since,
    conv,
    tail,
    tail_docs,
    halo,
    halo_docs,
    stats,
    plans,
    scales,
    activated,
    projected,
    stream,
    tokens,
    picks,
    blends,
    slots,
    hidden,
    pairs,
    outbound,
    blended,
    arrived,
    summed,
    returned,
    local_sem,
    halo_send,
    halo_recv,
    stat_send,
    stat_recv,
    plan_send,
    plan_recv,
    scale_send,
    scale_recv,
    act_send,
    act_recv,
    plane_send,
    plane_recv,
    spread_send,
    spread_recv,
    twin_send,
    twin_recv,
    swap_send,
    swap_recv,
    sum_send,
    sum_recv,
    back_send,
    back_recv,
):
    sp = lax.axis_index("sp")
    tp = lax.axis_index("tp")
    rows, cols = residual.shape
    width = cols * n_tp
    lookback = conv_kernel.shape[0] - 1
    pad = tail.shape[0]
    planes = n_sp // 2
    plane = sp // 2
    core = sp % 2
    twin = plane * 2 + 1 - core
    chunk = rows // 2
    half = chunk // 2
    across_x = tp + 1 - 2 * (tp % 2)
    across_y = (tp + 2) % n_tp
    diagonal = (across_x + 2) % n_tp
    loads = [
        pltpu.make_async_copy(src, dst, local_sem.at[i])
        for i, (src, dst) in enumerate(
            ((proj_hbm, proj), (gate_hbm, gate), (up_hbm, up), (down_hbm, down))
        )
    ]
    for load in loads:
        load.start()

    barrier = pltpu.get_barrier_semaphore()
    for i in range(1, n_sp):
        pl.semaphore_signal(
            barrier, inc=1, device_id=((sp + i) % n_sp, tp), device_id_type=pl.DeviceIdType.MESH
        )
    for i in range(1, n_tp):
        pl.semaphore_signal(
            barrier, inc=1, device_id=(sp, (tp + i) % n_tp), device_id_type=pl.DeviceIdType.MESH
        )
    sends = []

    def go(*args):
        send = remote(*args)
        send.start()
        sends.append(send)

    def landed(ref, sem):
        remote(ref, ref, act_send.at[0, 0], sem, sp, tp).wait_recv()

    def col_block(t):
        return pl.ds(pl.multiple_of(t * cols, 128), cols)

    def row_block(start, size):
        return pl.ds(pl.multiple_of(start, size), size)

    def spread_start(ref, start, ss, rs):
        block = ref.at[row_block(start, chunk), col_block(tp)]
        go(block, block, ss(1), rs(1), sp, across_x)
        go(block, block, ss(2), rs(2), sp, across_y)

    def spread_relay(ref, start, ss, rs):
        landed(ref.at[row_block(start, chunk), col_block(across_x)], rs(1))
        block = ref.at[row_block(start, half), col_block(across_x)]
        go(block, block, ss(3), rs(3), sp, across_y)
        landed(ref.at[row_block(start, chunk), col_block(across_y)], rs(2))
        block = ref.at[row_block(start + half, half), col_block(across_y)]
        go(block, block, ss(0), rs(0), sp, across_x)

    def spread_finish(ref, start, rs):
        landed(ref.at[row_block(start, half), col_block(diagonal)], rs(3))
        landed(ref.at[row_block(start + half, half), col_block(diagonal)], rs(0))

    def stats_start(i, q, first, second):
        lane = lax.broadcasted_iota(jnp.int32, (chunk, 128), 1)
        both = jnp.where(lane == 0, first, jnp.where(lane == 1, second, 0.0))
        stats[i, q, 0] = jnp.transpose(both)[0:8]
        for j in range(1, n_tp):
            go(
                stats.at[i, q, 0],
                stats.at[i, q, j],
                stat_send.at[i, q, j],
                stat_recv.at[i, q, j],
                sp,
                (tp + j) % n_tp,
            )

    def stats_total(i, q):
        total = stats[i, q, 0]
        for j in range(1, n_tp):
            landed(stats.at[i, q, j], stat_recv.at[i, q, j])
            total = total + stats[i, q, j]
        return total

    def gain_row(ref):
        return jnp.concatenate(
            [ref[i : i + 1, :].astype(jnp.float32) for i in range(cols // 128)], 1
        )

    gated = (
        conv_value[...].astype(jnp.float32) * jax.nn.sigmoid(conv_gate[...].astype(jnp.float32))
    ).astype(jnp.bfloat16)
    extended[pl.ds(pad, rows), :] = gated.astype(jnp.float32)
    tail[...] = gated[rows - pad :]
    doc_rows = jnp.transpose(jnp.broadcast_to(docs[...].astype(jnp.float32), (128, rows)))
    doc_extended[pl.ds(pad, rows), :] = doc_rows
    tail_docs[...] = doc_rows[rows - pad :]
    taps[...] = conv_kernel[...].astype(jnp.float32)
    plans[sp] = jnp.concatenate(
        [routes[...].astype(jnp.float32), route_weight[...], jnp.zeros((4, rows), jnp.float32)], 0
    )
    pl.semaphore_wait(barrier, n_sp - 1 + n_tp - 1)
    next_sp = (sp + 1) % n_sp
    go(tail, halo, halo_send.at[0], halo_recv.at[0], next_sp, tp)
    go(tail_docs, halo_docs, halo_send.at[1], halo_recv.at[1], next_sp, tp)
    for i in range(1, n_sp):
        go(plans.at[sp], plans.at[sp], plan_send.at[i], plan_recv.at[sp], (sp + i) % n_sp, tp)

    part = min(64, chunk)

    def convolve(r):
        here = pl.ds(r * part, part)
        own = doc_extended[pl.ds(pad + r * part, part), :]
        count = jnp.zeros((part, 128), jnp.float32)
        for back in range(1, lookback + 1):
            count = count + jnp.where(
                doc_extended[pl.ds(pad + r * part - back, part), :] == own, 1.0, 0.0
            )
        since[here, :] = count

        @pl.loop(0, cols // 128)
        def _(c):
            at = pl.ds(pl.multiple_of(c * 128, 128), 128)
            reach = since[here, :]
            total = jnp.zeros((part, 128), jnp.float32)
            for tap in range(lookback + 1):
                value = extended[pl.ds(pad - lookback + r * part + tap, part), at]
                total = total + jnp.where(
                    reach >= lookback - tap, value * taps[tap : tap + 1, at], 0.0
                )
            conv[here, at] = total

    def channel_stats(q):
        conv_out = conv[pl.ds(q * chunk, chunk), :]
        stats_start(
            0,
            q,
            jnp.sum(conv_out, 1, keepdims=True),
            jnp.sum(conv_out * conv_out, 1, keepdims=True),
        )

    def sems(ref, *index):
        return lambda i: ref.at[(*index, i)]

    def activate(q):
        here = pl.ds(q * chunk, chunk)
        back = jnp.transpose(jnp.concatenate([stats_total(0, q)] * 16, 0))
        mean = back[:, 0:1] / width
        scale = lax.rsqrt(back[:, 1:2] / width - mean * mean + epsilon)
        v = (conv[here, :] - mean) * scale * gain_row(ln_gain)
        activated[here, col_block(tp)] = (v * jax.nn.sigmoid(v)).astype(jnp.bfloat16)
        spread_start(activated, q * chunk, sems(act_send, q), sems(act_recv, q))

    def project(q, t):
        return jnp.dot(
            activated[pl.ds(q * chunk, chunk), col_block(t)],
            proj[col_block(t), :],
            preferred_element_type=jnp.float32,
        )

    parts = chunk // part
    for r in range(parts, 2 * parts):
        convolve(r)
    channel_stats(1)
    for r in range(1, parts):
        convolve(r)
    landed(halo, halo_recv.at[0])
    landed(halo_docs, halo_recv.at[1])
    inside = sp > 0
    extended[pl.ds(0, pad), :] = jnp.where(inside, halo[...].astype(jnp.float32), 0.0)
    doc_extended[pl.ds(0, pad), :] = jnp.where(inside, halo_docs[...], -1.0)
    convolve(0)
    channel_stats(0)
    activate(1)
    activate(0)

    for i in range(1, n_sp):
        e = (sp + i) % n_sp
        landed(plans.at[e], plan_recv.at[e])
    token = lax.broadcasted_iota(jnp.int32, (rows, rows), 0)
    later = jnp.where(
        token < lax.broadcasted_iota(jnp.int32, (rows, rows), 1), 1.0, 0.0
    ).astype(jnp.bfloat16)
    slot_id = lax.broadcasted_iota(jnp.int32, (cap, rows), 0)

    def named_by(s, expert):
        plan = plans[s]
        first = plan[0:1] == expert
        second = plan[1:2] == expert
        weight = jnp.where(first, plan[2:3], 0.0) + jnp.where(second, plan[3:4], 0.0)
        return jnp.where(first | second, 1.0, 0.0), weight

    def slots_of(sources, expert):
        both = [named_by(s, expert) for s in sources]
        named = jnp.concatenate([n for n, _ in both] + [jnp.zeros_like(both[0][0])] * (8 - len(both)), 0)
        rank = jnp.dot(named.astype(jnp.bfloat16), later, preferred_element_type=jnp.float32)
        slot = jnp.where(named > 0.5, rank, -1.0).astype(jnp.int32)
        return [(slot[i : i + 1], weight) for i, (_, weight) in enumerate(both)]

    mine = slots_of([2 * p + core for p in range(planes)], sp.astype(jnp.float32))
    rest = slots_of([2 * p + 1 - core for p in range(planes)], sp.astype(jnp.float32))
    other = slots_of([2 * p + core for p in range(planes)], twin.astype(jnp.float32))
    for p in range(planes):
        slot, weight = mine[p]
        picks[p, 0:cap] = jnp.where(slot == slot_id, 1.0, 0.0).astype(jnp.bfloat16)
        own_blend = jnp.where(slot == slot_id, weight, 0.0)
        slot, weight = rest[p]
        picks[p, cap : 2 * cap] = jnp.where(slot == slot_id, 1.0, 0.0).astype(jnp.bfloat16)
        slot, weight = other[p]
        twin_blend = jnp.where(slot == slot_id, weight, 0.0)
        blends[p] = jnp.transpose(jnp.concatenate([own_blend, twin_blend], 0)).astype(jnp.bfloat16)

    order = [0] + sorted(range(1, planes), key=lambda k: -min(k, planes - k))

    plane_order = {
        1: [(order[1], 1)],
        0: [(order[1], 0)] + [(k, q) for k in order[2:] for q in (1, 0)],
    }

    def source(k):
        return (plane + k) % planes * 2 + core

    def first_row(k, q):
        return source(k) * rows + q * chunk

    def residual_rows(q):
        here = pl.ds(q * chunk, chunk)
        spread_relay(activated, q * chunk, sems(act_send, q), sems(act_recv, q))
        projected[here, :] += project(q, across_x) + project(q, across_y)
        spread_finish(activated, q * chunk, sems(act_recv, q))
        total = projected[here, :] + project(q, diagonal)
        stream_rows = (
            residual[here, :].astype(jnp.float32)
            + total.astype(jnp.bfloat16).astype(jnp.float32)
        ).astype(jnp.bfloat16)
        stream[here, :] = stream_rows
        stream_part = stream_rows.astype(jnp.float32)
        tokens[row_block(first_row(0, q), chunk), col_block(tp)] = (
            stream_part * gain_row(norm_gain)
        ).astype(jnp.bfloat16)
        spread_start(tokens, first_row(0, q), sems(spread_send, 0, q), sems(spread_recv, 0, q))
        for k, part_q in plane_order[q]:
            block = tokens.at[row_block(first_row(0, part_q), chunk), col_block(tp)]
            go(
                block,
                block,
                plane_send.at[k, part_q],
                plane_recv.at[k, part_q],
                (plane - k + planes) % planes * 2 + core,
                tp,
            )
        square = jnp.sum(stream_part * stream_part, 1, keepdims=True)
        stats_start(1, q, square, square)

    loads[0].wait()
    for q in (1, 0):
        projected[pl.ds(q * chunk, chunk), :] = project(q, tp)
    residual_rows(1)
    residual_rows(0)

    def spread(k, q):
        block = tokens.at[row_block(first_row(k, q), chunk), col_block(tp)]
        landed(block, plane_recv.at[k, q])
        spread_start(tokens, first_row(k, q), sems(spread_send, k, q), sems(spread_recv, k, q))

    def relay(k, q):
        spread_relay(tokens, first_row(k, q), sems(spread_send, k, q), sems(spread_recv, k, q))

    def finish(k, q):
        spread_finish(tokens, first_row(k, q), sems(spread_recv, k, q))
        block = tokens.at[row_block(first_row(k, q), chunk), :]
        go(block, block, twin_send.at[k, q], twin_recv.at[k, q], twin, tp)

    def share_scales():
        for q in range(2):
            scales[sp, :, pl.ds(q * chunk, chunk)] = lax.rsqrt(
                stats_total(1, q) / width + epsilon
            )
        for i in range(1, n_sp):
            go(
                scales.at[sp],
                scales.at[sp],
                scale_send.at[i],
                scale_recv.at[sp],
                (sp + i) % n_sp,
                tp,
            )

    def gather(k):
        p = (plane + k) % planes
        for q in range(2):
            start = (2 * p + 1 - core) * rows + q * chunk
            landed(tokens.at[row_block(start, chunk), :], twin_recv.at[k, q])
        for j in range(2):
            s = 2 * p + (core if j == 0 else 1 - core)
            if k == 0 and j == 0:
                pass
            else:
                landed(scales.at[s], scale_recv.at[s])
            here = pl.ds(j * cap, cap)
            pick = picks[p, here, :]
            slots[here, :] = jnp.dot(
                pick, tokens[row_block(s * rows, rows), :], preferred_element_type=jnp.float32
            ).astype(jnp.bfloat16)
            scale = jnp.sum(pick.astype(jnp.float32) * scales[s][0:1, :], 1, keepdims=True)
            since[here, :] = jnp.broadcast_to(scale, (cap, 128))

    def raise_up(k, piece):
        size = gate.shape[1] // 2
        at = pl.ds(piece * size, size)
        scale = jnp.concatenate([since[0 : 2 * cap, :]] * (size // 128), 1)
        g = scale * jnp.dot(slots[...], gate[:, at], preferred_element_type=jnp.float32)
        u = scale * jnp.dot(slots[...], up[:, at], preferred_element_type=jnp.float32)
        hidden[:, at] = (g * jax.nn.sigmoid(g) * u).astype(jnp.bfloat16)

    def bring_down(k, piece):
        size = width // 2
        at = pl.ds(piece * size, size)
        result = jnp.dot(
            hidden[...], down[:, at], preferred_element_type=jnp.float32
        ).astype(jnp.bfloat16)
        pairs[k, 0:cap, at] = result[0:cap]
        outbound[k, :, at] = result[cap:]
        if piece == 1:
            go(
                outbound.at[k],
                pairs.at[k, pl.ds(cap, cap), :],
                swap_send.at[k],
                swap_recv.at[k],
                twin,
                tp,
            )

    low, high = pl.ds(0, chunk), pl.ds(chunk, chunk)

    def combine(k):
        p = (plane + k) % planes
        landed(pairs.at[k, pl.ds(cap, cap), :], swap_recv.at[k])

        blended[k] = jnp.dot(
            blends[p], pairs[k], preferred_element_type=jnp.float32
        ).astype(jnp.bfloat16)

        for i, (part_rows, block, peer) in enumerate(
            (
                (low, diagonal, across_x),
                (high, diagonal, across_y),
                (low, across_x, across_x),
                (high, across_y, across_y),
            )
        ):
            go(
                blended.at[k, part_rows, col_block(block)],
                arrived.at[k, i, low],
                sum_send.at[k, i],
                sum_recv.at[k, i],
                sp,
                peer,
            )

    def pass_on(k):
        for i, (part_rows, peer) in enumerate(((low, across_y), (high, across_x))):
            landed(arrived.at[k, i, low], sum_recv.at[k, i])
            arrived[k, 2 + i, high] = (
                blended[k, part_rows, col_block(peer)].astype(jnp.float32)
                + arrived[k, i, low].astype(jnp.float32)
            ).astype(jnp.bfloat16)
            go(
                arrived.at[k, 2 + i, high],
                arrived.at[k, i, high],
                sum_send.at[k, 4 + i],
                sum_recv.at[k, 4 + i],
                sp,
                peer,
            )

    def give_back(k):
        for i, part_rows in enumerate((low, high)):
            landed(arrived.at[k, 2 + i, low], sum_recv.at[k, 2 + i])
            landed(arrived.at[k, i, high], sum_recv.at[k, 4 + i])
            total = (
                blended[k, part_rows, col_block(tp)].astype(jnp.float32)
                + arrived[k, 2 + i, low].astype(jnp.float32)
                + arrived[k, i, high].astype(jnp.float32)
            )
            if k == 0:
                here = pl.ds(i * chunk, chunk)
                total = total + stream[here, :].astype(jnp.float32)
                for j in order[1:]:
                    landed(returned.at[j, part_rows], back_recv.at[j, i])
                    total = total + returned[j, part_rows].astype(jnp.float32)
                mixed[here, :] = total.astype(jnp.bfloat16)
            else:
                summed[k, part_rows] = total.astype(jnp.bfloat16)
                go(
                    summed.at[k, part_rows],
                    returned.at[k, part_rows],
                    back_send.at[k, i],
                    back_recv.at[k, i],
                    source(k),
                    tp,
                )

    def weights_ready():
        for load in loads[1:]:
            load.wait()

    steps = {
        "R": relay,
        "S": spread,
        "F": finish,
        "G": gather,
        "U": raise_up,
        "D": bring_down,
        "C": combine,
        "P": pass_on,
        "V": give_back,
        "H": share_scales,
        "L": weights_ready,
    }
    for word in schedule:
        indices = [int(digit) for digit in word[1:]]
        steps[word[0]](*[order[i] for i in indices[:1]], *indices[1:])
    for send in sends:
        send.wait_send()


def fused(operands, rows, cols, n_sp, n_tp, cap, width, units, taps):
    planes = n_sp // 2
    pad = (taps - 1 + 15) // 16 * 16
    chunk = rows // 2
    bf16, f32 = jnp.bfloat16, jnp.float32
    dma = pltpu.SemaphoreType.DMA
    vmem = pl.BlockSpec(memory_space=pltpu.VMEM)
    anywhere = pl.BlockSpec(memory_space=pl.ANY)
    return pl.pallas_call(
        functools.partial(fused_kernel, n_sp, n_tp, cap),
        out_shape=jax.ShapeDtypeStruct((rows, cols), bf16),
        in_specs=[vmem] * 9 + [anywhere] * 4,
        out_specs=vmem,
        scratch_shapes=[
            pltpu.VMEM((width, cols), bf16),
            pltpu.VMEM((width, units), bf16),
            pltpu.VMEM((width, units), bf16),
            pltpu.VMEM((units, width), bf16),
            pltpu.VMEM((taps, cols), f32),
            pltpu.VMEM((pad + rows, cols), f32),
            pltpu.VMEM((pad + rows, 128), f32),
            pltpu.VMEM((max(rows, 2 * cap), 128), f32),
            pltpu.VMEM((rows, cols), f32),
            pltpu.VMEM((pad, cols), bf16),
            pltpu.VMEM((pad, 128), f32),
            pltpu.VMEM((pad, cols), bf16),
            pltpu.VMEM((pad, 128), f32),
            pltpu.VMEM((2, 2, n_tp, 8, chunk), f32),
            pltpu.VMEM((n_sp, 8, rows), f32),
            pltpu.VMEM((n_sp, 8, rows), f32),
            pltpu.VMEM((rows, width), bf16),
            pltpu.VMEM((rows, cols), f32),
            pltpu.VMEM((rows, cols), bf16),
            pltpu.VMEM((n_sp * rows, width), bf16),
            pltpu.VMEM((planes, 2 * cap, rows), bf16),
            pltpu.VMEM((planes, rows, 2 * cap), bf16),
            pltpu.VMEM((2 * cap, width), bf16),
            pltpu.VMEM((2 * cap, units), bf16),
            pltpu.VMEM((planes, 2 * cap, width), bf16),
            pltpu.VMEM((planes, cap, width), bf16),
            pltpu.VMEM((planes, rows, width), bf16),
            pltpu.VMEM((planes, 4, rows, cols), bf16),
            pltpu.VMEM((planes, rows, cols), bf16),
            pltpu.VMEM((planes, rows, cols), bf16),
            dma((4,)),
            dma((2,)),
            dma((2,)),
            dma((2, 2, n_tp)),
            dma((2, 2, n_tp)),
            dma((n_sp,)),
            dma((n_sp,)),
            dma((n_sp,)),
            dma((n_sp,)),
            dma((2, 4)),
            dma((2, 4)),
            dma((planes, 2)),
            dma((planes, 2)),
            dma((planes, 2, 4)),
            dma((planes, 2, 4)),
            dma((planes, 2)),
            dma((planes, 2)),
            dma((planes,)),
            dma((planes,)),
            dma((planes, 6)),
            dma((planes, 6)),
            dma((planes, 2)),
            dma((planes, 2)),
        ],
        compiler_params=pltpu.CompilerParams(
            collective_id=0, has_side_effects=True, vmem_limit_bytes=56 << 20
        ),
    )(*operands)


def per_device(
    residual_in,
    conv_value,
    conv_gate,
    doc_ids,
    conv_kernel,
    ln_gain,
    out_weight,
    norm_gain,
    routes,
    route_weight,
    gate_w,
    up_w,
    down_w,
):
    rows, cols = residual_in.shape
    n_sp = lax.axis_size("sp")
    n_tp = lax.axis_size("tp")
    cap = 4 * rows // n_sp
    _, width, units = gate_w.shape
    group_rows = n_sp // groups * cap
    taps = conv_kernel.shape[0]
    pad = (taps - 1 + 15) // 16 * 16
    if n_tp == 4 and n_sp == 8:
        operands = (
            residual_in,
            conv_value,
            conv_gate,
            doc_ids.reshape(1, rows),
            conv_kernel,
            ln_gain.reshape(cols // 128, 128),
            norm_gain.reshape(cols // 128, 128),
            routes.T,
            route_weight.T,
            out_weight,
            gate_w[0],
            up_w[0],
            down_w[0],
        )
        return fused(operands, rows, cols, n_sp, n_tp, cap, width, units, taps)
    bf16, f32 = jnp.bfloat16, jnp.float32
    dma = pltpu.SemaphoreType.DMA
    vmem = pl.BlockSpec(memory_space=pltpu.VMEM)
    anywhere = pl.BlockSpec(memory_space=pl.ANY)
    return pl.pallas_call(
        functools.partial(layer_kernel, n_sp, n_tp, cap),
        out_shape=jax.ShapeDtypeStruct((rows, cols), bf16),
        in_specs=[vmem] * 9 + [anywhere] * 4,
        out_specs=vmem,
        scratch_shapes=[
            pltpu.VMEM((width, cols), bf16),
            pltpu.VMEM((width, units), bf16),
            pltpu.VMEM((width, units), bf16),
            pltpu.VMEM((units, width), bf16),
            pltpu.VMEM((taps, cols), f32),
            pltpu.VMEM((pad + rows, cols), f32),
            pltpu.VMEM((pad + rows, 128), f32),
            pltpu.VMEM((rows, 128), f32),
            pltpu.VMEM((rows, cols), f32),
            pltpu.VMEM((pad, cols), bf16),
            pltpu.VMEM((pad, 128), f32),
            pltpu.VMEM((pad, cols), bf16),
            pltpu.VMEM((pad, 128), f32),
            pltpu.VMEM((2, n_tp, 8, rows), f32),
            pltpu.VMEM((rows, width), bf16),
            pltpu.VMEM((rows, cols), f32),
            pltpu.VMEM((rows, cols), bf16),
            pltpu.VMEM((rows, cols), bf16),
            pltpu.VMEM((n_sp, rows, cap), bf16),
            pltpu.VMEM((n_sp, cap, cols), bf16),
            pltpu.VMEM((n_sp * cap, width), bf16),
            pltpu.VMEM((group_rows, units), bf16),
            pltpu.VMEM((groups, group_rows, width), bf16),
            pltpu.VMEM((groups, n_tp, group_rows, cols), bf16),
            pltpu.VMEM((groups, group_rows, cols), bf16),
            pltpu.VMEM((n_sp, cap, cols), bf16),
            pltpu.VMEM((n_sp, rows, cap), bf16),
            pltpu.VMEM((n_sp, rows, cap), bf16),
            dma((4,)),
            dma((2,)),
            dma((2,)),
            dma((2, n_tp)),
            dma((2, n_tp)),
            dma((n_tp,)),
            dma((n_tp,)),
            dma((n_sp,)),
            dma((n_sp,)),
            dma((groups, n_tp)),
            dma((groups, n_tp)),
            dma((groups, n_tp + 2)),
            dma((groups, n_tp + 2)),
            dma((n_sp,)),
            dma((n_sp,)),
        ],
        compiler_params=pltpu.CompilerParams(
            collective_id=0, has_side_effects=True, vmem_limit_bytes=54 << 20
        ),
    )(
        residual_in,
        conv_value,
        conv_gate,
        doc_ids.reshape(1, rows),
        conv_kernel,
        ln_gain.reshape(1, cols),
        norm_gain.reshape(1, cols),
        routes,
        route_weight,
        out_weight,
        gate_w[0],
        up_w[0],
        down_w[0],
    )


def solution(mesh):
    in_specs = (
        P("sp", "tp"),
        P("sp", "tp"),
        P("sp", "tp"),
        P("sp"),
        P(None, "tp"),
        P("tp"),
        P(None, "tp"),
        P("tp"),
        P("sp", None),
        P("sp", None),
        P("sp", None, "tp"),
        P("sp", None, "tp"),
        P("sp", "tp", None),
    )
    out_specs = P("sp", "tp")
    return jax.shard_map(
        per_device, mesh=mesh, in_specs=in_specs, out_specs=out_specs, check_vma=False
    )
```

```python
import functools

import jax
import jax.numpy as jnp
from jax import lax
from jax.experimental import pallas as pl
from jax.experimental.pallas import tpu as pltpu
from jax.sharding import PartitionSpec as P

epsilon = 1e-06
groups = 4


def transposed_dot(a, b):
    return lax.dot_general(a, b, (((0,), (0,)), ((), ())), preferred_element_type=jnp.float32)


def remote(src, dst, send_sem, recv_sem, sp, tp):
    return pltpu.make_async_remote_copy(
        src_ref=src,
        dst_ref=dst,
        send_sem=send_sem,
        recv_sem=recv_sem,
        device_id=(sp, tp),
        device_id_type=pl.DeviceIdType.MESH,
    )


def layer_kernel(
    n_sp,
    n_tp,
    cap,
    residual,
    conv_value,
    conv_gate,
    docs,
    conv_kernel,
    ln_gain,
    norm_gain,
    routes,
    route_weight,
    proj_hbm,
    gate_hbm,
    up_hbm,
    down_hbm,
    mixed,
    proj,
    gate,
    up,
    down,
    taps,
    extended,
    doc_extended,
    since,
    conv,
    tail,
    tail_docs,
    halo,
    halo_docs,
    stats,
    activated,
    projected,
    stream,
    normed,
    chosen,
    outbound,
    slots,
    hidden,
    partial,
    arrived,
    summed,
    returned,
    weight_hi,
    weight_lo,
    local_sem,
    halo_send,
    halo_recv,
    stat_send,
    stat_recv,
    act_send,
    act_recv,
    out_send,
    out_recv,
    spread_send,
    spread_recv,
    sum_send,
    sum_recv,
    back_send,
    back_recv,
):
    sp = lax.axis_index("sp")
    tp = lax.axis_index("tp")
    rows, cols = residual.shape
    width = cols * n_tp
    lookback = conv_kernel.shape[0] - 1
    pad = tail.shape[0]
    per_group = n_sp // groups
    group_rows = per_group * cap
    my_group = sp // per_group
    my_member = sp % per_group
    relays = n_tp == 4
    across_x = tp + 1 - 2 * (tp % 2)
    across_y = (tp + 2) % n_tp
    diagonal = (across_x + 2) % n_tp
    loads = [
        pltpu.make_async_copy(src, dst, local_sem.at[i])
        for i, (src, dst) in enumerate(
            ((proj_hbm, proj), (gate_hbm, gate), (up_hbm, up), (down_hbm, down))
        )
    ]
    for load in loads:
        load.start()

    barrier = pltpu.get_barrier_semaphore()
    for i in range(1, n_sp):
        pl.semaphore_signal(
            barrier, inc=1, device_id=((sp + i) % n_sp, tp), device_id_type=pl.DeviceIdType.MESH
        )
    for i in range(1, n_tp):
        pl.semaphore_signal(
            barrier, inc=1, device_id=(sp, (tp + i) % n_tp), device_id_type=pl.DeviceIdType.MESH
        )
    sends = []

    def go(*args):
        send = remote(*args)
        send.start()
        sends.append(send)

    def landed(ref, sem):
        remote(ref, ref, act_send.at[0], sem, sp, tp).wait_recv()

    def col_block(t):
        return pl.ds(pl.multiple_of(t * cols, 128), cols)

    def spread_start(ref, start, size, ss, rs):
        block = ref.at[pl.ds(start, size), col_block(tp)]
        if relays:
            go(block, block, ss(1), rs(1), sp, across_x)
            go(block, block, ss(2), rs(2), sp, across_y)
        else:
            for j in range(1, n_tp):
                go(block, block, ss(j), rs(j), sp, (tp + j) % n_tp)

    def spread_relay(ref, start, size, ss, rs):
        if relays:
            half = size // 2
            landed(ref.at[pl.ds(start, size), col_block(across_x)], rs(1))
            block = ref.at[pl.ds(start, half), col_block(across_x)]
            go(block, block, ss(3), rs(3), sp, across_y)
            landed(ref.at[pl.ds(start, size), col_block(across_y)], rs(2))
            block = ref.at[pl.ds(start + half, half), col_block(across_y)]
            go(block, block, ss(0), rs(0), sp, across_x)

    def spread_finish(ref, start, size, rs):
        if relays:
            half = size // 2
            landed(ref.at[pl.ds(start, half), col_block(diagonal)], rs(3))
            landed(ref.at[pl.ds(start + half, half), col_block(diagonal)], rs(0))
        else:
            for j in range(1, n_tp):
                landed(
                    ref.at[pl.ds(start, size), col_block((tp - j + n_tp) % n_tp)], rs(j)
                )

    def stats_start(i, first, second):
        lane = lax.broadcasted_iota(jnp.int32, (rows, 128), 1)
        both = jnp.where(lane == 0, first, jnp.where(lane == 1, second, 0.0))
        stats[i, 0] = jnp.transpose(both)[0:8]
        for j in range(1, n_tp):
            go(
                stats.at[i, 0],
                stats.at[i, j],
                stat_send.at[i, j],
                stat_recv.at[i, j],
                sp,
                (tp + j) % n_tp,
            )

    def stats_finish(i):
        total = stats[i, 0]
        for j in range(1, n_tp):
            landed(stats.at[i, j], stat_recv.at[i, j])
            total = total + stats[i, j]
        back = jnp.transpose(jnp.concatenate([total] * 16, 0))
        return back[:, 0:1], back[:, 1:2]

    gated = (
        conv_value[...].astype(jnp.float32) * jax.nn.sigmoid(conv_gate[...].astype(jnp.float32))
    ).astype(jnp.bfloat16)
    extended[pl.ds(pad, rows), :] = gated.astype(jnp.float32)
    tail[...] = gated[rows - pad :]
    doc_rows = jnp.transpose(
        jnp.broadcast_to(docs[...].astype(jnp.float32), (128, rows))
    )
    doc_extended[pl.ds(pad, rows), :] = doc_rows
    tail_docs[...] = doc_rows[rows - pad :]
    taps[...] = conv_kernel[...].astype(jnp.float32)
    pl.semaphore_wait(barrier, n_sp - 1 + n_tp - 1)
    next_sp = (sp + 1) % n_sp
    tails = [
        remote(tail, halo, halo_send.at[0], halo_recv.at[0], next_sp, tp),
        remote(tail_docs, halo_docs, halo_send.at[1], halo_recv.at[1], next_sp, tp),
    ]
    for send in tails:
        send.start()
        sends.append(send)

    part = min(64, rows)

    def convolve(r):
        here = pl.ds(r * part, part)
        own = doc_extended[pl.ds(pad + r * part, part), :]
        count = jnp.zeros((part, 128), jnp.float32)
        for back in range(1, lookback + 1):
            count = count + jnp.where(
                doc_extended[pl.ds(pad + r * part - back, part), :] == own, 1.0, 0.0
            )
        since[here, :] = count

        @pl.loop(0, cols // 128)
        def _(c):
            at = pl.ds(pl.multiple_of(c * 128, 128), 128)
            reach = since[here, :]
            total = jnp.zeros((part, 128), jnp.float32)
            for tap in range(lookback + 1):
                value = extended[pl.ds(pad - lookback + r * part + tap, part), at]
                total = total + jnp.where(
                    reach >= lookback - tap, value * taps[tap : tap + 1, at], 0.0
                )
            conv[here, at] = total

    for r in range(1, rows // part):
        convolve(r)
    landed(halo, halo_recv.at[0])
    landed(halo_docs, halo_recv.at[1])
    inside = sp > 0
    extended[pl.ds(0, pad), :] = jnp.where(inside, halo[...].astype(jnp.float32), 0.0)
    doc_extended[pl.ds(0, pad), :] = jnp.where(inside, halo_docs[...], -1.0)
    convolve(0)
    conv_out = conv[...]
    stats_start(
        0,
        jnp.sum(conv_out, 1, keepdims=True),
        jnp.sum(conv_out * conv_out, 1, keepdims=True),
    )

    expert_id = lax.broadcasted_iota(jnp.int32, (rows, n_sp), 1)
    first = routes[:, 0:1] == expert_id
    second = routes[:, 1:2] == expert_id
    named = jnp.where(first | second, 1.0, 0.0)
    earlier = jnp.where(
        lax.broadcasted_iota(jnp.int32, (rows, rows), 1)
        < lax.broadcasted_iota(jnp.int32, (rows, rows), 0),
        1.0,
        0.0,
    ).astype(jnp.bfloat16)
    rank = jnp.dot(earlier, named.astype(jnp.bfloat16), preferred_element_type=jnp.float32)
    slot = jnp.where(first | second, rank, -1.0).astype(jnp.int32)
    weight = jnp.where(first, route_weight[:, 0:1], 0.0) + jnp.where(
        second, route_weight[:, 1:2], 0.0
    )
    slot_id = lax.broadcasted_iota(jnp.int32, (rows, cap), 1)
    for e in range(n_sp):
        chosen[e] = jnp.where(slot[:, e : e + 1] == slot_id, 1.0, 0.0).astype(jnp.bfloat16)

    channel_sum, channel_sq = stats_finish(0)
    mean = channel_sum / width
    scale = lax.rsqrt(channel_sq / width - mean * mean + epsilon)
    v = (conv[...] - mean) * scale * ln_gain[...].astype(jnp.float32)
    activated[:, col_block(tp)] = (v * jax.nn.sigmoid(v)).astype(jnp.bfloat16)

    def act_block(i):
        return act_send.at[i]

    def act_arrival(i):
        return act_recv.at[i]

    spread_start(activated, 0, rows, act_block, act_arrival)
    loads[0].wait()

    def project(t):
        return jnp.dot(
            activated[:, col_block(t)],
            proj[pl.ds(pl.multiple_of(t * cols, 128), cols), :],
            preferred_element_type=jnp.float32,
        )

    projected[...] = project(tp)
    for e in range(n_sp):
        at = jnp.where(slot[:, e : e + 1] == slot_id, weight[:, e : e + 1], 0.0)
        hi = at.astype(jnp.bfloat16)
        weight_hi[e] = hi
        weight_lo[e] = (at - hi.astype(jnp.float32)).astype(jnp.bfloat16)
    spread_relay(activated, 0, rows, act_block, act_arrival)
    if relays:
        projected[...] += project(across_x) + project(across_y)
    spread_finish(activated, 0, rows, act_arrival)
    if relays:
        projected[...] += project(diagonal)
    else:
        for j in range(1, n_tp):
            projected[...] += project((tp + j) % n_tp)
    stream[...] = (
        residual[...].astype(jnp.float32)
        + projected[...].astype(jnp.bfloat16).astype(jnp.float32)
    ).astype(jnp.bfloat16)
    stream_part = stream[...].astype(jnp.float32)
    square = jnp.sum(stream_part * stream_part, 1, keepdims=True)
    stats_start(1, square, square)
    row_total, _ = stats_finish(1)
    normed[...] = (
        stream[...].astype(jnp.float32)
        * lax.rsqrt(row_total / width + epsilon)
        * norm_gain[...].astype(jnp.float32)
    ).astype(jnp.bfloat16)

    def source_rows(s):
        return pl.ds(pl.multiple_of(s * cap, cap), cap)

    def group_start(k):
        return pl.multiple_of((my_group + k) % groups * group_rows, group_rows)

    for k in range(groups):
        for j in range(per_group):
            dest = (my_group - k + groups) % groups * per_group + (my_member + j) % per_group
            rows_out = transposed_dot(chosen[dest], normed[...]).astype(jnp.bfloat16)
            if k == 0 and j == 0:
                slots[source_rows(sp), col_block(tp)] = rows_out
                continue
            outbound[dest] = rows_out
            go(
                outbound.at[dest],
                slots.at[source_rows(sp), col_block(tp)],
                out_send.at[k * per_group + j],
                out_recv.at[sp],
                dest,
                tp,
            )

    def spread_sems(sems, k):
        return lambda i: sems.at[k, i]

    def spread(k):
        for j in range(per_group):
            if k == 0 and j == 0:
                continue
            source = (my_group + k) % groups * per_group + (my_member + j) % per_group
            landed(slots.at[source_rows(source), col_block(tp)], out_recv.at[source])
        spread_start(
            slots, group_start(k), group_rows, spread_sems(spread_send, k), spread_sems(spread_recv, k)
        )

    def relay(k):
        spread_relay(
            slots, group_start(k), group_rows, spread_sems(spread_send, k), spread_sems(spread_recv, k)
        )

    half = group_rows // 2
    low, high = pl.ds(0, half), pl.ds(half, half)

    def compute(k):
        spread_finish(slots, group_start(k), group_rows, spread_sems(spread_recv, k))
        x = pl.ds(group_start(k), group_rows)
        units = gate.shape[1]
        tile = min(256, units)

        @pl.loop(0, units // tile)
        def _(n):
            at = pl.ds(pl.multiple_of(n * tile, tile), tile)
            g = jnp.dot(slots[x, :], gate[:, at], preferred_element_type=jnp.float32)
            u = jnp.dot(slots[x, :], up[:, at], preferred_element_type=jnp.float32)
            hidden[:, at] = (g * jax.nn.sigmoid(g) * u).astype(jnp.bfloat16)

        @pl.loop(0, width // 256)
        def _(n):
            at = pl.ds(pl.multiple_of(n * 256, 256), 256)
            partial[k, :, at] = jnp.dot(
                hidden[...], down[:, at], preferred_element_type=jnp.float32
            ).astype(jnp.bfloat16)

        if relays:
            for i, (part_rows, block, peer) in enumerate(
                (
                    (low, across_x, across_x),
                    (low, diagonal, across_x),
                    (high, across_y, across_y),
                    (high, diagonal, across_y),
                )
            ):
                go(
                    partial.at[k, part_rows, col_block(block)],
                    arrived.at[k, i, low],
                    sum_send.at[k, i],
                    sum_recv.at[k, i],
                    sp,
                    peer,
                )
        else:
            for j in range(1, n_tp):
                peer = (tp + j) % n_tp
                go(
                    partial.at[k, :, col_block(peer)],
                    arrived.at[k, j],
                    sum_send.at[k, j],
                    sum_recv.at[k, j],
                    sp,
                    peer,
                )

    def pass_on(k):
        if relays:
            for i, (part_rows, peer) in enumerate(((low, across_y), (high, across_x))):
                landed(arrived.at[k, 2 * i + 1, low], sum_recv.at[k, 2 * i + 1])
                arrived[k, 2 + i, high] = (
                    partial[k, part_rows, col_block(peer)].astype(jnp.float32)
                    + arrived[k, 2 * i + 1, low].astype(jnp.float32)
                ).astype(jnp.bfloat16)
                go(
                    arrived.at[k, 2 + i, high],
                    arrived.at[k, i, high],
                    sum_send.at[k, 4 + i],
                    sum_recv.at[k, 4 + i],
                    sp,
                    peer,
                )

    def give_back(k):
        if relays:
            for i, part_rows in enumerate((low, high)):
                landed(arrived.at[k, 2 * i, low], sum_recv.at[k, 2 * i])
                landed(arrived.at[k, i, high], sum_recv.at[k, 4 + i])
                summed[k, part_rows] = (
                    partial[k, part_rows, col_block(tp)].astype(jnp.float32)
                    + arrived[k, 2 * i, low].astype(jnp.float32)
                    + arrived[k, i, high].astype(jnp.float32)
                ).astype(jnp.bfloat16)
        else:
            total = partial[k, :, col_block(tp)].astype(jnp.float32)
            for j in range(1, n_tp):
                landed(arrived.at[k, j], sum_recv.at[k, j])
                total = total + arrived[k, j].astype(jnp.float32)
            summed[k] = total.astype(jnp.bfloat16)
        for j in range(per_group):
            member = (my_member + j) % per_group
            source = (my_group + k) % groups * per_group + member
            part = pl.ds(pl.multiple_of(member * cap, cap), cap)
            if k == 0 and j == 0:
                returned[sp] = summed[k, part, :]
                continue
            go(
                summed.at[k, part, :],
                returned.at[sp],
                back_send.at[k * per_group + j],
                back_recv.at[sp],
                source,
                tp,
            )

    spread(0)
    spread(1)
    relay(0)
    spread(2)
    relay(1)
    for load in loads[1:]:
        load.wait()
    compute(0)
    spread(3)
    relay(2)
    compute(1)
    pass_on(0)
    relay(3)
    compute(2)
    pass_on(1)
    give_back(0)
    compute(3)
    pass_on(2)
    give_back(1)
    pass_on(3)
    give_back(2)
    give_back(3)
    for i in range(1, n_sp):
        e = (sp + i) % n_sp
        landed(returned.at[e], back_recv.at[e])
    routed = jnp.zeros((rows, cols), jnp.float32)
    for e in range(n_sp):
        routed = routed + jnp.dot(weight_hi[e], returned[e], preferred_element_type=jnp.float32)
        routed = routed + jnp.dot(weight_lo[e], returned[e], preferred_element_type=jnp.float32)
    mixed[...] = (stream[...].astype(jnp.float32) + routed).astype(jnp.bfloat16)
    for send in sends:
        send.wait_send()


schedule = (
    "R01", "R00", "H",
    "S11", "S10",
    "F01", "F00",
    "R11", "S21", "R10", "S20", "B", "L",
    "G0", "U00", "U01",
    "F11", "F10", "R21", "S31",
    "D00", "D01", "R20",
    "G1", "U10", "U11", "F21", "F20", "D10", "D11",
    "R31", "C1",
    "G2", "U20", "U21", "F31", "P1", "D20", "D21",
    "F30", "C2",
    "G3", "U30", "U31", "V1", "D30", "D31",
    "P2", "C3", "V2", "P3", "C0", "V3", "P0", "V0",
)


def fused_kernel(
    n_sp,
    n_tp,
    cap,
    residual,
    conv_value,
    conv_gate,
    docs,
    conv_kernel,
    ln_gain,
    norm_gain,
    routes,
    route_weight,
    proj_hbm,
    gate_hbm,
    up_hbm,
    down_hbm,
    mixed,
    proj,
    gate,
    up,
    down,
    taps,
    extended,
    doc_extended,
    since,
    conv,
    tail,
    tail_docs,
    halo,
    halo_docs,
    stats,
    plans,
    scales,
    activated,
    projected,
    stream,
    tokens,
    picks,
    blends,
    slots,
    hidden,
    pairs,
    outbound,
    blended,
    arrived,
    summed,
    returned,
    local_sem,
    halo_send,
    halo_recv,
    stat_send,
    stat_recv,
    plan_send,
    plan_recv,
    scale_send,
    scale_recv,
    act_send,
    act_recv,
    plane_send,
    plane_recv,
    spread_send,
    spread_recv,
    twin_send,
    twin_recv,
    swap_send,
    swap_recv,
    sum_send,
    sum_recv,
    back_send,
    back_recv,
):
    sp = lax.axis_index("sp")
    tp = lax.axis_index("tp")
    rows, cols = residual.shape
    width = cols * n_tp
    lookback = conv_kernel.shape[0] - 1
    pad = tail.shape[0]
    planes = n_sp // 2
    plane = sp // 2
    core = sp % 2
    twin = plane * 2 + 1 - core
    chunk = rows // 2
    strip = rows // 4
    across_x = tp + 1 - 2 * (tp % 2)
    across_y = (tp + 2) % n_tp
    diagonal = (across_x + 2) % n_tp
    loads = [
        pltpu.make_async_copy(src, dst, local_sem.at[i])
        for i, (src, dst) in enumerate(
            ((proj_hbm, proj), (gate_hbm, gate), (up_hbm, up), (down_hbm, down))
        )
    ]
    for load in loads:
        load.start()

    barrier = pltpu.get_barrier_semaphore()
    for i in range(1, n_sp):
        pl.semaphore_signal(
            barrier, inc=1, device_id=((sp + i) % n_sp, tp), device_id_type=pl.DeviceIdType.MESH
        )
    for i in range(1, n_tp):
        pl.semaphore_signal(
            barrier, inc=1, device_id=(sp, (tp + i) % n_tp), device_id_type=pl.DeviceIdType.MESH
        )
    sends = []

    def go(*args):
        send = remote(*args)
        send.start()
        sends.append(send)

    def landed(ref, sem):
        remote(ref, ref, act_send.at[0, 0], sem, sp, tp).wait_recv()

    def col_block(t):
        return pl.ds(pl.multiple_of(t * cols, 128), cols)

    def row_block(start, size):
        return pl.ds(pl.multiple_of(start, size), size)

    def spread_start(ref, start, size, ss, rs):
        block = ref.at[row_block(start, size), col_block(tp)]
        go(block, block, ss(1), rs(1), sp, across_x)
        go(block, block, ss(2), rs(2), sp, across_y)

    def spread_relay(ref, start, size, ss, rs):
        half = size // 2
        landed(ref.at[row_block(start, size), col_block(across_x)], rs(1))
        block = ref.at[row_block(start, half), col_block(across_x)]
        go(block, block, ss(3), rs(3), sp, across_y)
        landed(ref.at[row_block(start, size), col_block(across_y)], rs(2))
        block = ref.at[row_block(start + half, half), col_block(across_y)]
        go(block, block, ss(0), rs(0), sp, across_x)

    def spread_finish(ref, start, size, rs):
        half = size // 2
        landed(ref.at[row_block(start, half), col_block(diagonal)], rs(3))
        landed(ref.at[row_block(start + half, half), col_block(diagonal)], rs(0))

    def stats_start(i, first, second):
        lane = lax.broadcasted_iota(jnp.int32, (first.shape[0], 128), 1)
        both = jnp.where(lane == 0, first, jnp.where(lane == 1, second, 0.0))
        if first.shape[0] < 128:
            both = jnp.concatenate([both, jnp.zeros((128 - first.shape[0], 128), jnp.float32)], 0)
        stats[i, 0] = jnp.transpose(both)[0:8]
        for j in range(1, n_tp):
            go(
                stats.at[i, 0],
                stats.at[i, j],
                stat_send.at[i, j],
                stat_recv.at[i, j],
                sp,
                (tp + j) % n_tp,
            )

    def stats_total(i):
        total = stats[i, 0]
        for j in range(1, n_tp):
            landed(stats.at[i, j], stat_recv.at[i, j])
            total = total + stats[i, j]
        return total

    def gain_row(ref):
        return jnp.concatenate(
            [ref[i : i + 1, :].astype(jnp.float32) for i in range(cols // 128)], 1
        )

    gated = (
        conv_value[...].astype(jnp.float32) * jax.nn.sigmoid(conv_gate[...].astype(jnp.float32))
    ).astype(jnp.bfloat16)
    extended[pl.ds(pad, rows), :] = gated.astype(jnp.float32)
    tail[...] = gated[rows - pad :]
    doc_rows = jnp.transpose(jnp.broadcast_to(docs[...].astype(jnp.float32), (128, rows)))
    doc_extended[pl.ds(pad, rows), :] = doc_rows
    tail_docs[...] = doc_rows[rows - pad :]
    taps[...] = conv_kernel[...].astype(jnp.float32)
    plans[sp] = jnp.concatenate(
        [routes[...].astype(jnp.float32), route_weight[...], jnp.zeros((4, rows), jnp.float32)], 0
    )
    pl.semaphore_wait(barrier, n_sp - 1 + n_tp - 1)
    next_sp = (sp + 1) % n_sp
    go(tail, halo, halo_send.at[0], halo_recv.at[0], next_sp, tp)
    go(tail_docs, halo_docs, halo_send.at[1], halo_recv.at[1], next_sp, tp)
    for i in range(1, n_sp):
        go(plans.at[sp], plans.at[sp], plan_send.at[i], plan_recv.at[sp], (sp + i) % n_sp, tp)

    part = strip

    def convolve(r):
        here = pl.ds(r * part, part)
        own = doc_extended[pl.ds(pad + r * part, part), :]
        count = jnp.zeros((part, 128), jnp.float32)
        for back in range(1, lookback + 1):
            count = count + jnp.where(
                doc_extended[pl.ds(pad + r * part - back, part), :] == own, 1.0, 0.0
            )
        blocks = [pl.ds(c * 128, 128) for c in range(cols // 128)]
        totals = [jnp.zeros((part, 128), jnp.float32) for _ in blocks]
        for tap in range(lookback + 1):
            near = count >= lookback - tap
            rows_of_tap = pl.ds(pad - lookback + r * part + tap, part)
            for c, at in enumerate(blocks):
                value = extended[rows_of_tap, at] * taps[tap : tap + 1, at]
                totals[c] = totals[c] + jnp.where(near, value, 0.0)
        for c, at in enumerate(blocks):
            conv[here, at] = totals[c]

    def channel_stats(r):
        conv_out = conv[pl.ds(r * strip, strip), :]
        stats_start(
            r,
            jnp.sum(conv_out, 1, keepdims=True),
            jnp.sum(conv_out * conv_out, 1, keepdims=True),
        )

    def sems(ref, *index):
        return lambda i: ref.at[(*index, i)]

    def activate(r):
        here = pl.ds(r * strip, strip)
        back = jnp.transpose(jnp.concatenate([stats_total(r)] * 16, 0))[0:strip]
        mean = back[:, 0:1] / width
        scale = lax.rsqrt(back[:, 1:2] / width - mean * mean + epsilon)
        v = (conv[here, :] - mean) * scale * gain_row(ln_gain)
        activated[here, col_block(tp)] = (v * jax.nn.sigmoid(v)).astype(jnp.bfloat16)
        spread_start(activated, r * strip, strip, sems(act_send, r), sems(act_recv, r))

    def project(r, t):
        return jnp.dot(
            activated[pl.ds(r * strip, strip), col_block(t)],
            proj[col_block(t), :],
            preferred_element_type=jnp.float32,
        )

    for r in (3, 2, 1):
        convolve(r)
        channel_stats(r)
    activate(3)
    landed(halo, halo_recv.at[0])
    landed(halo_docs, halo_recv.at[1])
    inside = sp > 0
    extended[pl.ds(0, pad), :] = jnp.where(inside, halo[...].astype(jnp.float32), 0.0)
    doc_extended[pl.ds(0, pad), :] = jnp.where(inside, halo_docs[...], -1.0)
    convolve(0)
    channel_stats(0)
    for r in (2, 1, 0):
        activate(r)

    for i in range(1, n_sp):
        e = (sp + i) % n_sp
        landed(plans.at[e], plan_recv.at[e])
    token = lax.broadcasted_iota(jnp.int32, (rows, rows), 0)
    later = jnp.where(
        token < lax.broadcasted_iota(jnp.int32, (rows, rows), 1), 1.0, 0.0
    ).astype(jnp.bfloat16)
    slot_id = lax.broadcasted_iota(jnp.int32, (cap, rows), 0)

    def named_by(s, expert):
        plan = plans[s]
        first = plan[0:1] == expert
        second = plan[1:2] == expert
        weight = jnp.where(first, plan[2:3], 0.0) + jnp.where(second, plan[3:4], 0.0)
        return jnp.where(first | second, 1.0, 0.0), weight

    def slots_of(sources, expert):
        both = [named_by(s, expert) for s in sources]
        named = jnp.concatenate([n for n, _ in both] + [jnp.zeros_like(both[0][0])] * (8 - len(both)), 0)
        rank = jnp.dot(named.astype(jnp.bfloat16), later, preferred_element_type=jnp.float32)
        slot = jnp.where(named > 0.5, rank, -1.0).astype(jnp.int32)
        return [(slot[i : i + 1], weight) for i, (_, weight) in enumerate(both)]

    mine = slots_of([2 * p + core for p in range(planes)], sp.astype(jnp.float32))
    rest = slots_of([2 * p + 1 - core for p in range(planes)], sp.astype(jnp.float32))
    other = slots_of([2 * p + core for p in range(planes)], twin.astype(jnp.float32))
    for p in range(planes):
        slot, weight = mine[p]
        picks[p, 0:cap] = jnp.where(slot == slot_id, 1.0, 0.0).astype(jnp.bfloat16)
        own_blend = jnp.where(slot == slot_id, weight, 0.0)
        slot, weight = rest[p]
        picks[p, cap : 2 * cap] = jnp.where(slot == slot_id, 1.0, 0.0).astype(jnp.bfloat16)
        slot, weight = other[p]
        twin_blend = jnp.where(slot == slot_id, weight, 0.0)
        blends[p] = jnp.transpose(jnp.concatenate([own_blend, twin_blend], 0)).astype(jnp.bfloat16)

    order = [0] + sorted(range(1, planes), key=lambda k: -min(k, planes - k))

    plane_order = {
        1: [(order[1], 1)],
        0: [(order[1], 0)] + [(k, q) for k in order[2:] for q in (1, 0) if (k, q) != (order[-1], 0)],
    }

    def source(k):
        return (plane + k) % planes * 2 + core

    def first_row(k, q):
        return source(k) * rows + q * chunk

    def relay_strip(r):
        spread_relay(activated, r * strip, strip, sems(act_send, r), sems(act_recv, r))
        here = pl.ds(r * strip, strip)
        projected[here, :] += project(r, across_x) + project(r, across_y)

    def settle(r):
        here = pl.ds(r * strip, strip)
        spread_finish(activated, r * strip, strip, sems(act_recv, r))
        total = projected[here, :] + project(r, diagonal)
        stream_rows = (
            residual[here, :].astype(jnp.float32)
            + total.astype(jnp.bfloat16).astype(jnp.float32)
        ).astype(jnp.bfloat16)
        stream[here, :] = stream_rows
        tokens[row_block(sp * rows + r * strip, strip), col_block(tp)] = (
            stream_rows.astype(jnp.float32) * gain_row(norm_gain)
        ).astype(jnp.bfloat16)

    def send_tokens(q):
        spread_start(
            tokens, first_row(0, q), chunk, sems(spread_send, 0, q), sems(spread_recv, 0, q)
        )
        for k, part_q in plane_order[q]:
            block = tokens.at[row_block(first_row(0, part_q), chunk), col_block(tp)]
            go(
                block,
                block,
                plane_send.at[k, part_q],
                plane_recv.at[k, part_q],
                (plane - k + planes) % planes * 2 + core,
                tp,
            )
        stream_part = stream[pl.ds(q * chunk, chunk), :].astype(jnp.float32)
        square = jnp.sum(stream_part * stream_part, 1, keepdims=True)
        stats_start(4 + q, square, square)

    loads[0].wait()
    for r in (3, 2, 1, 0):
        projected[pl.ds(r * strip, strip), :] = project(r, tp)
    relay_strip(3)
    relay_strip(2)
    settle(3)
    relay_strip(1)
    settle(2)
    send_tokens(1)
    relay_strip(0)
    settle(1)
    settle(0)
    send_tokens(0)

    def spread(k, q):
        block = tokens.at[row_block(first_row(k, q), chunk), col_block(tp)]
        landed(block, plane_recv.at[k, q])
        spread_start(tokens, first_row(k, q), chunk, sems(spread_send, k, q), sems(spread_recv, k, q))

    def relay(k, q):
        spread_relay(tokens, first_row(k, q), chunk, sems(spread_send, k, q), sems(spread_recv, k, q))

    def send_wide():
        k = order[-1]
        block = tokens.at[row_block(first_row(0, 0), chunk), :]
        go(
            block,
            block,
            plane_send.at[k, 0],
            plane_recv.at[k, 0],
            (plane - k + planes) % planes * 2 + core,
            tp,
        )

    def finish(k, q):
        block = tokens.at[row_block(first_row(k, q), chunk), :]
        if (k, q) == (order[-1], 0):
            landed(block, plane_recv.at[k, q])
        else:
            spread_finish(tokens, first_row(k, q), chunk, sems(spread_recv, k, q))
        go(block, block, twin_send.at[k, q], twin_recv.at[k, q], twin, tp)

    def share_scales():
        for q in range(2):
            scales[sp, :, pl.ds(q * chunk, chunk)] = lax.rsqrt(
                stats_total(4 + q) / width + epsilon
            )
        for i in range(1, n_sp):
            go(
                scales.at[sp],
                scales.at[sp],
                scale_send.at[i],
                scale_recv.at[sp],
                (sp + i) % n_sp,
                tp,
            )

    def gather(k):
        p = (plane + k) % planes
        for q in range(2):
            start = (2 * p + 1 - core) * rows + q * chunk
            landed(tokens.at[row_block(start, chunk), :], twin_recv.at[k, q])
        for j in range(2):
            s = 2 * p + (core if j == 0 else 1 - core)
            if k == 0 and j == 0:
                pass
            else:
                landed(scales.at[s], scale_recv.at[s])
            here = pl.ds(j * cap, cap)
            pick = picks[p, here, :]
            slots[here, :] = jnp.dot(
                pick, tokens[row_block(s * rows, rows), :], preferred_element_type=jnp.float32
            ).astype(jnp.bfloat16)
            scale = jnp.sum(pick.astype(jnp.float32) * scales[s][0:1, :], 1, keepdims=True)
            since[here, :] = jnp.broadcast_to(scale, (cap, 128))

    def raise_up(k, piece):
        size = gate.shape[1] // 2
        at = pl.ds(piece * size, size)
        scale = jnp.concatenate([since[0 : 2 * cap, :]] * (size // 128), 1)
        g = scale * jnp.dot(slots[...], gate[:, at], preferred_element_type=jnp.float32)
        u = scale * jnp.dot(slots[...], up[:, at], preferred_element_type=jnp.float32)
        hidden[:, at] = (g * jax.nn.sigmoid(g) * u).astype(jnp.bfloat16)

    def bring_down(k, piece):
        size = width // 2
        at = pl.ds(piece * size, size)
        result = jnp.dot(
            hidden[...], down[:, at], preferred_element_type=jnp.float32
        ).astype(jnp.bfloat16)
        pairs[k, 0:cap, at] = result[0:cap]
        outbound[k, :, at] = result[cap:]
        if piece == 1:
            go(
                outbound.at[k],
                pairs.at[k, pl.ds(cap, cap), :],
                swap_send.at[k],
                swap_recv.at[k],
                twin,
                tp,
            )

    low, high = pl.ds(0, chunk), pl.ds(chunk, chunk)

    def combine(k):
        p = (plane + k) % planes
        landed(pairs.at[k, pl.ds(cap, cap), :], swap_recv.at[k])

        blended[k] = jnp.dot(
            blends[p], pairs[k], preferred_element_type=jnp.float32
        ).astype(jnp.bfloat16)

        for i, (part_rows, block, peer) in enumerate(
            (
                (low, diagonal, across_x),
                (high, diagonal, across_y),
                (low, across_x, across_x),
                (high, across_y, across_y),
            )
        ):
            go(
                blended.at[k, part_rows, col_block(block)],
                arrived.at[k, i, low],
                sum_send.at[k, i],
                sum_recv.at[k, i],
                sp,
                peer,
            )

    def pass_on(k):
        for i, (part_rows, peer) in enumerate(((low, across_y), (high, across_x))):
            landed(arrived.at[k, i, low], sum_recv.at[k, i])
            arrived[k, 2 + i, high] = (
                blended[k, part_rows, col_block(peer)].astype(jnp.float32)
                + arrived[k, i, low].astype(jnp.float32)
            ).astype(jnp.bfloat16)
            go(
                arrived.at[k, 2 + i, high],
                arrived.at[k, i, high],
                sum_send.at[k, 4 + i],
                sum_recv.at[k, 4 + i],
                sp,
                peer,
            )

    def give_back(k):
        for i, part_rows in enumerate((low, high)):
            landed(arrived.at[k, 2 + i, low], sum_recv.at[k, 2 + i])
            landed(arrived.at[k, i, high], sum_recv.at[k, 4 + i])
            total = (
                blended[k, part_rows, col_block(tp)].astype(jnp.float32)
                + arrived[k, 2 + i, low].astype(jnp.float32)
                + arrived[k, i, high].astype(jnp.float32)
            )
            if k == 0:
                here = pl.ds(i * chunk, chunk)
                total = total + stream[here, :].astype(jnp.float32)
                for j in order[1:]:
                    landed(returned.at[j, part_rows], back_recv.at[j, i])
                    total = total + returned[j, part_rows].astype(jnp.float32)
                mixed[here, :] = total.astype(jnp.bfloat16)
            else:
                summed[k, part_rows] = total.astype(jnp.bfloat16)
                go(
                    summed.at[k, part_rows],
                    returned.at[k, part_rows],
                    back_send.at[k, i],
                    back_recv.at[k, i],
                    source(k),
                    tp,
                )

    def weights_ready():
        for load in loads[1:]:
            load.wait()

    steps = {
        "R": relay,
        "S": spread,
        "F": finish,
        "G": gather,
        "U": raise_up,
        "D": bring_down,
        "C": combine,
        "P": pass_on,
        "V": give_back,
        "B": send_wide,
        "H": share_scales,
        "L": weights_ready,
    }
    for word in schedule:
        indices = [int(digit) for digit in word[1:]]
        steps[word[0]](*[order[i] for i in indices[:1]], *indices[1:])
    for send in sends:
        send.wait_send()


def fused(operands, rows, cols, n_sp, n_tp, cap, width, units, taps):
    planes = n_sp // 2
    pad = (taps - 1 + 15) // 16 * 16
    chunk = rows // 2
    bf16, f32 = jnp.bfloat16, jnp.float32
    dma = pltpu.SemaphoreType.DMA
    vmem = pl.BlockSpec(memory_space=pltpu.VMEM)
    anywhere = pl.BlockSpec(memory_space=pl.ANY)
    return pl.pallas_call(
        functools.partial(fused_kernel, n_sp, n_tp, cap),
        out_shape=jax.ShapeDtypeStruct((rows, cols), bf16),
        in_specs=[vmem] * 9 + [anywhere] * 4,
        out_specs=vmem,
        scratch_shapes=[
            pltpu.VMEM((width, cols), bf16),
            pltpu.VMEM((width, units), bf16),
            pltpu.VMEM((width, units), bf16),
            pltpu.VMEM((units, width), bf16),
            pltpu.VMEM((taps, cols), f32),
            pltpu.VMEM((pad + rows, cols), f32),
            pltpu.VMEM((pad + rows, 128), f32),
            pltpu.VMEM((max(rows, 2 * cap), 128), f32),
            pltpu.VMEM((rows, cols), f32),
            pltpu.VMEM((pad, cols), bf16),
            pltpu.VMEM((pad, 128), f32),
            pltpu.VMEM((pad, cols), bf16),
            pltpu.VMEM((pad, 128), f32),
            pltpu.VMEM((6, n_tp, 8, 128), f32),
            pltpu.VMEM((n_sp, 8, rows), f32),
            pltpu.VMEM((n_sp, 8, rows), f32),
            pltpu.VMEM((rows, width), bf16),
            pltpu.VMEM((rows, cols), f32),
            pltpu.VMEM((rows, cols), bf16),
            pltpu.VMEM((n_sp * rows, width), bf16),
            pltpu.VMEM((planes, 2 * cap, rows), bf16),
            pltpu.VMEM((planes, rows, 2 * cap), bf16),
            pltpu.VMEM((2 * cap, width), bf16),
            pltpu.VMEM((2 * cap, units), bf16),
            pltpu.VMEM((planes, 2 * cap, width), bf16),
            pltpu.VMEM((planes, cap, width), bf16),
            pltpu.VMEM((planes, rows, width), bf16),
            pltpu.VMEM((planes, 4, rows, cols), bf16),
            pltpu.VMEM((planes, rows, cols), bf16),
            pltpu.VMEM((planes, rows, cols), bf16),
            dma((4,)),
            dma((2,)),
            dma((2,)),
            dma((6, n_tp)),
            dma((6, n_tp)),
            dma((n_sp,)),
            dma((n_sp,)),
            dma((n_sp,)),
            dma((n_sp,)),
            dma((4, 4)),
            dma((4, 4)),
            dma((planes, 2)),
            dma((planes, 2)),
            dma((planes, 2, 4)),
            dma((planes, 2, 4)),
            dma((planes, 2)),
            dma((planes, 2)),
            dma((planes,)),
            dma((planes,)),
            dma((planes, 6)),
            dma((planes, 6)),
            dma((planes, 2)),
            dma((planes, 2)),
        ],
        compiler_params=pltpu.CompilerParams(
            collective_id=0, has_side_effects=True, vmem_limit_bytes=56 << 20
        ),
    )(*operands)


def per_device(
    residual_in,
    conv_value,
    conv_gate,
    doc_ids,
    conv_kernel,
    ln_gain,
    out_weight,
    norm_gain,
    routes,
    route_weight,
    gate_w,
    up_w,
    down_w,
):
    rows, cols = residual_in.shape
    n_sp = lax.axis_size("sp")
    n_tp = lax.axis_size("tp")
    cap = 4 * rows // n_sp
    _, width, units = gate_w.shape
    group_rows = n_sp // groups * cap
    taps = conv_kernel.shape[0]
    pad = (taps - 1 + 15) // 16 * 16
    if n_tp == 4 and n_sp == 8:
        operands = (
            residual_in,
            conv_value,
            conv_gate,
            doc_ids.reshape(1, rows),
            conv_kernel,
            ln_gain.reshape(cols // 128, 128),
            norm_gain.reshape(cols // 128, 128),
            routes.T,
            route_weight.T,
            out_weight,
            gate_w[0],
            up_w[0],
            down_w[0],
        )
        return fused(operands, rows, cols, n_sp, n_tp, cap, width, units, taps)
    bf16, f32 = jnp.bfloat16, jnp.float32
    dma = pltpu.SemaphoreType.DMA
    vmem = pl.BlockSpec(memory_space=pltpu.VMEM)
    anywhere = pl.BlockSpec(memory_space=pl.ANY)
    return pl.pallas_call(
        functools.partial(layer_kernel, n_sp, n_tp, cap),
        out_shape=jax.ShapeDtypeStruct((rows, cols), bf16),
        in_specs=[vmem] * 9 + [anywhere] * 4,
        out_specs=vmem,
        scratch_shapes=[
            pltpu.VMEM((width, cols), bf16),
            pltpu.VMEM((width, units), bf16),
            pltpu.VMEM((width, units), bf16),
            pltpu.VMEM((units, width), bf16),
            pltpu.VMEM((taps, cols), f32),
            pltpu.VMEM((pad + rows, cols), f32),
            pltpu.VMEM((pad + rows, 128), f32),
            pltpu.VMEM((rows, 128), f32),
            pltpu.VMEM((rows, cols), f32),
            pltpu.VMEM((pad, cols), bf16),
            pltpu.VMEM((pad, 128), f32),
            pltpu.VMEM((pad, cols), bf16),
            pltpu.VMEM((pad, 128), f32),
            pltpu.VMEM((2, n_tp, 8, rows), f32),
            pltpu.VMEM((rows, width), bf16),
            pltpu.VMEM((rows, cols), f32),
            pltpu.VMEM((rows, cols), bf16),
            pltpu.VMEM((rows, cols), bf16),
            pltpu.VMEM((n_sp, rows, cap), bf16),
            pltpu.VMEM((n_sp, cap, cols), bf16),
            pltpu.VMEM((n_sp * cap, width), bf16),
            pltpu.VMEM((group_rows, units), bf16),
            pltpu.VMEM((groups, group_rows, width), bf16),
            pltpu.VMEM((groups, n_tp, group_rows, cols), bf16),
            pltpu.VMEM((groups, group_rows, cols), bf16),
            pltpu.VMEM((n_sp, cap, cols), bf16),
            pltpu.VMEM((n_sp, rows, cap), bf16),
            pltpu.VMEM((n_sp, rows, cap), bf16),
            dma((4,)),
            dma((2,)),
            dma((2,)),
            dma((2, n_tp)),
            dma((2, n_tp)),
            dma((n_tp,)),
            dma((n_tp,)),
            dma((n_sp,)),
            dma((n_sp,)),
            dma((groups, n_tp)),
            dma((groups, n_tp)),
            dma((groups, n_tp + 2)),
            dma((groups, n_tp + 2)),
            dma((n_sp,)),
            dma((n_sp,)),
        ],
        compiler_params=pltpu.CompilerParams(
            collective_id=0, has_side_effects=True, vmem_limit_bytes=54 << 20
        ),
    )(
        residual_in,
        conv_value,
        conv_gate,
        doc_ids.reshape(1, rows),
        conv_kernel,
        ln_gain.reshape(1, cols),
        norm_gain.reshape(1, cols),
        routes,
        route_weight,
        out_weight,
        gate_w[0],
        up_w[0],
        down_w[0],
    )


def solution(mesh):
    in_specs = (
        P("sp", "tp"),
        P("sp", "tp"),
        P("sp", "tp"),
        P("sp"),
        P(None, "tp"),
        P("tp"),
        P(None, "tp"),
        P("tp"),
        P("sp", None),
        P("sp", None),
        P("sp", None, "tp"),
        P("sp", None, "tp"),
        P("sp", "tp", None),
    )
    out_specs = P("sp", "tp")
    return jax.shard_map(
        per_device, mesh=mesh, in_specs=in_specs, out_specs=out_specs, check_vma=False
    )
```

```python
import functools

import jax
import jax.numpy as jnp
from jax import lax
from jax.experimental import pallas as pl
from jax.experimental.pallas import tpu as pltpu
from jax.sharding import PartitionSpec as P

epsilon = 1e-06
groups = 4


def transposed_dot(a, b):
    return lax.dot_general(a, b, (((0,), (0,)), ((), ())), preferred_element_type=jnp.float32)


def remote(src, dst, send_sem, recv_sem, sp, tp):
    return pltpu.make_async_remote_copy(
        src_ref=src,
        dst_ref=dst,
        send_sem=send_sem,
        recv_sem=recv_sem,
        device_id=(sp, tp),
        device_id_type=pl.DeviceIdType.MESH,
    )


def layer_kernel(
    n_sp,
    n_tp,
    cap,
    residual,
    conv_value,
    conv_gate,
    docs,
    conv_kernel,
    ln_gain,
    norm_gain,
    routes,
    route_weight,
    proj_hbm,
    gate_hbm,
    up_hbm,
    down_hbm,
    mixed,
    proj,
    gate,
    up,
    down,
    taps,
    extended,
    doc_extended,
    since,
    conv,
    tail,
    tail_docs,
    halo,
    halo_docs,
    stats,
    activated,
    projected,
    stream,
    normed,
    chosen,
    outbound,
    slots,
    hidden,
    partial,
    arrived,
    summed,
    returned,
    weight_hi,
    weight_lo,
    local_sem,
    halo_send,
    halo_recv,
    stat_send,
    stat_recv,
    act_send,
    act_recv,
    out_send,
    out_recv,
    spread_send,
    spread_recv,
    sum_send,
    sum_recv,
    back_send,
    back_recv,
):
    sp = lax.axis_index("sp")
    tp = lax.axis_index("tp")
    rows, cols = residual.shape
    width = cols * n_tp
    lookback = conv_kernel.shape[0] - 1
    pad = tail.shape[0]
    per_group = n_sp // groups
    group_rows = per_group * cap
    my_group = sp // per_group
    my_member = sp % per_group
    relays = n_tp == 4
    across_x = tp + 1 - 2 * (tp % 2)
    across_y = (tp + 2) % n_tp
    diagonal = (across_x + 2) % n_tp
    loads = [
        pltpu.make_async_copy(src, dst, local_sem.at[i])
        for i, (src, dst) in enumerate(
            ((proj_hbm, proj), (gate_hbm, gate), (up_hbm, up), (down_hbm, down))
        )
    ]
    for load in loads:
        load.start()

    barrier = pltpu.get_barrier_semaphore()
    for i in range(1, n_sp):
        pl.semaphore_signal(
            barrier, inc=1, device_id=((sp + i) % n_sp, tp), device_id_type=pl.DeviceIdType.MESH
        )
    for i in range(1, n_tp):
        pl.semaphore_signal(
            barrier, inc=1, device_id=(sp, (tp + i) % n_tp), device_id_type=pl.DeviceIdType.MESH
        )
    sends = []

    def go(*args):
        send = remote(*args)
        send.start()
        sends.append(send)

    def landed(ref, sem):
        remote(ref, ref, act_send.at[0], sem, sp, tp).wait_recv()

    def col_block(t):
        return pl.ds(pl.multiple_of(t * cols, 128), cols)

    def spread_start(ref, start, size, ss, rs):
        block = ref.at[pl.ds(start, size), col_block(tp)]
        if relays:
            go(block, block, ss(1), rs(1), sp, across_x)
            go(block, block, ss(2), rs(2), sp, across_y)
        else:
            for j in range(1, n_tp):
                go(block, block, ss(j), rs(j), sp, (tp + j) % n_tp)

    def spread_relay(ref, start, size, ss, rs):
        if relays:
            half = size // 2
            landed(ref.at[pl.ds(start, size), col_block(across_x)], rs(1))
            block = ref.at[pl.ds(start, half), col_block(across_x)]
            go(block, block, ss(3), rs(3), sp, across_y)
            landed(ref.at[pl.ds(start, size), col_block(across_y)], rs(2))
            block = ref.at[pl.ds(start + half, half), col_block(across_y)]
            go(block, block, ss(0), rs(0), sp, across_x)

    def spread_finish(ref, start, size, rs):
        if relays:
            half = size // 2
            landed(ref.at[pl.ds(start, half), col_block(diagonal)], rs(3))
            landed(ref.at[pl.ds(start + half, half), col_block(diagonal)], rs(0))
        else:
            for j in range(1, n_tp):
                landed(
                    ref.at[pl.ds(start, size), col_block((tp - j + n_tp) % n_tp)], rs(j)
                )

    def stats_start(i, first, second):
        lane = lax.broadcasted_iota(jnp.int32, (rows, 128), 1)
        both = jnp.where(lane == 0, first, jnp.where(lane == 1, second, 0.0))
        stats[i, 0] = jnp.transpose(both)[0:8]
        for j in range(1, n_tp):
            go(
                stats.at[i, 0],
                stats.at[i, j],
                stat_send.at[i, j],
                stat_recv.at[i, j],
                sp,
                (tp + j) % n_tp,
            )

    def stats_finish(i):
        total = stats[i, 0]
        for j in range(1, n_tp):
            landed(stats.at[i, j], stat_recv.at[i, j])
            total = total + stats[i, j]
        back = jnp.transpose(jnp.concatenate([total] * 16, 0))
        return back[:, 0:1], back[:, 1:2]

    gated = (
        conv_value[...].astype(jnp.float32) * jax.nn.sigmoid(conv_gate[...].astype(jnp.float32))
    ).astype(jnp.bfloat16)
    extended[pl.ds(pad, rows), :] = gated.astype(jnp.float32)
    tail[...] = gated[rows - pad :]
    doc_rows = jnp.transpose(
        jnp.broadcast_to(docs[...].astype(jnp.float32), (128, rows))
    )
    doc_extended[pl.ds(pad, rows), :] = doc_rows
    tail_docs[...] = doc_rows[rows - pad :]
    taps[...] = conv_kernel[...].astype(jnp.float32)
    pl.semaphore_wait(barrier, n_sp - 1 + n_tp - 1)
    next_sp = (sp + 1) % n_sp
    tails = [
        remote(tail, halo, halo_send.at[0], halo_recv.at[0], next_sp, tp),
        remote(tail_docs, halo_docs, halo_send.at[1], halo_recv.at[1], next_sp, tp),
    ]
    for send in tails:
        send.start()
        sends.append(send)

    part = min(64, rows)

    def convolve(r):
        here = pl.ds(r * part, part)
        own = doc_extended[pl.ds(pad + r * part, part), :]
        count = jnp.zeros((part, 128), jnp.float32)
        for back in range(1, lookback + 1):
            count = count + jnp.where(
                doc_extended[pl.ds(pad + r * part - back, part), :] == own, 1.0, 0.0
            )
        since[here, :] = count

        @pl.loop(0, cols // 128)
        def _(c):
            at = pl.ds(pl.multiple_of(c * 128, 128), 128)
            reach = since[here, :]
            total = jnp.zeros((part, 128), jnp.float32)
            for tap in range(lookback + 1):
                value = extended[pl.ds(pad - lookback + r * part + tap, part), at]
                total = total + jnp.where(
                    reach >= lookback - tap, value * taps[tap : tap + 1, at], 0.0
                )
            conv[here, at] = total

    for r in range(1, rows // part):
        convolve(r)
    landed(halo, halo_recv.at[0])
    landed(halo_docs, halo_recv.at[1])
    inside = sp > 0
    extended[pl.ds(0, pad), :] = jnp.where(inside, halo[...].astype(jnp.float32), 0.0)
    doc_extended[pl.ds(0, pad), :] = jnp.where(inside, halo_docs[...], -1.0)
    convolve(0)
    conv_out = conv[...]
    stats_start(
        0,
        jnp.sum(conv_out, 1, keepdims=True),
        jnp.sum(conv_out * conv_out, 1, keepdims=True),
    )

    expert_id = lax.broadcasted_iota(jnp.int32, (rows, n_sp), 1)
    first = routes[:, 0:1] == expert_id
    second = routes[:, 1:2] == expert_id
    named = jnp.where(first | second, 1.0, 0.0)
    earlier = jnp.where(
        lax.broadcasted_iota(jnp.int32, (rows, rows), 1)
        < lax.broadcasted_iota(jnp.int32, (rows, rows), 0),
        1.0,
        0.0,
    ).astype(jnp.bfloat16)
    rank = jnp.dot(earlier, named.astype(jnp.bfloat16), preferred_element_type=jnp.float32)
    slot = jnp.where(first | second, rank, -1.0).astype(jnp.int32)
    weight = jnp.where(first, route_weight[:, 0:1], 0.0) + jnp.where(
        second, route_weight[:, 1:2], 0.0
    )
    slot_id = lax.broadcasted_iota(jnp.int32, (rows, cap), 1)
    for e in range(n_sp):
        chosen[e] = jnp.where(slot[:, e : e + 1] == slot_id, 1.0, 0.0).astype(jnp.bfloat16)

    channel_sum, channel_sq = stats_finish(0)
    mean = channel_sum / width
    scale = lax.rsqrt(channel_sq / width - mean * mean + epsilon)
    v = (conv[...] - mean) * scale * ln_gain[...].astype(jnp.float32)
    activated[:, col_block(tp)] = (v * jax.nn.sigmoid(v)).astype(jnp.bfloat16)

    def act_block(i):
        return act_send.at[i]

    def act_arrival(i):
        return act_recv.at[i]

    spread_start(activated, 0, rows, act_block, act_arrival)
    loads[0].wait()

    def project(t):
        return jnp.dot(
            activated[:, col_block(t)],
            proj[pl.ds(pl.multiple_of(t * cols, 128), cols), :],
            preferred_element_type=jnp.float32,
        )

    projected[...] = project(tp)
    for e in range(n_sp):
        at = jnp.where(slot[:, e : e + 1] == slot_id, weight[:, e : e + 1], 0.0)
        hi = at.astype(jnp.bfloat16)
        weight_hi[e] = hi
        weight_lo[e] = (at - hi.astype(jnp.float32)).astype(jnp.bfloat16)
    spread_relay(activated, 0, rows, act_block, act_arrival)
    if relays:
        projected[...] += project(across_x) + project(across_y)
    spread_finish(activated, 0, rows, act_arrival)
    if relays:
        projected[...] += project(diagonal)
    else:
        for j in range(1, n_tp):
            projected[...] += project((tp + j) % n_tp)
    stream[...] = (
        residual[...].astype(jnp.float32)
        + projected[...].astype(jnp.bfloat16).astype(jnp.float32)
    ).astype(jnp.bfloat16)
    stream_part = stream[...].astype(jnp.float32)
    square = jnp.sum(stream_part * stream_part, 1, keepdims=True)
    stats_start(1, square, square)
    row_total, _ = stats_finish(1)
    normed[...] = (
        stream[...].astype(jnp.float32)
        * lax.rsqrt(row_total / width + epsilon)
        * norm_gain[...].astype(jnp.float32)
    ).astype(jnp.bfloat16)

    def source_rows(s):
        return pl.ds(pl.multiple_of(s * cap, cap), cap)

    def group_start(k):
        return pl.multiple_of((my_group + k) % groups * group_rows, group_rows)

    for k in range(groups):
        for j in range(per_group):
            dest = (my_group - k + groups) % groups * per_group + (my_member + j) % per_group
            rows_out = transposed_dot(chosen[dest], normed[...]).astype(jnp.bfloat16)
            if k == 0 and j == 0:
                slots[source_rows(sp), col_block(tp)] = rows_out
                continue
            outbound[dest] = rows_out
            go(
                outbound.at[dest],
                slots.at[source_rows(sp), col_block(tp)],
                out_send.at[k * per_group + j],
                out_recv.at[sp],
                dest,
                tp,
            )

    def spread_sems(sems, k):
        return lambda i: sems.at[k, i]

    def spread(k):
        for j in range(per_group):
            if k == 0 and j == 0:
                continue
            source = (my_group + k) % groups * per_group + (my_member + j) % per_group
            landed(slots.at[source_rows(source), col_block(tp)], out_recv.at[source])
        spread_start(
            slots, group_start(k), group_rows, spread_sems(spread_send, k), spread_sems(spread_recv, k)
        )

    def relay(k):
        spread_relay(
            slots, group_start(k), group_rows, spread_sems(spread_send, k), spread_sems(spread_recv, k)
        )

    half = group_rows // 2
    low, high = pl.ds(0, half), pl.ds(half, half)

    def compute(k):
        spread_finish(slots, group_start(k), group_rows, spread_sems(spread_recv, k))
        x = pl.ds(group_start(k), group_rows)
        units = gate.shape[1]
        tile = min(256, units)

        @pl.loop(0, units // tile)
        def _(n):
            at = pl.ds(pl.multiple_of(n * tile, tile), tile)
            g = jnp.dot(slots[x, :], gate[:, at], preferred_element_type=jnp.float32)
            u = jnp.dot(slots[x, :], up[:, at], preferred_element_type=jnp.float32)
            hidden[:, at] = (g * jax.nn.sigmoid(g) * u).astype(jnp.bfloat16)

        @pl.loop(0, width // 256)
        def _(n):
            at = pl.ds(pl.multiple_of(n * 256, 256), 256)
            partial[k, :, at] = jnp.dot(
                hidden[...], down[:, at], preferred_element_type=jnp.float32
            ).astype(jnp.bfloat16)

        if relays:
            for i, (part_rows, block, peer) in enumerate(
                (
                    (low, across_x, across_x),
                    (low, diagonal, across_x),
                    (high, across_y, across_y),
                    (high, diagonal, across_y),
                )
            ):
                go(
                    partial.at[k, part_rows, col_block(block)],
                    arrived.at[k, i, low],
                    sum_send.at[k, i],
                    sum_recv.at[k, i],
                    sp,
                    peer,
                )
        else:
            for j in range(1, n_tp):
                peer = (tp + j) % n_tp
                go(
                    partial.at[k, :, col_block(peer)],
                    arrived.at[k, j],
                    sum_send.at[k, j],
                    sum_recv.at[k, j],
                    sp,
                    peer,
                )

    def pass_on(k):
        if relays:
            for i, (part_rows, peer) in enumerate(((low, across_y), (high, across_x))):
                landed(arrived.at[k, 2 * i + 1, low], sum_recv.at[k, 2 * i + 1])
                arrived[k, 2 + i, high] = (
                    partial[k, part_rows, col_block(peer)].astype(jnp.float32)
                    + arrived[k, 2 * i + 1, low].astype(jnp.float32)
                ).astype(jnp.bfloat16)
                go(
                    arrived.at[k, 2 + i, high],
                    arrived.at[k, i, high],
                    sum_send.at[k, 4 + i],
                    sum_recv.at[k, 4 + i],
                    sp,
                    peer,
                )

    def give_back(k):
        if relays:
            for i, part_rows in enumerate((low, high)):
                landed(arrived.at[k, 2 * i, low], sum_recv.at[k, 2 * i])
                landed(arrived.at[k, i, high], sum_recv.at[k, 4 + i])
                summed[k, part_rows] = (
                    partial[k, part_rows, col_block(tp)].astype(jnp.float32)
                    + arrived[k, 2 * i, low].astype(jnp.float32)
                    + arrived[k, i, high].astype(jnp.float32)
                ).astype(jnp.bfloat16)
        else:
            total = partial[k, :, col_block(tp)].astype(jnp.float32)
            for j in range(1, n_tp):
                landed(arrived.at[k, j], sum_recv.at[k, j])
                total = total + arrived[k, j].astype(jnp.float32)
            summed[k] = total.astype(jnp.bfloat16)
        for j in range(per_group):
            member = (my_member + j) % per_group
            source = (my_group + k) % groups * per_group + member
            part = pl.ds(pl.multiple_of(member * cap, cap), cap)
            if k == 0 and j == 0:
                returned[sp] = summed[k, part, :]
                continue
            go(
                summed.at[k, part, :],
                returned.at[sp],
                back_send.at[k * per_group + j],
                back_recv.at[sp],
                source,
                tp,
            )

    spread(0)
    spread(1)
    relay(0)
    spread(2)
    relay(1)
    for load in loads[1:]:
        load.wait()
    compute(0)
    spread(3)
    relay(2)
    compute(1)
    pass_on(0)
    relay(3)
    compute(2)
    pass_on(1)
    give_back(0)
    compute(3)
    pass_on(2)
    give_back(1)
    pass_on(3)
    give_back(2)
    give_back(3)
    for i in range(1, n_sp):
        e = (sp + i) % n_sp
        landed(returned.at[e], back_recv.at[e])
    routed = jnp.zeros((rows, cols), jnp.float32)
    for e in range(n_sp):
        routed = routed + jnp.dot(weight_hi[e], returned[e], preferred_element_type=jnp.float32)
        routed = routed + jnp.dot(weight_lo[e], returned[e], preferred_element_type=jnp.float32)
    mixed[...] = (stream[...].astype(jnp.float32) + routed).astype(jnp.bfloat16)
    for send in sends:
        send.wait_send()


schedule = (
    "R01", "H", "S11", "R00", "R11", "S10", "F00", "F01", "L", "S21", "G0", "U00", "R10", "U01", "F11", "D00", "S20", "F10", "S31", "R21", "D01", "B", "G1", "U11", "R20", "U10", "D10", "D11", "R31", "F21", "C1", "F20", "G2", "U20", "F31", "U21", "P1", "D20", "D21", "C2", "F30", "V1", "G3", "U30", "U31", "P2", "D30", "D31", "C3", "V2", "P3", "C0", "V3", "P0", "V0",
)


def fused_kernel(
    n_sp,
    n_tp,
    cap,
    residual,
    conv_value,
    conv_gate,
    docs,
    conv_kernel,
    ln_gain,
    norm_gain,
    routes,
    route_weight,
    proj_hbm,
    gate_hbm,
    up_hbm,
    down_hbm,
    mixed,
    proj,
    gate,
    up,
    down,
    taps,
    extended,
    doc_extended,
    since,
    conv,
    tail,
    tail_docs,
    halo,
    halo_docs,
    stats,
    plans,
    scales,
    activated,
    projected,
    stream,
    tokens,
    picks,
    blends,
    slots,
    hidden,
    pairs,
    outbound,
    blended,
    arrived,
    summed,
    returned,
    local_sem,
    halo_send,
    halo_recv,
    stat_send,
    stat_recv,
    plan_send,
    plan_recv,
    scale_send,
    scale_recv,
    act_send,
    act_recv,
    plane_send,
    plane_recv,
    spread_send,
    spread_recv,
    twin_send,
    twin_recv,
    swap_send,
    swap_recv,
    sum_send,
    sum_recv,
    back_send,
    back_recv,
):
    sp = lax.axis_index("sp")
    tp = lax.axis_index("tp")
    rows, cols = residual.shape
    width = cols * n_tp
    lookback = conv_kernel.shape[0] - 1
    pad = tail.shape[0]
    planes = n_sp // 2
    plane = sp // 2
    core = sp % 2
    twin = plane * 2 + 1 - core
    chunk = rows // 2
    strip = rows // 4
    across_x = tp + 1 - 2 * (tp % 2)
    across_y = (tp + 2) % n_tp
    diagonal = (across_x + 2) % n_tp
    loads = [
        pltpu.make_async_copy(src, dst, local_sem.at[i])
        for i, (src, dst) in enumerate(
            ((proj_hbm, proj), (gate_hbm, gate), (up_hbm, up), (down_hbm, down))
        )
    ]
    for load in loads:
        load.start()

    barrier = pltpu.get_barrier_semaphore()
    for i in range(1, n_sp):
        pl.semaphore_signal(
            barrier, inc=1, device_id=((sp + i) % n_sp, tp), device_id_type=pl.DeviceIdType.MESH
        )
    for i in range(1, n_tp):
        pl.semaphore_signal(
            barrier, inc=1, device_id=(sp, (tp + i) % n_tp), device_id_type=pl.DeviceIdType.MESH
        )
    sends = []

    def go(*args):
        send = remote(*args)
        send.start()
        sends.append(send)

    def landed(ref, sem):
        remote(ref, ref, act_send.at[0, 0], sem, sp, tp).wait_recv()

    def col_block(t):
        return pl.ds(pl.multiple_of(t * cols, 128), cols)

    def row_block(start, size):
        return pl.ds(pl.multiple_of(start, size), size)

    def spread_start(ref, start, size, ss, rs):
        block = ref.at[row_block(start, size), col_block(tp)]
        go(block, block, ss(1), rs(1), sp, across_x)
        go(block, block, ss(2), rs(2), sp, across_y)

    def spread_relay(ref, start, size, ss, rs):
        half = size // 2
        landed(ref.at[row_block(start, size), col_block(across_x)], rs(1))
        block = ref.at[row_block(start, half), col_block(across_x)]
        go(block, block, ss(3), rs(3), sp, across_y)
        landed(ref.at[row_block(start, size), col_block(across_y)], rs(2))
        block = ref.at[row_block(start + half, half), col_block(across_y)]
        go(block, block, ss(0), rs(0), sp, across_x)

    def spread_finish(ref, start, size, rs):
        half = size // 2
        landed(ref.at[row_block(start, half), col_block(diagonal)], rs(3))
        landed(ref.at[row_block(start + half, half), col_block(diagonal)], rs(0))

    def stats_start(i, first, second):
        lane = lax.broadcasted_iota(jnp.int32, (first.shape[0], 128), 1)
        both = jnp.where(lane == 0, first, jnp.where(lane == 1, second, 0.0))
        if first.shape[0] < 128:
            both = jnp.concatenate([both, jnp.zeros((128 - first.shape[0], 128), jnp.float32)], 0)
        stats[i, 0] = jnp.transpose(both)[0:8]
        for j in range(1, n_tp):
            go(
                stats.at[i, 0],
                stats.at[i, j],
                stat_send.at[i, j],
                stat_recv.at[i, j],
                sp,
                (tp + j) % n_tp,
            )

    def stats_total(i):
        total = stats[i, 0]
        for j in range(1, n_tp):
            landed(stats.at[i, j], stat_recv.at[i, j])
            total = total + stats[i, j]
        return total

    def gain_row(ref):
        return jnp.concatenate(
            [ref[i : i + 1, :].astype(jnp.float32) for i in range(cols // 128)], 1
        )

    gated = (
        conv_value[...].astype(jnp.float32) * jax.nn.sigmoid(conv_gate[...].astype(jnp.float32))
    ).astype(jnp.bfloat16)
    extended[pl.ds(pad, rows), :] = gated.astype(jnp.float32)
    tail[...] = gated[rows - pad :]
    doc_rows = jnp.transpose(jnp.broadcast_to(docs[...].astype(jnp.float32), (128, rows)))
    doc_extended[pl.ds(pad, rows), :] = doc_rows
    tail_docs[...] = doc_rows[rows - pad :]
    taps[...] = conv_kernel[...].astype(jnp.float32)
    plans[sp] = jnp.concatenate(
        [routes[...].astype(jnp.float32), route_weight[...], jnp.zeros((4, rows), jnp.float32)], 0
    )
    pl.semaphore_wait(barrier, n_sp - 1 + n_tp - 1)
    next_sp = (sp + 1) % n_sp
    go(tail, halo, halo_send.at[0], halo_recv.at[0], next_sp, tp)
    go(tail_docs, halo_docs, halo_send.at[1], halo_recv.at[1], next_sp, tp)
    for i in range(1, n_sp):
        go(plans.at[sp], plans.at[sp], plan_send.at[i], plan_recv.at[sp], (sp + i) % n_sp, tp)

    part = strip

    def convolve(r):
        here = pl.ds(r * part, part)
        own = doc_extended[pl.ds(pad + r * part, part), :]
        count = jnp.zeros((part, 128), jnp.float32)
        for back in range(1, lookback + 1):
            count = count + jnp.where(
                doc_extended[pl.ds(pad + r * part - back, part), :] == own, 1.0, 0.0
            )
        blocks = [pl.ds(c * 128, 128) for c in range(cols // 128)]
        totals = [jnp.zeros((part, 128), jnp.float32) for _ in blocks]
        for tap in range(lookback + 1):
            near = count >= lookback - tap
            rows_of_tap = pl.ds(pad - lookback + r * part + tap, part)
            for c, at in enumerate(blocks):
                value = extended[rows_of_tap, at] * taps[tap : tap + 1, at]
                totals[c] = totals[c] + jnp.where(near, value, 0.0)
        for c, at in enumerate(blocks):
            conv[here, at] = totals[c]

    def channel_stats(r):
        conv_out = conv[pl.ds(r * strip, strip), :]
        stats_start(
            r,
            jnp.sum(conv_out, 1, keepdims=True),
            jnp.sum(conv_out * conv_out, 1, keepdims=True),
        )

    def sems(ref, *index):
        return lambda i: ref.at[(*index, i)]

    def activate(r):
        here = pl.ds(r * strip, strip)
        back = jnp.transpose(jnp.concatenate([stats_total(r)] * 16, 0))[0:strip]
        mean = back[:, 0:1] / width
        scale = lax.rsqrt(back[:, 1:2] / width - mean * mean + epsilon)
        v = (conv[here, :] - mean) * scale * gain_row(ln_gain)
        activated[here, col_block(tp)] = (v * jax.nn.sigmoid(v)).astype(jnp.bfloat16)
        spread_start(activated, r * strip, strip, sems(act_send, r), sems(act_recv, r))

    def project(r, t):
        return jnp.dot(
            activated[pl.ds(r * strip, strip), col_block(t)],
            proj[col_block(t), :],
            preferred_element_type=jnp.float32,
        )

    for r in (3, 2, 1):
        convolve(r)
        channel_stats(r)
    activate(3)
    landed(halo, halo_recv.at[0])
    landed(halo_docs, halo_recv.at[1])
    inside = sp > 0
    extended[pl.ds(0, pad), :] = jnp.where(inside, halo[...].astype(jnp.float32), 0.0)
    doc_extended[pl.ds(0, pad), :] = jnp.where(inside, halo_docs[...], -1.0)
    convolve(0)
    channel_stats(0)
    for r in (2, 1, 0):
        activate(r)

    for i in range(1, n_sp):
        e = (sp + i) % n_sp
        landed(plans.at[e], plan_recv.at[e])
    token = lax.broadcasted_iota(jnp.int32, (rows, rows), 0)
    later = jnp.where(
        token < lax.broadcasted_iota(jnp.int32, (rows, rows), 1), 1.0, 0.0
    ).astype(jnp.bfloat16)
    slot_id = lax.broadcasted_iota(jnp.int32, (cap, rows), 0)

    def named_by(s, expert):
        plan = plans[s]
        first = plan[0:1] == expert
        second = plan[1:2] == expert
        weight = jnp.where(first, plan[2:3], 0.0) + jnp.where(second, plan[3:4], 0.0)
        return jnp.where(first | second, 1.0, 0.0), weight

    def slots_of(sources, expert):
        both = [named_by(s, expert) for s in sources]
        named = jnp.concatenate([n for n, _ in both] + [jnp.zeros_like(both[0][0])] * (8 - len(both)), 0)
        rank = jnp.dot(named.astype(jnp.bfloat16), later, preferred_element_type=jnp.float32)
        slot = jnp.where(named > 0.5, rank, -1.0).astype(jnp.int32)
        return [(slot[i : i + 1], weight) for i, (_, weight) in enumerate(both)]

    mine = slots_of([2 * p + core for p in range(planes)], sp.astype(jnp.float32))
    rest = slots_of([2 * p + 1 - core for p in range(planes)], sp.astype(jnp.float32))
    other = slots_of([2 * p + core for p in range(planes)], twin.astype(jnp.float32))
    for p in range(planes):
        slot, weight = mine[p]
        picks[p, 0:cap] = jnp.where(slot == slot_id, 1.0, 0.0).astype(jnp.bfloat16)
        own_blend = jnp.where(slot == slot_id, weight, 0.0)
        slot, weight = rest[p]
        picks[p, cap : 2 * cap] = jnp.where(slot == slot_id, 1.0, 0.0).astype(jnp.bfloat16)
        slot, weight = other[p]
        twin_blend = jnp.where(slot == slot_id, weight, 0.0)
        blends[p] = jnp.transpose(jnp.concatenate([own_blend, twin_blend], 0)).astype(jnp.bfloat16)

    order = [0] + sorted(range(1, planes), key=lambda k: -min(k, planes - k))

    plane_order = {
        1: [(order[1], 1)],
        0: [(order[1], 0)] + [(k, q) for k in order[2:] for q in (1, 0) if (k, q) != (order[-1], 0)],
    }

    def source(k):
        return (plane + k) % planes * 2 + core

    def first_row(k, q):
        return source(k) * rows + q * chunk

    def relay_strip(r):
        spread_relay(activated, r * strip, strip, sems(act_send, r), sems(act_recv, r))
        here = pl.ds(r * strip, strip)
        projected[here, :] += project(r, across_x) + project(r, across_y)

    def settle(r):
        here = pl.ds(r * strip, strip)
        spread_finish(activated, r * strip, strip, sems(act_recv, r))
        total = projected[here, :] + project(r, diagonal)
        stream_rows = (
            residual[here, :].astype(jnp.float32)
            + total.astype(jnp.bfloat16).astype(jnp.float32)
        ).astype(jnp.bfloat16)
        stream[here, :] = stream_rows
        tokens[row_block(sp * rows + r * strip, strip), col_block(tp)] = (
            stream_rows.astype(jnp.float32) * gain_row(norm_gain)
        ).astype(jnp.bfloat16)

    def send_tokens(q):
        spread_start(
            tokens, first_row(0, q), chunk, sems(spread_send, 0, q), sems(spread_recv, 0, q)
        )
        for k, part_q in plane_order[q]:
            block = tokens.at[row_block(first_row(0, part_q), chunk), col_block(tp)]
            go(
                block,
                block,
                plane_send.at[k, part_q],
                plane_recv.at[k, part_q],
                (plane - k + planes) % planes * 2 + core,
                tp,
            )
        stream_part = stream[pl.ds(q * chunk, chunk), :].astype(jnp.float32)
        square = jnp.sum(stream_part * stream_part, 1, keepdims=True)
        stats_start(4 + q, square, square)

    loads[0].wait()
    for r in (3, 2, 1, 0):
        projected[pl.ds(r * strip, strip), :] = project(r, tp)
    relay_strip(3)
    relay_strip(2)
    settle(3)
    relay_strip(1)
    settle(2)
    send_tokens(1)
    relay_strip(0)
    settle(1)
    settle(0)
    send_tokens(0)

    def spread(k, q):
        block = tokens.at[row_block(first_row(k, q), chunk), col_block(tp)]
        landed(block, plane_recv.at[k, q])
        spread_start(tokens, first_row(k, q), chunk, sems(spread_send, k, q), sems(spread_recv, k, q))

    def relay(k, q):
        spread_relay(tokens, first_row(k, q), chunk, sems(spread_send, k, q), sems(spread_recv, k, q))

    def send_wide():
        k = order[-1]
        block = tokens.at[row_block(first_row(0, 0), chunk), :]
        go(
            block,
            block,
            plane_send.at[k, 0],
            plane_recv.at[k, 0],
            (plane - k + planes) % planes * 2 + core,
            tp,
        )

    def finish(k, q):
        block = tokens.at[row_block(first_row(k, q), chunk), :]
        if (k, q) == (order[-1], 0):
            landed(block, plane_recv.at[k, q])
        else:
            spread_finish(tokens, first_row(k, q), chunk, sems(spread_recv, k, q))
        go(block, block, twin_send.at[k, q], twin_recv.at[k, q], twin, tp)

    def share_scales():
        for q in range(2):
            scales[sp, :, pl.ds(q * chunk, chunk)] = lax.rsqrt(
                stats_total(4 + q) / width + epsilon
            )
        for i in range(1, n_sp):
            go(
                scales.at[sp],
                scales.at[sp],
                scale_send.at[i],
                scale_recv.at[sp],
                (sp + i) % n_sp,
                tp,
            )

    def gather(k):
        p = (plane + k) % planes
        for q in range(2):
            start = (2 * p + 1 - core) * rows + q * chunk
            landed(tokens.at[row_block(start, chunk), :], twin_recv.at[k, q])
        for j in range(2):
            s = 2 * p + (core if j == 0 else 1 - core)
            if k == 0 and j == 0:
                pass
            else:
                landed(scales.at[s], scale_recv.at[s])
            here = pl.ds(j * cap, cap)
            pick = picks[p, here, :]
            slots[here, :] = jnp.dot(
                pick, tokens[row_block(s * rows, rows), :], preferred_element_type=jnp.float32
            ).astype(jnp.bfloat16)
            scale = jnp.sum(pick.astype(jnp.float32) * scales[s][0:1, :], 1, keepdims=True)
            since[here, :] = jnp.broadcast_to(scale, (cap, 128))

    def raise_up(k, piece):
        size = gate.shape[1] // 2
        at = pl.ds(piece * size, size)
        scale = jnp.concatenate([since[0 : 2 * cap, :]] * (size // 128), 1)
        g = scale * jnp.dot(slots[...], gate[:, at], preferred_element_type=jnp.float32)
        u = scale * jnp.dot(slots[...], up[:, at], preferred_element_type=jnp.float32)
        hidden[:, at] = (g * jax.nn.sigmoid(g) * u).astype(jnp.bfloat16)

    def bring_down(k, piece):
        size = width // 2
        at = pl.ds(piece * size, size)
        result = jnp.dot(
            hidden[...], down[:, at], preferred_element_type=jnp.float32
        ).astype(jnp.bfloat16)
        pairs[k, 0:cap, at] = result[0:cap]
        outbound[k, :, at] = result[cap:]
        if piece == 1:
            go(
                outbound.at[k],
                pairs.at[k, pl.ds(cap, cap), :],
                swap_send.at[k],
                swap_recv.at[k],
                twin,
                tp,
            )

    low, high = pl.ds(0, chunk), pl.ds(chunk, chunk)

    def combine(k):
        p = (plane + k) % planes
        landed(pairs.at[k, pl.ds(cap, cap), :], swap_recv.at[k])

        blended[k] = jnp.dot(
            blends[p], pairs[k], preferred_element_type=jnp.float32
        ).astype(jnp.bfloat16)

        for i, (part_rows, block, peer) in enumerate(
            (
                (low, diagonal, across_x),
                (high, diagonal, across_y),
                (low, across_x, across_x),
                (high, across_y, across_y),
            )
        ):
            go(
                blended.at[k, part_rows, col_block(block)],
                arrived.at[k, i, low],
                sum_send.at[k, i],
                sum_recv.at[k, i],
                sp,
                peer,
            )

    def pass_on(k):
        for i, (part_rows, peer) in enumerate(((low, across_y), (high, across_x))):
            landed(arrived.at[k, i, low], sum_recv.at[k, i])
            arrived[k, 2 + i, high] = (
                blended[k, part_rows, col_block(peer)].astype(jnp.float32)
                + arrived[k, i, low].astype(jnp.float32)
            ).astype(jnp.bfloat16)
            go(
                arrived.at[k, 2 + i, high],
                arrived.at[k, i, high],
                sum_send.at[k, 4 + i],
                sum_recv.at[k, 4 + i],
                sp,
                peer,
            )

    def give_back(k):
        for i, part_rows in enumerate((low, high)):
            landed(arrived.at[k, 2 + i, low], sum_recv.at[k, 2 + i])
            landed(arrived.at[k, i, high], sum_recv.at[k, 4 + i])
            total = (
                blended[k, part_rows, col_block(tp)].astype(jnp.float32)
                + arrived[k, 2 + i, low].astype(jnp.float32)
                + arrived[k, i, high].astype(jnp.float32)
            )
            if k == 0:
                here = pl.ds(i * chunk, chunk)
                total = total + stream[here, :].astype(jnp.float32)
                for j in order[1:]:
                    landed(returned.at[j, part_rows], back_recv.at[j, i])
                    total = total + returned[j, part_rows].astype(jnp.float32)
                mixed[here, :] = total.astype(jnp.bfloat16)
            else:
                summed[k, part_rows] = total.astype(jnp.bfloat16)
                go(
                    summed.at[k, part_rows],
                    returned.at[k, part_rows],
                    back_send.at[k, i],
                    back_recv.at[k, i],
                    source(k),
                    tp,
                )

    def weights_ready():
        for load in loads[1:]:
            load.wait()

    steps = {
        "R": relay,
        "S": spread,
        "F": finish,
        "G": gather,
        "U": raise_up,
        "D": bring_down,
        "C": combine,
        "P": pass_on,
        "V": give_back,
        "B": send_wide,
        "H": share_scales,
        "L": weights_ready,
    }
    for word in schedule:
        indices = [int(digit) for digit in word[1:]]
        steps[word[0]](*[order[i] for i in indices[:1]], *indices[1:])
    for send in sends:
        send.wait_send()


def fused(operands, rows, cols, n_sp, n_tp, cap, width, units, taps):
    planes = n_sp // 2
    pad = (taps - 1 + 15) // 16 * 16
    chunk = rows // 2
    bf16, f32 = jnp.bfloat16, jnp.float32
    dma = pltpu.SemaphoreType.DMA
    vmem = pl.BlockSpec(memory_space=pltpu.VMEM)
    anywhere = pl.BlockSpec(memory_space=pl.ANY)
    return pl.pallas_call(
        functools.partial(fused_kernel, n_sp, n_tp, cap),
        out_shape=jax.ShapeDtypeStruct((rows, cols), bf16),
        in_specs=[vmem] * 9 + [anywhere] * 4,
        out_specs=vmem,
        scratch_shapes=[
            pltpu.VMEM((width, cols), bf16),
            pltpu.VMEM((width, units), bf16),
            pltpu.VMEM((width, units), bf16),
            pltpu.VMEM((units, width), bf16),
            pltpu.VMEM((taps, cols), f32),
            pltpu.VMEM((pad + rows, cols), f32),
            pltpu.VMEM((pad + rows, 128), f32),
            pltpu.VMEM((max(rows, 2 * cap), 128), f32),
            pltpu.VMEM((rows, cols), f32),
            pltpu.VMEM((pad, cols), bf16),
            pltpu.VMEM((pad, 128), f32),
            pltpu.VMEM((pad, cols), bf16),
            pltpu.VMEM((pad, 128), f32),
            pltpu.VMEM((6, n_tp, 8, 128), f32),
            pltpu.VMEM((n_sp, 8, rows), f32),
            pltpu.VMEM((n_sp, 8, rows), f32),
            pltpu.VMEM((rows, width), bf16),
            pltpu.VMEM((rows, cols), f32),
            pltpu.VMEM((rows, cols), bf16),
            pltpu.VMEM((n_sp * rows, width), bf16),
            pltpu.VMEM((planes, 2 * cap, rows), bf16),
            pltpu.VMEM((planes, rows, 2 * cap), bf16),
            pltpu.VMEM((2 * cap, width), bf16),
            pltpu.VMEM((2 * cap, units), bf16),
            pltpu.VMEM((planes, 2 * cap, width), bf16),
            pltpu.VMEM((planes, cap, width), bf16),
            pltpu.VMEM((planes, rows, width), bf16),
            pltpu.VMEM((planes, 4, rows, cols), bf16),
            pltpu.VMEM((planes, rows, cols), bf16),
            pltpu.VMEM((planes, rows, cols), bf16),
            dma((4,)),
            dma((2,)),
            dma((2,)),
            dma((6, n_tp)),
            dma((6, n_tp)),
            dma((n_sp,)),
            dma((n_sp,)),
            dma((n_sp,)),
            dma((n_sp,)),
            dma((4, 4)),
            dma((4, 4)),
            dma((planes, 2)),
            dma((planes, 2)),
            dma((planes, 2, 4)),
            dma((planes, 2, 4)),
            dma((planes, 2)),
            dma((planes, 2)),
            dma((planes,)),
            dma((planes,)),
            dma((planes, 6)),
            dma((planes, 6)),
            dma((planes, 2)),
            dma((planes, 2)),
        ],
        compiler_params=pltpu.CompilerParams(
            collective_id=0, has_side_effects=True, vmem_limit_bytes=56 << 20
        ),
    )(*operands)


def per_device(
    residual_in,
    conv_value,
    conv_gate,
    doc_ids,
    conv_kernel,
    ln_gain,
    out_weight,
    norm_gain,
    routes,
    route_weight,
    gate_w,
    up_w,
    down_w,
):
    rows, cols = residual_in.shape
    n_sp = lax.axis_size("sp")
    n_tp = lax.axis_size("tp")
    cap = 4 * rows // n_sp
    _, width, units = gate_w.shape
    group_rows = n_sp // groups * cap
    taps = conv_kernel.shape[0]
    pad = (taps - 1 + 15) // 16 * 16
    if n_tp == 4 and n_sp == 8:
        operands = (
            residual_in,
            conv_value,
            conv_gate,
            doc_ids.reshape(1, rows),
            conv_kernel,
            ln_gain.reshape(cols // 128, 128),
            norm_gain.reshape(cols // 128, 128),
            routes.T,
            route_weight.T,
            out_weight,
            gate_w[0],
            up_w[0],
            down_w[0],
        )
        return fused(operands, rows, cols, n_sp, n_tp, cap, width, units, taps)
    bf16, f32 = jnp.bfloat16, jnp.float32
    dma = pltpu.SemaphoreType.DMA
    vmem = pl.BlockSpec(memory_space=pltpu.VMEM)
    anywhere = pl.BlockSpec(memory_space=pl.ANY)
    return pl.pallas_call(
        functools.partial(layer_kernel, n_sp, n_tp, cap),
        out_shape=jax.ShapeDtypeStruct((rows, cols), bf16),
        in_specs=[vmem] * 9 + [anywhere] * 4,
        out_specs=vmem,
        scratch_shapes=[
            pltpu.VMEM((width, cols), bf16),
            pltpu.VMEM((width, units), bf16),
            pltpu.VMEM((width, units), bf16),
            pltpu.VMEM((units, width), bf16),
            pltpu.VMEM((taps, cols), f32),
            pltpu.VMEM((pad + rows, cols), f32),
            pltpu.VMEM((pad + rows, 128), f32),
            pltpu.VMEM((rows, 128), f32),
            pltpu.VMEM((rows, cols), f32),
            pltpu.VMEM((pad, cols), bf16),
            pltpu.VMEM((pad, 128), f32),
            pltpu.VMEM((pad, cols), bf16),
            pltpu.VMEM((pad, 128), f32),
            pltpu.VMEM((2, n_tp, 8, rows), f32),
            pltpu.VMEM((rows, width), bf16),
            pltpu.VMEM((rows, cols), f32),
            pltpu.VMEM((rows, cols), bf16),
            pltpu.VMEM((rows, cols), bf16),
            pltpu.VMEM((n_sp, rows, cap), bf16),
            pltpu.VMEM((n_sp, cap, cols), bf16),
            pltpu.VMEM((n_sp * cap, width), bf16),
            pltpu.VMEM((group_rows, units), bf16),
            pltpu.VMEM((groups, group_rows, width), bf16),
            pltpu.VMEM((groups, n_tp, group_rows, cols), bf16),
            pltpu.VMEM((groups, group_rows, cols), bf16),
            pltpu.VMEM((n_sp, cap, cols), bf16),
            pltpu.VMEM((n_sp, rows, cap), bf16),
            pltpu.VMEM((n_sp, rows, cap), bf16),
            dma((4,)),
            dma((2,)),
            dma((2,)),
            dma((2, n_tp)),
            dma((2, n_tp)),
            dma((n_tp,)),
            dma((n_tp,)),
            dma((n_sp,)),
            dma((n_sp,)),
            dma((groups, n_tp)),
            dma((groups, n_tp)),
            dma((groups, n_tp + 2)),
            dma((groups, n_tp + 2)),
            dma((n_sp,)),
            dma((n_sp,)),
        ],
        compiler_params=pltpu.CompilerParams(
            collective_id=0, has_side_effects=True, vmem_limit_bytes=54 << 20
        ),
    )(
        residual_in,
        conv_value,
        conv_gate,
        doc_ids.reshape(1, rows),
        conv_kernel,
        ln_gain.reshape(1, cols),
        norm_gain.reshape(1, cols),
        routes,
        route_weight,
        out_weight,
        gate_w[0],
        up_w[0],
        down_w[0],
    )


def solution(mesh):
    in_specs = (
        P("sp", "tp"),
        P("sp", "tp"),
        P("sp", "tp"),
        P("sp"),
        P(None, "tp"),
        P("tp"),
        P(None, "tp"),
        P("tp"),
        P("sp", None),
        P("sp", None),
        P("sp", None, "tp"),
        P("sp", None, "tp"),
        P("sp", "tp", None),
    )
    out_specs = P("sp", "tp")
    return jax.shard_map(
        per_device, mesh=mesh, in_specs=in_specs, out_specs=out_specs, check_vma=False
    )
```
